32 devices in a mesh: sp: 8 (over z, x), tp: 4 (over y, core).
Axes of the slice: x: 2, y: 2, z: 4, core: 2. Of those that a mesh axis runs over, the one named last changes fastest.
Arguments:
- query_one: bfloat16 [2048, 512], P('sp', 'tp'), may hold values from -100 to 100, as said below
- key_one: bfloat16 [2048, 512], P('sp', 'tp'), may hold values from -8 to 8
- query_two: bfloat16 [2048, 512], P('sp', 'tp'), may hold values from -100 to 100, as said below
- key_two: bfloat16 [2048, 512], P('sp', 'tp'), may hold values from -8 to 8
- values: bfloat16 [2048, 1024], P('sp', 'tp'), may hold values from -6 to 6
- mix_lambda: float32 [8], P('tp'), may hold values from 0.3 to 0.8
- head_gain: float32 [128], replicated, may hold values from 0.1 to 1.9
- residual_in: bfloat16 [2048, 2048], P(('sp', 'tp')), may hold values from -6 to 6
- out_weight: bfloat16 [1024, 2048], replicated, may hold values from -0.1875 to 0.1875
- norm_gain: float32 [2048], replicated, may hold values from 0.1 to 1.9
- route_ids: int32 [2048, 2], P(('sp', 'tp')), may hold values from 0 to 15, all different within a row; in each aligned block of 64 rows (0 to 63, 64 to 127, ...) at most 16 rows name the same one
- route_logits: float32 [2048, 2], P(('sp', 'tp')), may hold values from -6 to 6
- group_prob: float32 [2048], P(('sp', 'tp')), may hold values from 0.25 to 1
- gate_weight: bfloat16 [16, 2048, 1024], P('sp', None, 'tp'), may hold values from -0.125 to 0.125
- up_weight: bfloat16 [16, 2048, 1024], P('sp', None, 'tp'), may hold values from -0.125 to 0.125
- down_weight: bfloat16 [16, 1024, 2048], P('sp', 'tp'), may hold values from -0.1875 to 0.1875
Outputs:
- layer_out: bfloat16 [2048, 2048], P(('sp', 'tp'))
The draws below stay inside these ranges and needn't reach their ends.
Inputs may be any that keep to these rules, and one draw needn't show every extreme that they name: `query_one`: drawn together with key_one. `query_two`: drawn together with key_two. `route_ids`: the experts of a row differ. In the rows of one device no expert is named more than 16 times, a bound that some block reaches.
All inputs are finite; a program needn't handle non-finite values.
Results may differ from the reference program's by a relative error of at most 0.014.
Values may be sent and summed in bfloat16 or wider, within the bound.
A program may use at most 128 MiB of HBM per device.

```python
import math
import jax
import jax.numpy as jnp
import numpy as np
from jax import lax

D = 2048
HEADS = 8
QK = 64
VD = 128
FF = 1024
TOP = 2
ROWS = 64
TOKENS = 2048
MIXW = 1024
EXPERTS = 16
CAP = 16
N_SP = 8
N_TP = 4


def draw_maps(key, which):
    streams = jax.random.split(jax.random.fold_in(key, which), 2)
    keys_drawn = 1.3 * jax.random.normal(streams[0], (TOKENS, HEADS * QK), jnp.float32)
    queries = 1.3 * jax.random.normal(streams[1], (TOKENS, HEADS * QK), jnp.float32)
    queries = jnp.clip(queries, -100.0, 100.0)
    keys_drawn = jnp.clip(keys_drawn, -8.0, 8.0)
    return (queries, keys_drawn)


def draw_query_one(key, part):
    return draw_maps(key, 11)[0].astype(jnp.bfloat16)


def draw_key_one(key, part):
    return draw_maps(key, 11)[1].astype(jnp.bfloat16)


def draw_query_two(key, part):
    return draw_maps(key, 23)[0].astype(jnp.bfloat16)


def draw_key_two(key, part):
    return draw_maps(key, 23)[1].astype(jnp.bfloat16)


def levels(key, shape, cuts, low, top_value):
    loudness = 1.0
    for position, parts in cuts:
        steps = jax.random.uniform(jax.random.fold_in(jax.random.fold_in(key, 6), position), (parts,), jnp.float32, low / len(cuts), top_value / len(cuts))
        loudness = loudness * jnp.repeat(jnp.exp(steps), shape[position] // parts).reshape((-1,) + (1,) * (len(shape) - 1 - position))
    return loudness


def deal_out(stream_key, own, number, rows, count, top, most, slope):
    sequence = jax.random.permutation(stream_key, count)
    crowded, common = load_shares(count, rows * top, most, slope, True), load_shares(count, rows * top, most, slope, False)
    places = jnp.arange(count)

    def named(sizes, rotation):
        used = int((sizes > 0).sum())
        fixed = max(1, used // 4)
        passed = fixed + (places - fixed + rotation * (used - fixed)) % max(1, count - fixed)
        return jnp.zeros((count,), jnp.int32).at[sequence[jnp.where(places < fixed, places, passed)]].set(jnp.asarray(sizes, jnp.int32))

    sizes = jnp.where(number % 4 == 0, named(crowded, number // 4), named(common, number - number // 4 - 1))
    mixed = jax.random.permutation(jax.random.fold_in(own, 3), count)
    donor, taker = mixed[0:count // 2 * 2:2], mixed[1:count // 2 * 2:2]
    slack = jnp.minimum(sizes[donor] - 1, most - sizes[taker]) // 2
    slack = jnp.where((donor == sequence[0]) | (taker == sequence[0]) | (sizes[taker] == 0), 0, jnp.maximum(slack, 0))
    passed = jax.random.randint(jax.random.fold_in(own, 4), (count // 2,), 0, 1 << 20) % (slack + 1)
    sizes = sizes.at[donor].add(-passed).at[taker].add(passed)
    labels = jnp.searchsorted(jnp.cumsum(sizes), jnp.arange(rows * top), side="right").astype(jnp.int32)
    grid = labels.reshape(top, rows).T
    grid = grid[jax.random.permutation(jax.random.fold_in(own, 1), rows)]
    rotation = jax.random.randint(jax.random.fold_in(own, 2), (rows, 1), 0, top)
    return jnp.take_along_axis(grid, (jnp.arange(top)[None, :] + rotation) % top, axis=1)


def load_shares(count, total, most, lean, full):
    portions = [(1 << 20) // math.isqrt(rank ** lean) + 1 for rank in range(1, count + 1)]
    largest = most if full else min(most, max(-(-total // count), total * portions[0] // sum(portions)))
    least = 1 if total - largest >= count - 1 else 0
    given, surplus = [largest] + [least] * (count - 1), total - largest - least * (count - 1)
    while surplus > 0:
        movable = [i for i in range(1, count) if given[i] < largest] or [i for i in range(1, count) if given[i] < most]
        pool, budget = sum([portions[i] for i in movable]), surplus
        for i in movable:
            more = min(most - given[i], max(1, budget * portions[i] // pool), surplus)
            given[i] = given[i] + more
            surplus = surplus - more
    return np.array(given)


def normal_values(key, shape, spread, reach, shards=(), held_as=jnp.bfloat16):
    entries = jax.random.normal(key, shape, jnp.float32) * spread
    if len(shards) > 0:
        entries = levels(key, shape, shards, -0.22, 0.18) * entries
    return jnp.clip(entries, min=-reach, max=reach).astype(held_as)


def setup_inputs(seed: int = 0) -> dict:
    splits = jax.random.split(jax.random.key(seed), 17)
    query_one = draw_query_one(jax.random.fold_in(splits[16], 71), 0)
    key_one = draw_key_one(jax.random.fold_in(splits[16], 71), 0)
    query_two = draw_query_two(jax.random.fold_in(splits[16], 71), 0)
    key_two = draw_key_two(jax.random.fold_in(splits[16], 71), 0)
    values = normal_values(splits[4], (TOKENS, MIXW), 1.0, 6.0, ((0, 8), (1, 4)))
    mix_lambda = jnp.clip(0.3 + 0.5 * jax.random.uniform(splits[5], (HEADS,), jnp.float32) ** levels(splits[5], (HEADS,), ((0, 4),), -0.2, 0.2), 0.3, 0.8)
    head_gain = jnp.clip(1.0 + 0.18 * jax.random.normal(splits[6], (VD,), jnp.float32), 0.1, 1.9)
    residual_in = normal_values(splits[7], (TOKENS, D), 1.0, 6.0, ((0, 32),))
    out_weight = normal_values(splits[8], (MIXW, D), MIXW ** -0.5, 0.1875)
    norm_gain = jnp.clip(1.0 + 0.18 * jax.random.normal(splits[9], (D,), jnp.float32), 0.1, 1.9)
    route_ids_keys = jax.random.split(jax.random.fold_in(splits[10], 1), TOKENS // ROWS)
    route_ids_turns = jax.random.permutation(jax.random.fold_in(splits[10], 3), TOKENS // ROWS)
    route_ids = jax.vmap(lambda own, number: deal_out(jax.random.fold_in(splits[10], 2), own, number, ROWS, EXPERTS, TOP, CAP, 2))(route_ids_keys, route_ids_turns).reshape((TOKENS, TOP))
    route_logits = normal_values(splits[11], (TOKENS, TOP), 1.0, 6.0, ((0, 32),), jnp.float32)
    group_prob = jnp.clip(0.25 + 0.75 * jax.random.uniform(splits[12], (TOKENS,), jnp.float32) ** levels(splits[12], (TOKENS,), ((0, 32),), -0.2, 0.2), 0.25, 1.0)
    gate_weight = normal_values(splits[13], (EXPERTS, D, FF), D ** -0.5, 0.125, ((0, 8), (2, 4)))
    up_weight = normal_values(splits[14], (EXPERTS, D, FF), D ** -0.5, 0.125, ((0, 8), (2, 4)))
    down_weight = normal_values(splits[15], (EXPERTS, FF, D), FF ** -0.5, 0.1875, ((0, 8), (1, 4)))
    return {"query_one": query_one, "key_one": key_one, "query_two": query_two, "key_two": key_two, "values": values, "mix_lambda": mix_lambda, "head_gain": head_gain, "residual_in": residual_in, "out_weight": out_weight, "norm_gain": norm_gain, "route_ids": route_ids, "route_logits": route_logits, "group_prob": group_prob, "gate_weight": gate_weight, "up_weight": up_weight, "down_weight": down_weight}


norm_epsilon = 1e-06

def round_kept(value):
    return lax.optimization_barrier(value.astype(jnp.bfloat16)).astype(jnp.float32)

def head_output(query_a, key_a, query_b, key_b, head_values, weight_two, gain):
    score_scale = 1.0 / math.sqrt(QK)
    block_rows = min(512, TOKENS)

    def one_map(queries, keys):
        scores = jnp.dot(queries, keys.T, preferred_element_type=jnp.float32) * score_scale
        top_score = lax.optimization_barrier(jnp.max(scores, axis=-1, keepdims=True))
        expo = jnp.exp(scores - top_score)
        summed = lax.optimization_barrier(jnp.sum(expo, axis=-1, keepdims=True))
        return jnp.dot(expo.astype(jnp.bfloat16), head_values, preferred_element_type=jnp.float32) / summed

    def one_block(pair):
        block_a, block_b = pair
        combined = one_map(block_a, key_a) - weight_two * one_map(block_b, key_b)
        combined = combined * lax.rsqrt(lax.optimization_barrier(jnp.mean(combined * combined, axis=-1, keepdims=True)) + norm_epsilon) * gain
        return combined.astype(jnp.bfloat16)
    blocks = lax.map(one_block, (query_a.reshape(TOKENS // block_rows, block_rows, QK), query_b.reshape(TOKENS // block_rows, block_rows, QK)))
    return blocks.reshape(TOKENS, VD)

def reference(query_one, key_one, query_two, key_two, values, mix_lambda, head_gain, residual_in, out_weight, norm_gain, route_ids, route_logits, group_prob, gate_weight, up_weight, down_weight):

    def by_head(array, size):
        return array.reshape(TOKENS, HEADS, size).transpose(1, 0, 2)

    def run_head(packed):
        qa, ka, qb, kb, vals, weight_two = packed
        return head_output(qa, ka, qb, kb, vals, weight_two, head_gain)
    heads_out = lax.map(run_head, (by_head(query_one, QK), by_head(key_one, QK), by_head(query_two, QK), by_head(key_two, QK), by_head(values, VD), mix_lambda))
    attended = heads_out.transpose(1, 0, 2).reshape(TOKENS, MIXW)
    mix = jnp.dot(attended, out_weight, preferred_element_type=jnp.float32)
    hidden = (residual_in.astype(jnp.float32) + mix).astype(jnp.bfloat16)
    hidden_f = hidden.astype(jnp.float32)
    normed = (hidden_f * lax.rsqrt(lax.optimization_barrier(jnp.mean(hidden_f * hidden_f, axis=-1, keepdims=True)) + norm_epsilon) * norm_gain).astype(jnp.bfloat16)
    route_weight = jax.nn.softmax(route_logits, axis=-1) * group_prob[:, None]
    flat_ids = route_ids.reshape(-1)
    flat_weight = route_weight.reshape(-1)
    limit = CAP * N_SP * N_TP
    positions = jnp.arange(TOKENS * TOP, dtype=jnp.int32)
    block_ff = FF // N_TP

    def expert_step(running, expert):
        hit = flat_ids == expert
        rank = jnp.cumsum(hit.astype(jnp.int32)) - 1
        where_to = jnp.where(hit, rank, limit).astype(jnp.int32)
        chosen = jnp.zeros((limit,), jnp.int32).at[where_to].set(positions, mode='drop')
        live = jnp.zeros((limit,), jnp.float32).at[where_to].set(1.0, mode='drop')
        token_of = chosen // TOP
        picked = normed[token_of]
        gate = jnp.dot(picked, gate_weight[expert], preferred_element_type=jnp.float32)
        upper = jnp.dot(picked, up_weight[expert], preferred_element_type=jnp.float32)
        middle = (jax.nn.silu(gate) * upper).astype(jnp.bfloat16)
        down = down_weight[expert]
        summed = jnp.zeros((limit, D), jnp.float32)
        for piece in range(N_TP):
            part_sum = jnp.dot(middle[:, piece * block_ff:(piece + 1) * block_ff], down[piece * block_ff:(piece + 1) * block_ff], preferred_element_type=jnp.float32)
            summed = summed + round_kept(part_sum)
        expert_out = round_kept(summed)
        scaled = expert_out * (flat_weight[chosen] * live)[:, None]
        return (running.at[token_of].add(scaled), None)
    moe, _ = lax.scan(expert_step, jnp.zeros((TOKENS, D), jnp.float32), jnp.arange(EXPERTS, dtype=jnp.int32))
    return (hidden_f + moe).astype(jnp.bfloat16)
```

```python
import functools
import math

import jax
import jax.numpy as jnp
from jax import lax
from jax.experimental import pallas as pl
from jax.experimental.pallas import tpu as pltpu
from jax.sharding import PartitionSpec as P

norm_epsilon = 1e-06
MESH = pl.DeviceIdType.MESH
VMEM_LIMIT = 60 * 1024 * 1024


def pair_of(count):
    return 2 if count % 2 == 0 else 1


def greet(peers):
    barrier = pltpu.get_barrier_semaphore()
    for peer in peers:
        pl.semaphore_signal(barrier, inc=1, device_id=peer, device_id_type=MESH)
    pl.semaphore_wait(barrier, len(peers))


def attend_kernel(
    n_sp,
    n_tp,
    vd,
    k1_ref,
    k2_ref,
    v_ref,
    q1_ref,
    q2_ref,
    lam_ref,
    gain_ref,
    out_ref,
    kvp,
    qp,
    held,
    q_far,
    m_ref,
    l_ref,
    acc_ref,
    stage,
    cross_send,
    cross_recv,
    line_send,
    line_recv,
    side_send,
    side_recv,
    head_send,
    head_recv,
):
    inner = pair_of(n_sp)
    length = n_sp // inner
    half = length // 2
    me = lax.axis_index("sp")
    mt = lax.axis_index("tp")
    z, x = me // inner, me % inner
    head, zi = z // half, z % half
    rows = q1_ref.shape[0]
    qk = q1_ref.shape[1] // 2
    scale = 1.0 / math.sqrt(qk)
    exact = math.frexp(scale)[0] == 0.5
    early, after = (scale, 1.0) if exact else (1.0, scale)
    other = z * inner + (inner - 1 - x)
    mirror = (length - 1 - z) * inner + x
    far_zi = half - 1 - zi
    for h in range(2):
        kvp[h, :, 0:qk] = k1_ref[:, h * qk : (h + 1) * qk]
        kvp[h, :, qk : 2 * qk] = k2_ref[:, h * qk : (h + 1) * qk]
        kvp[h, :, 2 * qk : 2 * qk + vd] = v_ref[:, h * vd : (h + 1) * vd]
        qp[h, :, 0:qk] = q1_ref[:, h * qk : (h + 1) * qk] * jnp.bfloat16(early)
        qp[h, :, qk : 2 * qk] = q2_ref[:, h * qk : (h + 1) * qk] * jnp.bfloat16(early)

    def line_device(zz):
        return (head * half + zz) * inner + x

    peers = [{"sp": me, "tp": (mt + t) % n_tp} for t in range(1, n_tp)]
    peers += [{"sp": mirror, "tp": (mt + t) % n_tp} for t in range(n_tp)]
    if inner == 2:
        peers.append({"sp": other, "tp": mt})
    if half > 1:
        for shift in sorted({1, half - 1}):
            peers.append({"sp": line_device((zi + shift) % half), "tp": mt})
    greet(peers)

    def remote(src, dst, send, recv, sp):
        return pltpu.make_async_remote_copy(
            src_ref=src,
            dst_ref=dst,
            send_sem=send,
            recv_sem=recv,
            device_id={"sp": sp, "tp": mt},
            device_id_type=MESH,
        )

    cross_q = remote(qp.at[1 - head], q_far, cross_send.at[0], cross_recv.at[0], mirror)
    cross_kv = remote(
        kvp.at[1 - head], held.at[1, far_zi, x], cross_send.at[1], cross_recv.at[1], mirror
    )

    def line_copy(j, src, zz, way):
        ahead = jnp.clip(jnp.where(way == 0, zi + 1, zi - 1), 0, half - 1)
        return remote(
            src,
            held.at[j, zz, x],
            line_send.at[j, way, zz],
            line_recv.at[j, zz],
            line_device(ahead),
        )

    def side_copy(j, src, zz):
        return remote(src, held.at[j, zz, x], side_send.at[j, zz], side_recv.at[j, zz], other)

    def start_from(j, src):
        @pl.when(zi + 1 < half)
        def _():
            line_copy(j, src, zi, 0).start()

        @pl.when(zi > 0)
        def _():
            line_copy(j, src, zi, 1).start()

        if inner == 2:
            side_copy(j, src, zi).start()

    own = kvp.at[head]
    cross_kv.start()
    start_from(0, own)
    cross_q.start()
    m_ref[...] = jnp.full(m_ref.shape, -1e30, jnp.float32)
    l_ref[...] = jnp.zeros(l_ref.shape, jnp.float32)
    acc_ref[...] = jnp.zeros(acc_ref.shape, jnp.float32)

    def absorb(block, q_ref, group):
        vals = block[:, 2 * qk : 2 * qk + vd]
        for which in range(2):
            at = 2 * group + which
            scores = lax.dot_general(
                q_ref[:, which * qk : (which + 1) * qk],
                block[:, which * qk : (which + 1) * qk],
                (((1,), (1,)), ((), ())),
                preferred_element_type=jnp.float32,
            )
            if after != 1.0:
                scores = scores * after
            old = m_ref[at]
            new = jnp.maximum(old, jnp.max(scores, axis=1, keepdims=True))
            shrink = jnp.exp(old - new)
            expo = jnp.exp(scores - new[:, :1])
            m_ref[at] = new
            l_ref[at] = l_ref[at] * shrink + jnp.sum(expo, axis=1, keepdims=True)
            acc_ref[at] = acc_ref[at] * shrink[:, :1] + jnp.dot(
                expo.astype(jnp.bfloat16), vals, preferred_element_type=jnp.float32
            )

    q_own = qp.at[head]

    def absorb_both(block):
        absorb(block, q_own, 0)
        absorb(block, q_far, 1)

    def place(n):
        dist = (n + 1) // 2
        return jnp.where(n % 2 == 1, zi - dist, zi + dist), 1 - n % 2

    def line_steps(j, take):
        def line_step(n, carry):
            zz, way = place(n)

            @pl.when((zz >= 0) & (zz < half))
            def _():
                block = held.at[j, zz, x]
                line_copy(j, block, zz, way).wait_recv()
                ahead = jnp.where(way == 0, zi + 1, zi - 1)

                @pl.when((ahead >= 0) & (ahead < half))
                def _():
                    line_copy(j, block, zz, way).start()

                if inner == 2:
                    side_copy(j, block, zz).start()
                take(block)

            return carry

        lax.fori_loop(1, 2 * half - 1, line_step, 0)

    def line_again(j):
        def again(n, carry):
            zz, _ = place(n)

            @pl.when((zz >= 0) & (zz < half))
            def _():
                absorb(held.at[j, zz, x], q_far, 1)

            return carry

        lax.fori_loop(1, 2 * half - 1, again, 0)

    def side_steps(j, begin):
        def side_step(n, carry):
            zz, _ = place(n)

            @pl.when((zz >= 0) & (zz < half))
            def _():
                block = held.at[j, zz, 1 - x]
                side_copy(j, block, zz).wait_recv()
                absorb_both(block)

            return carry

        lax.fori_loop(begin, 2 * half - 1, side_step, 0)

    near = held.at[0, zi, 1 - x]
    far = held.at[1, zi, x]
    absorb(own, q_own, 0)
    if inner == 2:
        side_copy(0, near, zi).wait_recv()
        absorb(near, q_own, 0)
    line_steps(0, lambda block: absorb(block, q_own, 0))
    cross_kv.wait_recv()
    start_from(1, far)
    absorb(far, q_own, 0)
    cross_q.wait_recv()
    absorb(own, q_far, 1)
    absorb(far, q_far, 1)
    line_steps(1, absorb_both)
    line_again(0)
    if inner == 2:
        absorb(near, q_far, 1)
        side_steps(0, 1)
        side_steps(1, 0)

    share = rows // n_tp
    lam = lam_ref[head]
    columns = pl.ds(pl.multiple_of((mt * 2 + head) * vd, vd), vd)
    copies = []
    for group, sp in ((1, mirror), (0, me)):
        read_a = acc_ref[2 * group] / l_ref[2 * group][:, :1]
        read_b = acc_ref[2 * group + 1] / l_ref[2 * group + 1][:, :1]
        combined = read_a - lam * read_b
        combined = (
            combined
            * lax.rsqrt(jnp.mean(combined * combined, axis=-1, keepdims=True) + norm_epsilon)
            * gain_ref[...]
        )
        stage[group] = combined.astype(jnp.bfloat16)
        for t in range(n_tp):
            to = (mt + t) % n_tp
            span = pl.ds(pl.multiple_of(to * share, share), share)
            if group == 0 and t == 0:
                out_ref[:, columns] = stage[0, span, :]
                continue
            copy = pltpu.make_async_remote_copy(
                src_ref=stage.at[group, span],
                dst_ref=out_ref.at[:, columns],
                send_sem=head_send.at[group, t],
                recv_sem=head_recv.at[group, t],
                device_id={"sp": sp, "tp": to},
                device_id_type=MESH,
            )
            copy.start()
            copies.append(copy)

    cross_q.wait_send()
    cross_kv.wait_send()
    for j in range(2):

        def drain(n, carry):
            zz, way = place(n)

            @pl.when((zz >= 0) & (zz < half))
            def _():
                ahead = jnp.where(way == 0, zi + 1, zi - 1)

                @pl.when((ahead >= 0) & (ahead < half))
                def _():
                    line_copy(j, own, zz, way).wait_send()

                if inner == 2:
                    side_copy(j, own, zz).wait_send()

            return carry

        lax.fori_loop(1, 2 * half - 1, drain, 0)

        @pl.when(zi + 1 < half)
        def _():
            line_copy(j, own, zi, 0).wait_send()

        @pl.when(zi > 0)
        def _():
            line_copy(j, own, zi, 1).wait_send()

        if inner == 2:
            side_copy(j, own, zi).wait_send()
    for copy in copies:
        copy.wait()


def attend(n_sp, n_tp, k1, k2, v, q1, q2, lam, gain):
    rows = q1.shape[0]
    inner = pair_of(n_sp)
    half = n_sp // inner // 2
    assert lam.shape[0] == 2 and half * inner * 2 == n_sp
    vd = v.shape[1] // 2
    qk = q1.shape[1] // 2
    cols = 2 * qk + vd
    vmem = pl.BlockSpec(memory_space=pltpu.VMEM)
    dma = pltpu.SemaphoreType.DMA
    return pl.pallas_call(
        functools.partial(attend_kernel, n_sp, n_tp, vd),
        out_shape=jax.ShapeDtypeStruct((rows // n_tp, n_tp * 2 * vd), jnp.bfloat16),
        in_specs=[vmem] * 5 + [pl.BlockSpec(memory_space=pltpu.SMEM), vmem],
        out_specs=vmem,
        scratch_shapes=[
            pltpu.VMEM((2, rows, cols), jnp.bfloat16),
            pltpu.VMEM((2, rows, 2 * qk), jnp.bfloat16),
            pltpu.VMEM((2, half, inner, rows, cols), jnp.bfloat16),
            pltpu.VMEM((rows, 2 * qk), jnp.bfloat16),
            pltpu.VMEM((4, rows, 128), jnp.float32),
            pltpu.VMEM((4, rows, 128), jnp.float32),
            pltpu.VMEM((4, rows, vd), jnp.float32),
            pltpu.VMEM((2, rows, vd), jnp.bfloat16),
            dma((2,)),
            dma((2,)),
            dma((2, 2, half)),
            dma((2, half)),
            dma((2, half)),
            dma((2, half)),
            dma((2, n_tp)),
            dma((2, n_tp)),
        ],
        compiler_params=pltpu.CompilerParams(
            collective_id=0, has_side_effects=True, vmem_limit_bytes=VMEM_LIMIT
        ),
    )(k1, k2, v, q1, q2, lam, gain)


def layered_kernel(
    n_sp,
    n_tp,
    vd,
    k1_ref,
    k2_ref,
    v_ref,
    q1_ref,
    q2_ref,
    lam_ref,
    gain_ref,
    out_ref,
    kv_out,
    q_out,
    held,
    q_in,
    qt,
    m_ref,
    l_ref,
    acc_ref,
    stage,
    lam_mine,
    lam_far,
    first_send,
    core_send,
    side_send,
    kv_recv,
    q_recv,
    lam_sem,
    head_send,
    head_recv,
):
    inner, pair = 2, 2
    length = n_sp // inner
    me, mt = lax.axis_index("sp"), lax.axis_index("tp")
    z, x = me // inner, me % inner
    y, c = mt // pair, mt % pair
    rows, qk = q1_ref.shape[0], q1_ref.shape[1] // 2
    keys = 2 * qk
    scale = 1.0 / math.sqrt(qk)
    exact = math.frexp(scale)[0] == 0.5
    early, after = (scale, 1.0) if exact else (1.0, scale)
    home = c == z // pair
    partner = y * pair + (1 - c)
    across = z * inner + (1 - x)

    def spot(zz):
        return zz * inner + x

    barrier = pltpu.get_barrier_semaphore()
    peers = [(spot(zz), t) for zz in range(length) for t in range(n_tp)]
    for sp, tp in peers:

        @pl.when((sp != me) | (tp != mt))
        def _():
            pl.semaphore_signal(
                barrier, inc=1, device_id={"sp": sp, "tp": tp}, device_id_type=MESH
            )

    pl.semaphore_signal(barrier, inc=1, device_id={"sp": across, "tp": mt}, device_id_type=MESH)

    for h in range(2):
        at = slice(h * qk, (h + 1) * qk)
        block = jnp.concatenate([k1_ref[:, at], k2_ref[:, at]], axis=1)
        turned = jnp.concatenate(
            [
                v_ref[r : r + vd, h * vd : (h + 1) * vd].astype(jnp.float32).T
                for r in range(0, rows, vd)
            ],
            axis=0,
        ).astype(jnp.bfloat16)
        query = jnp.concatenate([q1_ref[:, at], q2_ref[:, at]], axis=1) * jnp.bfloat16(early)
        kv_out[h, :, 0:keys] = block
        kv_out[h, :, keys : keys + vd] = turned
        q_out[h] = query

        @pl.when(z == pair * c + h)
        def _():
            held[z, 0, :, 0:keys] = block
            held[z, 0, :, keys : keys + vd] = turned
            q_in[h] = query

    lam_mine[...] = jnp.full(lam_mine.shape, lam_ref[z % pair], jnp.float32)
    m_ref[...] = jnp.full(m_ref.shape, -1e30, jnp.float32)
    l_ref[...] = jnp.zeros(l_ref.shape, jnp.float32)
    acc_ref[...] = jnp.zeros(acc_ref.shape, jnp.float32)
    qt[...] = jnp.zeros(qt.shape, qt.dtype)
    pl.semaphore_wait(barrier, len(peers))

    def remote(src, dst, send, recv, sp, tp):
        return pltpu.make_async_remote_copy(
            src_ref=src,
            dst_ref=dst,
            send_sem=send,
            recv_sem=recv,
            device_id={"sp": sp, "tp": tp},
            device_id_type=MESH,
        )

    def first_q(h):
        return remote(
            q_out.at[h],
            q_in.at[z % pair],
            first_send.at[0, h],
            q_recv.at[z % pair],
            spot(pair * c + h),
            y * pair + z // pair,
        )

    def first_kv(h):
        return remote(
            kv_out.at[h],
            held.at[z, 0],
            first_send.at[1, h],
            kv_recv.at[z, 0],
            spot(pair * c + h),
            y * pair + z // pair,
        )

    def to_core(zz, side):
        block = held.at[zz, side]
        return remote(block, block, core_send.at[zz, side], kv_recv.at[zz, side], me, partner)

    def to_side(zz):
        return remote(
            held.at[zz, 0], held.at[zz, 1], side_send.at[zz], kv_recv.at[zz, 1], across, mt
        )

    lam_copy = remote(lam_mine, lam_far, lam_sem.at[0], lam_sem.at[1], me, partner)

    def away(h):
        return z != pair * c + h

    order = [z, z + 1 - 2 * (z % pair), pair - z // pair, (length - 1) * (1 - z // pair)]

    @pl.when(home)
    def _():
        to_side(z).start()
        to_core(z, 0).start()

    for h in range(2):

        @pl.when(away(h))
        def _():
            first_q(h).start()

    for h in range(2):

        @pl.when(away(h))
        def _():
            first_kv(h).start()

    lam_copy.start()

    for g in range(2):

        @pl.when((z != pair * c + g))
        def _():
            remote(
                q_out.at[g], q_in.at[g], first_send.at[0, g], q_recv.at[g], me, mt
            ).wait_recv()

        turned = q_in[g].astype(jnp.float32).T.astype(jnp.bfloat16)
        qt[0:qk, 2 * g * rows : (2 * g + 1) * rows] = turned[0:qk]
        qt[qk:keys, (2 * g + 1) * rows : (2 * g + 2) * rows] = turned[qk:keys]

    def absorb(zz, side):
        block_keys = held[zz, side, :, 0:keys]
        turned = jnp.concatenate(
            [held[zz, side, r : r + vd, keys : keys + vd] for r in range(0, rows, vd)], axis=1
        )
        for part in range(4):
            at = slice(part * rows, (part + 1) * rows)
            scores = jnp.dot(block_keys, qt[:, at], preferred_element_type=jnp.float32)
            if after != 1.0:
                scores = scores * after
            old = m_ref[:, at]
            new = jnp.maximum(old, jnp.max(scores, axis=0, keepdims=True))
            shrink = jnp.exp(old - new)
            expo = jnp.exp(scores - new)
            m_ref[:, at] = new
            l_ref[:, at] = l_ref[:, at] * shrink + jnp.sum(expo, axis=0, keepdims=True)
            acc_ref[:, at] = acc_ref[:, at] * shrink + jnp.dot(
                turned, expo.astype(jnp.bfloat16), preferred_element_type=jnp.float32
            )

    def take(zz):
        direct = zz // pair == c

        @pl.when((zz != z) | jnp.logical_not(home))
        def _():
            to_core(zz, 0).wait_recv()

        @pl.when(direct & (zz != z))
        def _():
            to_side(zz).start()
            to_core(zz, 0).start()

        absorb(zz, 0)
        to_core(zz, 1).wait_recv()

        @pl.when(direct)
        def _():
            to_core(zz, 1).start()

        absorb(zz, 1)

    def step(n, carry):
        take(jnp.where(n == 0, order[0], jnp.where(n == 1, order[1], jnp.where(n == 2, order[2], order[3]))))
        return carry

    lax.fori_loop(0, length, step, 0)

    share = rows // n_tp
    lam_copy.wait()
    lam = jnp.where(home, lam_mine[0:1, 0:1], lam_far[0:1, 0:1])
    head = y * length + z
    columns = pl.ds(pl.multiple_of(head * vd, vd), vd)

    def piece(g, t):
        to = (mt + t) % n_tp
        span = pl.ds(pl.multiple_of(to * share, share), share)
        return remote(
            stage.at[g, span],
            out_ref.at[:, columns],
            head_send.at[g, t],
            head_recv.at[head],
            spot(pair * c + g),
            to,
        )

    def own(g):
        return z == pair * c + g

    for g in (1, 0):
        reads = []
        for which in range(2):
            at = slice((2 * g + which) * rows, (2 * g + which + 1) * rows)
            reads.append(acc_ref[:, at] / l_ref[:, at])
        combined = reads[0] - lam * reads[1]
        combined = combined * lax.rsqrt(
            jnp.mean(combined * combined, axis=0, keepdims=True) + norm_epsilon
        )
        stage[g] = (combined.T * gain_ref[...]).astype(jnp.bfloat16)
        for t in range(1, n_tp):
            piece(g, t).start()

        @pl.when(own(g))
        def _():
            out_ref[:, columns] = stage[g, pl.ds(pl.multiple_of(mt * share, share), share), :]

        @pl.when(jnp.logical_not(own(g)))
        def _():
            piece(g, 0).start()

    def head_copy(hd):
        at = pl.ds(pl.multiple_of(hd * vd, vd), vd)
        return remote(
            stage.at[0, 0:share], out_ref.at[:, at], head_send.at[0, 0], head_recv.at[hd], me, mt
        )

    for hd in range(2 * n_tp):

        @pl.when((hd != head) | jnp.logical_not(home))
        def _():
            head_copy(hd).wait_recv()

    for g in range(2):
        for t in range(1, n_tp):
            piece(g, t).wait_send()

        @pl.when(jnp.logical_not(own(g)))
        def _():
            piece(g, 0).wait_send()

        @pl.when(away(g))
        def _():
            first_q(g).wait_send()
            first_kv(g).wait_send()

    for zz in range(length):

        @pl.when(c == zz // pair)
        def _():
            to_side(zz).wait_send()
            to_core(zz, 0).wait_send()
            to_core(zz, 1).wait_send()


def layered(n_sp, n_tp, k1, k2, v, q1, q2, lam, gain):
    rows = q1.shape[0]
    length = n_sp // 2
    vd = v.shape[1] // 2
    keys = q1.shape[1]
    cols = keys + vd
    vmem = pl.BlockSpec(memory_space=pltpu.VMEM)
    dma = pltpu.SemaphoreType.DMA
    return pl.pallas_call(
        functools.partial(layered_kernel, n_sp, n_tp, vd),
        out_shape=jax.ShapeDtypeStruct((rows // n_tp, n_tp * 2 * vd), jnp.bfloat16),
        in_specs=[vmem] * 5 + [pl.BlockSpec(memory_space=pltpu.SMEM), vmem],
        out_specs=vmem,
        scratch_shapes=[
            pltpu.VMEM((2, rows, cols), jnp.bfloat16),
            pltpu.VMEM((2, rows, keys), jnp.bfloat16),
            pltpu.VMEM((length, 2, rows, cols), jnp.bfloat16),
            pltpu.VMEM((2, rows, keys), jnp.bfloat16),
            pltpu.VMEM((keys, 4 * rows), jnp.bfloat16),
            pltpu.VMEM((1, 4 * rows), jnp.float32),
            pltpu.VMEM((1, 4 * rows), jnp.float32),
            pltpu.VMEM((vd, 4 * rows), jnp.float32),
            pltpu.VMEM((2, rows, vd), jnp.bfloat16),
            pltpu.VMEM((8, 128), jnp.float32),
            pltpu.VMEM((8, 128), jnp.float32),
            dma((2, 2)),
            dma((length, 2)),
            dma((length,)),
            dma((length, 2)),
            dma((2,)),
            dma((2,)),
            dma((2, n_tp)),
            dma((2 * n_tp,)),
        ],
        compiler_params=pltpu.CompilerParams(
            collective_id=4, has_side_effects=True, vmem_limit_bytes=VMEM_LIMIT
        ),
    )(k1, k2, v, q1, q2, lam, gain)


def layers_fit(n_sp, n_tp, rows, vd, keys, heads):
    square = heads == 2 and n_sp == 8 and pair_of(n_tp) == 2
    return square and rows % (2 * vd) == 0 and rows // vd * vd == rows and vd == keys


def tp_peers(n_tp):
    inner = pair_of(n_tp)
    mt = lax.axis_index("tp")
    o, c = mt // inner, mt % inner
    across = [((o + d) % (n_tp // inner)) * inner + c for d in range(1, n_tp // inner)]
    return inner, across, o * inner + (inner - 1 - c)


def greet_all(n_sp, n_tp):
    me, mt = lax.axis_index("sp"), lax.axis_index("tp")
    inner, across, partner = tp_peers(n_tp)
    peers = [{"sp": (me + s) % n_sp, "tp": mt} for s in range(1, n_sp)]
    peers += [{"sp": me, "tp": t} for t in across]
    if inner == 2:
        peers.append({"sp": me, "tp": partner})
    greet(peers)


def dispatch_kernel(
    n_sp, n_tp, rows_ref, out_ref, sp_send, sp_recv, y_send, y_recv, c_send, c_recv, own_sem
):
    me, mt = lax.axis_index("sp"), lax.axis_index("tp")
    inner, across, partner = tp_peers(n_tp)
    groups = n_tp // inner
    o = mt // inner
    greet_all(n_sp, n_tp)

    def sp_copy(d):
        to = (me + d) % n_sp
        return pltpu.make_async_remote_copy(
            src_ref=rows_ref.at[to],
            dst_ref=out_ref.at[:, mt, me],
            send_sem=sp_send.at[d],
            recv_sem=sp_recv.at[d],
            device_id={"sp": to, "tp": mt},
            device_id_type=MESH,
        )

    def tp_copy(t, s, to, send, recv):
        return pltpu.make_async_remote_copy(
            src_ref=out_ref.at[:, t, s],
            dst_ref=out_ref.at[:, t, s],
            send_sem=send,
            recv_sem=recv,
            device_id={"sp": me, "tp": to},
            device_id_type=MESH,
        )

    order = sorted(range(1, n_sp), key=lambda d: min(d, n_sp - d))
    for d in reversed(order):
        sp_copy(d).start()
    own = pltpu.make_async_copy(rows_ref.at[me], out_ref.at[:, mt, me], own_sem)
    own.start()
    own.wait()
    started = []

    def spread(d):
        s = (me - d + n_sp) % n_sp
        for g in range(1, groups):
            copy = tp_copy(mt, s, across[g - 1], y_send.at[g, d], y_recv.at[g, d])
            copy.start()
            started.append(copy)
        if inner == 2:
            copy = tp_copy(mt, s, partner, c_send.at[0, d], c_recv.at[0, d])
            copy.start()
            started.append(copy)

    def relay(d):
        s = (me - d + n_sp) % n_sp
        for g in range(1, groups):
            source = ((o - g + groups) % groups) * inner + mt % inner
            tp_copy(source, s, partner, y_send.at[g, d], y_recv.at[g, d]).wait_recv()
            if inner == 2:
                copy = tp_copy(source, s, partner, c_send.at[g, d], c_recv.at[g, d])
                copy.start()
                started.append(copy)

    order = order[::-1]
    sequence = [0] + order
    spread(0)
    for i, d in enumerate(order):
        sp_copy(d).wait_recv()
        spread(d)
        relay(sequence[i])
    relay(sequence[-1])
    for d in range(n_sp):
        s = (me - d + n_sp) % n_sp
        if inner == 2:
            for g in range(groups):
                source = ((o - g + groups) % groups) * inner + (1 - mt % inner)
                tp_copy(source, s, partner, c_send.at[g, d], c_recv.at[g, d]).wait_recv()
    for copy in started:
        copy.wait_send()
    for d in order:
        sp_copy(d).wait_send()


def dispatch(n_sp, n_tp, rows):
    _, experts, cap, width = rows.shape
    groups = n_tp // pair_of(n_tp)
    sem = pltpu.SemaphoreType.DMA
    hbm = pl.BlockSpec(memory_space=pltpu.VMEM)
    return pl.pallas_call(
        functools.partial(dispatch_kernel, n_sp, n_tp),
        out_shape=jax.ShapeDtypeStruct((experts, n_tp, n_sp, cap, width), rows.dtype),
        in_specs=[hbm],
        out_specs=pl.BlockSpec(memory_space=pl.ANY),
        scratch_shapes=[
            sem((n_sp,)),
            sem((n_sp,)),
            sem((groups, n_sp)),
            sem((groups, n_sp)),
            sem((groups, n_sp)),
            sem((groups, n_sp)),
            sem,
        ],
        compiler_params=pltpu.CompilerParams(
            collective_id=1, has_side_effects=True, vmem_limit_bytes=VMEM_LIMIT
        ),
    )(rows)


def collect_kernel(
    n_sp,
    n_tp,
    part_ref,
    out_ref,
    from_core,
    from_across,
    summed,
    total,
    c_send,
    c_recv,
    y_send,
    y_recv,
    sp_send,
    sp_recv,
):
    me, mt = lax.axis_index("sp"), lax.axis_index("tp")
    inner, across, partner = tp_peers(n_tp)
    groups = n_tp // inner
    o, c = mt // inner, mt % inner
    greet_all(n_sp, n_tp)
    order = sorted(range(1, n_sp), key=lambda d: min(d, n_sp - d), reverse=True) + [0]

    def to_of(d):
        return (me + d) % n_sp

    def core_copy(d, g):
        row = ((o + g) % groups) * inner + (inner - 1 - c)
        return pltpu.make_async_remote_copy(
            src_ref=part_ref.at[:, row, to_of(d)],
            dst_ref=from_core.at[d, g],
            send_sem=c_send.at[d, g],
            recv_sem=c_recv.at[d, g],
            device_id={"sp": me, "tp": partner},
            device_id_type=MESH,
        )

    def across_copy(d, g):
        return pltpu.make_async_remote_copy(
            src_ref=summed.at[d, g],
            dst_ref=from_across.at[d, g],
            send_sem=y_send.at[d, g],
            recv_sem=y_recv.at[d, g],
            device_id={"sp": me, "tp": across[g - 1]},
            device_id_type=MESH,
        )

    def sp_copy(d):
        return pltpu.make_async_remote_copy(
            src_ref=total.at[d],
            dst_ref=out_ref.at[me],
            send_sem=sp_send.at[d],
            recv_sem=sp_recv.at[d],
            device_id={"sp": to_of(d), "tp": mt},
            device_id_type=MESH,
        )

    if inner == 2:
        for d in order:
            for g in list(range(1, groups)) + [0]:
                core_copy(d, g).start()

    def pair_sum(d, g):
        row = ((o + g) % groups) * inner + c
        value = part_ref[:, row, to_of(d)].astype(jnp.float32)
        if inner == 2:
            core_copy(d, g).wait_recv()
            value = value + from_core[d, g].astype(jnp.float32)
        return value

    def first(d):
        for g in range(1, groups):
            summed[d, g] = pair_sum(d, g).astype(summed.dtype)
            across_copy(d, g).start()

    def second(d):
        value = pair_sum(d, 0)
        for g in range(1, groups):
            across_copy(d, g).wait_recv()
            value = value + from_across[d, g].astype(jnp.float32)
        value = value.astype(total.dtype)
        if d == 0:
            out_ref[me] = value
        else:
            total[d] = value
            sp_copy(d).start()

    ahead = min(3, n_sp)
    for d in order[:ahead]:
        first(d)
    for i, d in enumerate(order):
        second(d)
        if i + ahead < n_sp:
            first(order[i + ahead])
    for d in range(1, n_sp):
        sp_copy(d).wait_recv()
    for d in range(n_sp):
        if d:
            sp_copy(d).wait_send()
        for g in range(groups):
            if g:
                across_copy(d, g).wait_send()
            if inner == 2:
                core_copy(d, g).wait_send()


def collect(n_sp, n_tp, part):
    experts, _, _, cap, width = part.shape
    groups = n_tp // pair_of(n_tp)
    sem = pltpu.SemaphoreType.DMA
    vmem = pl.BlockSpec(memory_space=pltpu.VMEM)
    piece = (experts, cap, width)
    return pl.pallas_call(
        functools.partial(collect_kernel, n_sp, n_tp),
        out_shape=jax.ShapeDtypeStruct((n_sp,) + piece, part.dtype),
        in_specs=[vmem],
        out_specs=vmem,
        scratch_shapes=[
            pltpu.VMEM((n_sp, groups) + piece, part.dtype),
            pltpu.VMEM((n_sp, groups) + piece, part.dtype),
            pltpu.VMEM((n_sp, groups) + piece, part.dtype),
            pltpu.VMEM((n_sp,) + piece, part.dtype),
            sem((n_sp, groups)),
            sem((n_sp, groups)),
            sem((n_sp, groups)),
            sem((n_sp, groups)),
            sem((n_sp,)),
            sem((n_sp,)),
        ],
        compiler_params=pltpu.CompilerParams(
            collective_id=2, has_side_effects=True, vmem_limit_bytes=VMEM_LIMIT
        ),
    )(part)


def experts_kernel(
    n_sp,
    n_tp,
    rows_ref,
    gate_hbm,
    up_hbm,
    down_hbm,
    out_ref,
    held,
    part,
    from_core,
    from_across,
    summed,
    total,
    gate_w,
    up_w,
    down_w,
    w_sem,
    own_sem,
    sp_send,
    sp_recv,
    y_send,
    y_recv,
    c_send,
    c_recv,
    rc_send,
    rc_recv,
    ry_send,
    ry_recv,
    rs_send,
    rs_recv,
):
    me, mt = lax.axis_index("sp"), lax.axis_index("tp")
    inner_sp = pair_of(n_sp)
    length = n_sp // inner_sp
    z, x = me // inner_sp, me % inner_sp
    inner, across, partner = tp_peers(n_tp)
    groups = n_tp // inner
    o, c = mt // inner, mt % inner
    experts, cap = rows_ref.shape[1], rows_ref.shape[2]
    weights = [
        pltpu.make_async_copy(src, dst, w_sem.at[k])
        for k, (src, dst) in enumerate(((gate_hbm, gate_w), (up_hbm, up_w), (down_hbm, down_w)))
    ]
    for copy in weights:
        copy.start()
    greet_all(n_sp, n_tp)

    def side(i):
        return (x + i % inner_sp) % inner_sp

    def to_of(i):
        return ((z + i // inner_sp) % length) * inner_sp + side(i)

    def from_of(i):
        return ((z + length - i // inner_sp) % length) * inner_sp + side(i)

    def span(t):
        return pl.ds(pl.multiple_of(t * cap, cap), cap)

    def remote(src, dst, send, recv, sp, tp):
        return pltpu.make_async_remote_copy(
            src_ref=src,
            dst_ref=dst,
            send_sem=send,
            recv_sem=recv,
            device_id={"sp": sp, "tp": tp},
            device_id_type=MESH,
        )

    def sp_copy(i):
        block = held.at[i, :, span(mt)]
        return remote(rows_ref.at[to_of(i)], block, sp_send.at[i], sp_recv.at[i], to_of(i), mt)

    def across_in(i, g, t):
        block = held.at[i, :, span(t)]
        return remote(block, block, y_send.at[g, i], y_recv.at[g, i], me, across[g - 1])

    def core_in(i, g, t):
        block = held.at[i, :, span(t)]
        return remote(block, block, c_send.at[g, i], c_recv.at[g, i], me, partner)

    def core_out(i, g):
        row = ((o + g) % groups) * inner + (inner - 1 - c)
        block = part.at[i, :, span(row)]
        return remote(
            block, from_core.at[i, g], rc_send.at[i, g], rc_recv.at[i, g], me, partner
        )

    def across_out(i, g):
        return remote(
            summed.at[i, g],
            from_across.at[i, g],
            ry_send.at[i, g],
            ry_recv.at[i, g],
            me,
            across[g - 1],
        )

    def sp_out(i):
        to = from_of(i)
        return remote(total.at[i], out_ref.at[me], rs_send.at[i], rs_recv.at[i], to, mt)

    def source(g):
        return ((o - g + groups) % groups) * inner + c

    for i in range(1, n_sp):
        sp_copy(i).start()
    own = pltpu.make_async_copy(rows_ref.at[me], held.at[0, :, span(mt)], own_sem)
    own.start()
    own.wait()

    def spread(i):
        @pl.when(i > 0)
        def _():
            sp_copy(i).wait_recv()

        for g in range(1, groups):
            across_in(i, g, mt).start()
        if inner == 2:
            core_in(i, 0, mt).start()

    def relay(i):
        for g in range(1, groups):
            across_in(i, g, source(g)).wait_recv()
            if inner == 2:
                core_in(i, g, source(g)).start()

    def compute(i):
        @pl.when(i == late)
        def _():
            for copy in weights:
                copy.wait()

        if inner == 2:
            for g in range(groups):
                core_in(i, g, source(g)).wait_recv()
        for e in range(experts):
            rows = held[i, e]
            gate = jnp.dot(rows, gate_w[e], preferred_element_type=jnp.float32)
            upper = jnp.dot(rows, up_w[e], preferred_element_type=jnp.float32)
            middle = (gate / (1.0 + jnp.exp(-gate)) * upper).astype(jnp.bfloat16)
            part[i, e] = jnp.dot(middle, down_w[e], preferred_element_type=jnp.float32).astype(
                part.dtype
            )
        if inner == 2:
            for g in list(range(1, groups)) + [0]:
                core_out(i, g).start()

    def pair_sum(i, g):
        row = ((o + g) % groups) * inner + c
        value = part[i, :, span(row), :].astype(jnp.float32)
        if inner == 2:
            core_out(i, g).wait_recv()
            value = value + from_core[i, g].astype(jnp.float32)
        return value

    def first(i):
        for g in range(1, groups):
            summed[i, g] = pair_sum(i, g).astype(summed.dtype)
            across_out(i, g).start()

    def second(i):
        value = pair_sum(i, 0)
        for g in range(1, groups):
            across_out(i, g).wait_recv()
            value = value + from_across[i, g].astype(jnp.float32)
        value = value.astype(total.dtype)

        @pl.when(i == 0)
        def _():
            out_ref[me] = value

        @pl.when(i > 0)
        def _():
            total[i] = value
            sp_out(i).start()

    late = inner_sp if length > 1 else 0

    def turned(stage):
        return lambda k: stage(jnp.where(k < n_sp - late, k + late, n_sp - 1 - k))

    stages = (spread, relay) + tuple(turned(stage) for stage in (compute, first, second))
    lags = (0, 1, 2 + late, 3 + late, 5 + late)

    def step(i, carry):
        for stage, lag in zip(stages, lags):

            @pl.when((i >= lag) & (i < n_sp + lag))
            def _():
                stage(i - lag)

        return carry

    lax.fori_loop(0, n_sp + lags[-1], step, 0)

    def drain(i, carry):
        @pl.when(i > 0)
        def _():
            sp_out(i).wait_recv()
            sp_out(i).wait_send()
            sp_copy(i).wait_send()

        for g in range(groups):
            if g:
                across_in(i, g, mt).wait_send()
                across_out(i, g).wait_send()
            if inner == 2:
                core_in(i, g, mt).wait_send()
                core_out(i, g).wait_send()
        return carry

    lax.fori_loop(0, n_sp, drain, 0)


def run_experts(n_sp, n_tp, rows, gate_weight, up_weight, down_weight):
    _, experts, cap, width = rows.shape
    groups = n_tp // pair_of(n_tp)
    dma = pltpu.SemaphoreType.DMA
    vmem = pl.BlockSpec(memory_space=pltpu.VMEM)
    hbm = pl.BlockSpec(memory_space=pl.ANY)
    piece = (experts, cap, width)
    return pl.pallas_call(
        functools.partial(experts_kernel, n_sp, n_tp),
        out_shape=jax.ShapeDtypeStruct(rows.shape, rows.dtype),
        in_specs=[vmem, hbm, hbm, hbm],
        out_specs=vmem,
        scratch_shapes=[
            pltpu.VMEM((n_sp, experts, n_tp * cap, width), rows.dtype),
            pltpu.VMEM((n_sp, experts, n_tp * cap, width), rows.dtype),
            pltpu.VMEM((n_sp, groups) + piece, rows.dtype),
            pltpu.VMEM((n_sp, groups) + piece, rows.dtype),
            pltpu.VMEM((n_sp, groups) + piece, rows.dtype),
            pltpu.VMEM((n_sp,) + piece, rows.dtype),
            pltpu.VMEM(gate_weight.shape, gate_weight.dtype),
            pltpu.VMEM(up_weight.shape, up_weight.dtype),
            pltpu.VMEM(down_weight.shape, down_weight.dtype),
            dma((3,)),
            dma,
            dma((n_sp,)),
            dma((n_sp,)),
            dma((groups, n_sp)),
            dma((groups, n_sp)),
            dma((groups, n_sp)),
            dma((groups, n_sp)),
            dma((n_sp, groups)),
            dma((n_sp, groups)),
            dma((n_sp, groups)),
            dma((n_sp, groups)),
            dma((n_sp,)),
            dma((n_sp,)),
        ],
        compiler_params=pltpu.CompilerParams(
            collective_id=3, has_side_effects=True, vmem_limit_bytes=VMEM_LIMIT
        ),
    )(rows, gate_weight, up_weight, down_weight)


def on_device(
    n_sp,
    n_tp,
    query_one,
    key_one,
    query_two,
    key_two,
    values,
    mix_lambda,
    head_gain,
    residual_in,
    out_weight,
    norm_gain,
    route_ids,
    route_logits,
    group_prob,
    gate_weight,
    up_weight,
    down_weight,
):
    fits = layers_fit(
        n_sp,
        n_tp,
        query_one.shape[0],
        values.shape[1] // 2,
        query_one.shape[1],
        mix_lambda.shape[0],
    )
    token_heads = (layered if fits else attend)(
        n_sp,
        n_tp,
        key_one,
        key_two,
        values,
        query_one,
        query_two,
        mix_lambda,
        head_gain[None, :],
    )
    share = residual_in.shape[0]
    mix = jnp.dot(token_heads, out_weight, preferred_element_type=jnp.float32)
    hidden_f = (residual_in.astype(jnp.float32) + mix).astype(jnp.bfloat16).astype(jnp.float32)
    normed = (
        hidden_f
        * lax.rsqrt(jnp.mean(hidden_f * hidden_f, axis=-1, keepdims=True) + norm_epsilon)
        * norm_gain
    ).astype(jnp.bfloat16)
    width = normed.shape[1]
    top_count = route_ids.shape[1]
    local_experts = gate_weight.shape[0]
    expert_count = local_experts * n_sp
    capacity = max(2, 2 * share * top_count // expert_count)
    slots = expert_count * capacity
    flat_ids = route_ids.reshape(-1)
    one_hot = (flat_ids[:, None] == jnp.arange(expert_count, dtype=jnp.int32)[None, :]).astype(
        jnp.int32
    )
    earlier = jnp.cumsum(one_hot, axis=0) - one_hot
    rank = jnp.sum(earlier * one_hot, axis=1)
    slot_of = (flat_ids * capacity + rank).reshape(share, top_count)
    places = jnp.arange(slots, dtype=jnp.int32)
    table = sum(
        (places[:, None] == slot_of[None, :, k]).astype(jnp.bfloat16) for k in range(top_count)
    )
    outgoing = jnp.dot(table, normed, preferred_element_type=jnp.float32).astype(jnp.bfloat16)
    outgoing = outgoing.reshape(n_sp, local_experts, capacity, width)
    if capacity % 16 == 0:
        returned = run_experts(
            n_sp, n_tp, outgoing, gate_weight, up_weight, down_weight
        ).reshape(slots, width)
    else:
        everyone = dispatch(
            n_sp, n_tp, outgoing
        ).reshape(local_experts, n_tp * n_sp * capacity, width)
        gate = jnp.einsum("erd,edf->erf", everyone, gate_weight, preferred_element_type=jnp.float32)
        upper = jnp.einsum("erd,edf->erf", everyone, up_weight, preferred_element_type=jnp.float32)
        middle = (jax.nn.silu(gate) * upper).astype(jnp.bfloat16)
        part_sum = jnp.einsum(
            "erf,efd->erd", middle, down_weight, preferred_element_type=jnp.float32
        ).astype(jnp.bfloat16)
        returned = collect(
            n_sp, n_tp, part_sum.reshape(local_experts, n_tp, n_sp, capacity, width)
        ).reshape(slots, width)
    logits = [route_logits[:, k : k + 1] for k in range(top_count)]
    highest = functools.reduce(jnp.maximum, logits)
    powers = [jnp.exp(logit - highest) for logit in logits]
    route_weight = [power / sum(powers) * group_prob[:, None] for power in powers]
    spread = sum(
        jnp.where(places[None, :] == slot_of[:, k, None], route_weight[k], 0.0)
        for k in range(top_count)
    )
    high = spread.astype(jnp.bfloat16)
    low = (spread - high.astype(jnp.float32)).astype(jnp.bfloat16)
    both = jnp.dot(
        jnp.concatenate([high, low], axis=0), returned, preferred_element_type=jnp.float32
    )
    return (hidden_f + (both[:share] + both[share:])).astype(jnp.bfloat16)


def solution(mesh):
    in_specs = (
        P("sp", "tp"),
        P("sp", "tp"),
        P("sp", "tp"),
        P("sp", "tp"),
        P("sp", "tp"),
        P("tp"),
        P(),
        P(("sp", "tp"), None),
        P(),
        P(),
        P(("sp", "tp"), None),
        P(("sp", "tp"), None),
        P(("sp", "tp")),
        P("sp", None, "tp"),
        P("sp", None, "tp"),
        P("sp", "tp", None),
    )
    out_specs = P(("sp", "tp"), None)
    return jax.shard_map(
        functools.partial(on_device, mesh.shape["sp"], mesh.shape["tp"]),
        mesh=mesh,
        in_specs=in_specs,
        out_specs=out_specs,
        check_vma=False,
    )
```

```python
import functools
import math
import types

import jax
import jax.numpy as jnp
from jax import lax
from jax.experimental import pallas as pl
from jax.experimental.pallas import tpu as pltpu
from jax.sharding import PartitionSpec as P

norm_epsilon = 1e-06
MESH = pl.DeviceIdType.MESH
VMEM_LIMIT = 60 * 1024 * 1024


def pair_of(count):
    return 2 if count % 2 == 0 else 1


def greet(peers):
    barrier = pltpu.get_barrier_semaphore()
    for peer in peers:
        pl.semaphore_signal(barrier, inc=1, device_id=peer, device_id_type=MESH)
    pl.semaphore_wait(barrier, len(peers))


def attend_kernel(
    n_sp,
    n_tp,
    vd,
    k1_ref,
    k2_ref,
    v_ref,
    q1_ref,
    q2_ref,
    lam_ref,
    gain_ref,
    out_ref,
    kvp,
    qp,
    held,
    q_far,
    m_ref,
    l_ref,
    acc_ref,
    stage,
    cross_send,
    cross_recv,
    line_send,
    line_recv,
    side_send,
    side_recv,
    head_send,
    head_recv,
):
    inner = pair_of(n_sp)
    length = n_sp // inner
    half = length // 2
    me = lax.axis_index("sp")
    mt = lax.axis_index("tp")
    z, x = me // inner, me % inner
    head, zi = z // half, z % half
    rows = q1_ref.shape[0]
    qk = q1_ref.shape[1] // 2
    scale = 1.0 / math.sqrt(qk)
    exact = math.frexp(scale)[0] == 0.5
    early, after = (scale, 1.0) if exact else (1.0, scale)
    other = z * inner + (inner - 1 - x)
    mirror = (length - 1 - z) * inner + x
    far_zi = half - 1 - zi
    for h in range(2):
        kvp[h, :, 0:qk] = k1_ref[:, h * qk : (h + 1) * qk]
        kvp[h, :, qk : 2 * qk] = k2_ref[:, h * qk : (h + 1) * qk]
        kvp[h, :, 2 * qk : 2 * qk + vd] = v_ref[:, h * vd : (h + 1) * vd]
        qp[h, :, 0:qk] = q1_ref[:, h * qk : (h + 1) * qk] * jnp.bfloat16(early)
        qp[h, :, qk : 2 * qk] = q2_ref[:, h * qk : (h + 1) * qk] * jnp.bfloat16(early)

    def line_device(zz):
        return (head * half + zz) * inner + x

    peers = [{"sp": me, "tp": (mt + t) % n_tp} for t in range(1, n_tp)]
    peers += [{"sp": mirror, "tp": (mt + t) % n_tp} for t in range(n_tp)]
    if inner == 2:
        peers.append({"sp": other, "tp": mt})
    if half > 1:
        for shift in sorted({1, half - 1}):
            peers.append({"sp": line_device((zi + shift) % half), "tp": mt})
    greet(peers)

    def remote(src, dst, send, recv, sp):
        return pltpu.make_async_remote_copy(
            src_ref=src,
            dst_ref=dst,
            send_sem=send,
            recv_sem=recv,
            device_id={"sp": sp, "tp": mt},
            device_id_type=MESH,
        )

    cross_q = remote(qp.at[1 - head], q_far, cross_send.at[0], cross_recv.at[0], mirror)
    cross_kv = remote(
        kvp.at[1 - head], held.at[1, far_zi, x], cross_send.at[1], cross_recv.at[1], mirror
    )

    def line_copy(j, src, zz, way):
        ahead = jnp.clip(jnp.where(way == 0, zi + 1, zi - 1), 0, half - 1)
        return remote(
            src,
            held.at[j, zz, x],
            line_send.at[j, way, zz],
            line_recv.at[j, zz],
            line_device(ahead),
        )

    def side_copy(j, src, zz):
        return remote(src, held.at[j, zz, x], side_send.at[j, zz], side_recv.at[j, zz], other)

    def start_from(j, src):
        @pl.when(zi + 1 < half)
        def _():
            line_copy(j, src, zi, 0).start()

        @pl.when(zi > 0)
        def _():
            line_copy(j, src, zi, 1).start()

        if inner == 2:
            side_copy(j, src, zi).start()

    own = kvp.at[head]
    cross_kv.start()
    start_from(0, own)
    cross_q.start()
    m_ref[...] = jnp.full(m_ref.shape, -1e30, jnp.float32)
    l_ref[...] = jnp.zeros(l_ref.shape, jnp.float32)
    acc_ref[...] = jnp.zeros(acc_ref.shape, jnp.float32)

    def absorb(block, q_ref, group):
        vals = block[:, 2 * qk : 2 * qk + vd]
        for which in range(2):
            at = 2 * group + which
            scores = lax.dot_general(
                q_ref[:, which * qk : (which + 1) * qk],
                block[:, which * qk : (which + 1) * qk],
                (((1,), (1,)), ((), ())),
                preferred_element_type=jnp.float32,
            )
            if after != 1.0:
                scores = scores * after
            old = m_ref[at]
            new = jnp.maximum(old, jnp.max(scores, axis=1, keepdims=True))
            shrink = jnp.exp(old - new)
            expo = jnp.exp(scores - new[:, :1])
            m_ref[at] = new
            l_ref[at] = l_ref[at] * shrink + jnp.sum(expo, axis=1, keepdims=True)
            acc_ref[at] = acc_ref[at] * shrink[:, :1] + jnp.dot(
                expo.astype(jnp.bfloat16), vals, preferred_element_type=jnp.float32
            )

    q_own = qp.at[head]

    def absorb_both(block):
        absorb(block, q_own, 0)
        absorb(block, q_far, 1)

    def place(n):
        dist = (n + 1) // 2
        return jnp.where(n % 2 == 1, zi - dist, zi + dist), 1 - n % 2

    def line_steps(j, take):
        def line_step(n, carry):
            zz, way = place(n)

            @pl.when((zz >= 0) & (zz < half))
            def _():
                block = held.at[j, zz, x]
                line_copy(j, block, zz, way).wait_recv()
                ahead = jnp.where(way == 0, zi + 1, zi - 1)

                @pl.when((ahead >= 0) & (ahead < half))
                def _():
                    line_copy(j, block, zz, way).start()

                if inner == 2:
                    side_copy(j, block, zz).start()
                take(block)

            return carry

        lax.fori_loop(1, 2 * half - 1, line_step, 0)

    def line_again(j):
        def again(n, carry):
            zz, _ = place(n)

            @pl.when((zz >= 0) & (zz < half))
            def _():
                absorb(held.at[j, zz, x], q_far, 1)

            return carry

        lax.fori_loop(1, 2 * half - 1, again, 0)

    def side_steps(j, begin):
        def side_step(n, carry):
            zz, _ = place(n)

            @pl.when((zz >= 0) & (zz < half))
            def _():
                block = held.at[j, zz, 1 - x]
                side_copy(j, block, zz).wait_recv()
                absorb_both(block)

            return carry

        lax.fori_loop(begin, 2 * half - 1, side_step, 0)

    near = held.at[0, zi, 1 - x]
    far = held.at[1, zi, x]
    absorb(own, q_own, 0)
    if inner == 2:
        side_copy(0, near, zi).wait_recv()
        absorb(near, q_own, 0)
    line_steps(0, lambda block: absorb(block, q_own, 0))
    cross_kv.wait_recv()
    start_from(1, far)
    absorb(far, q_own, 0)
    cross_q.wait_recv()
    absorb(own, q_far, 1)
    absorb(far, q_far, 1)
    line_steps(1, absorb_both)
    line_again(0)
    if inner == 2:
        absorb(near, q_far, 1)
        side_steps(0, 1)
        side_steps(1, 0)

    share = rows // n_tp
    lam = lam_ref[head]
    columns = pl.ds(pl.multiple_of((mt * 2 + head) * vd, vd), vd)
    copies = []
    for group, sp in ((1, mirror), (0, me)):
        read_a = acc_ref[2 * group] / l_ref[2 * group][:, :1]
        read_b = acc_ref[2 * group + 1] / l_ref[2 * group + 1][:, :1]
        combined = read_a - lam * read_b
        combined = (
            combined
            * lax.rsqrt(jnp.mean(combined * combined, axis=-1, keepdims=True) + norm_epsilon)
            * gain_ref[...]
        )
        stage[group] = combined.astype(jnp.bfloat16)
        for t in range(n_tp):
            to = (mt + t) % n_tp
            span = pl.ds(pl.multiple_of(to * share, share), share)
            if group == 0 and t == 0:
                out_ref[:, columns] = stage[0, span, :]
                continue
            copy = pltpu.make_async_remote_copy(
                src_ref=stage.at[group, span],
                dst_ref=out_ref.at[:, columns],
                send_sem=head_send.at[group, t],
                recv_sem=head_recv.at[group, t],
                device_id={"sp": sp, "tp": to},
                device_id_type=MESH,
            )
            copy.start()
            copies.append(copy)

    cross_q.wait_send()
    cross_kv.wait_send()
    for j in range(2):

        def drain(n, carry):
            zz, way = place(n)

            @pl.when((zz >= 0) & (zz < half))
            def _():
                ahead = jnp.where(way == 0, zi + 1, zi - 1)

                @pl.when((ahead >= 0) & (ahead < half))
                def _():
                    line_copy(j, own, zz, way).wait_send()

                if inner == 2:
                    side_copy(j, own, zz).wait_send()

            return carry

        lax.fori_loop(1, 2 * half - 1, drain, 0)

        @pl.when(zi + 1 < half)
        def _():
            line_copy(j, own, zi, 0).wait_send()

        @pl.when(zi > 0)
        def _():
            line_copy(j, own, zi, 1).wait_send()

        if inner == 2:
            side_copy(j, own, zi).wait_send()
    for copy in copies:
        copy.wait()


def attend(n_sp, n_tp, k1, k2, v, q1, q2, lam, gain):
    rows = q1.shape[0]
    inner = pair_of(n_sp)
    half = n_sp // inner // 2
    assert lam.shape[0] == 2 and half * inner * 2 == n_sp
    vd = v.shape[1] // 2
    qk = q1.shape[1] // 2
    cols = 2 * qk + vd
    vmem = pl.BlockSpec(memory_space=pltpu.VMEM)
    dma = pltpu.SemaphoreType.DMA
    return pl.pallas_call(
        functools.partial(attend_kernel, n_sp, n_tp, vd),
        out_shape=jax.ShapeDtypeStruct((rows // n_tp, n_tp * 2 * vd), jnp.bfloat16),
        in_specs=[vmem] * 5 + [pl.BlockSpec(memory_space=pltpu.SMEM), vmem],
        out_specs=vmem,
        scratch_shapes=[
            pltpu.VMEM((2, rows, cols), jnp.bfloat16),
            pltpu.VMEM((2, rows, 2 * qk), jnp.bfloat16),
            pltpu.VMEM((2, half, inner, rows, cols), jnp.bfloat16),
            pltpu.VMEM((rows, 2 * qk), jnp.bfloat16),
            pltpu.VMEM((4, rows, 128), jnp.float32),
            pltpu.VMEM((4, rows, 128), jnp.float32),
            pltpu.VMEM((4, rows, vd), jnp.float32),
            pltpu.VMEM((2, rows, vd), jnp.bfloat16),
            dma((2,)),
            dma((2,)),
            dma((2, 2, half)),
            dma((2, half)),
            dma((2, half)),
            dma((2, half)),
            dma((2, n_tp)),
            dma((2, n_tp)),
        ],
        compiler_params=pltpu.CompilerParams(
            collective_id=0, has_side_effects=True, vmem_limit_bytes=VMEM_LIMIT
        ),
    )(k1, k2, v, q1, q2, lam, gain)


def tp_peers(n_tp):
    inner = pair_of(n_tp)
    mt = lax.axis_index("tp")
    o, c = mt // inner, mt % inner
    across = [((o + d) % (n_tp // inner)) * inner + c for d in range(1, n_tp // inner)]
    return inner, across, o * inner + (inner - 1 - c)


def greet_all(n_sp, n_tp):
    me, mt = lax.axis_index("sp"), lax.axis_index("tp")
    inner, across, partner = tp_peers(n_tp)
    peers = [{"sp": (me + s) % n_sp, "tp": mt} for s in range(1, n_sp)]
    peers += [{"sp": me, "tp": t} for t in across]
    if inner == 2:
        peers.append({"sp": me, "tp": partner})
    greet(peers)


def dispatch_kernel(
    n_sp, n_tp, rows_ref, out_ref, sp_send, sp_recv, y_send, y_recv, c_send, c_recv, own_sem
):
    me, mt = lax.axis_index("sp"), lax.axis_index("tp")
    inner, across, partner = tp_peers(n_tp)
    groups = n_tp // inner
    o = mt // inner
    greet_all(n_sp, n_tp)

    def sp_copy(d):
        to = (me + d) % n_sp
        return pltpu.make_async_remote_copy(
            src_ref=rows_ref.at[to],
            dst_ref=out_ref.at[:, mt, me],
            send_sem=sp_send.at[d],
            recv_sem=sp_recv.at[d],
            device_id={"sp": to, "tp": mt},
            device_id_type=MESH,
        )

    def tp_copy(t, s, to, send, recv):
        return pltpu.make_async_remote_copy(
            src_ref=out_ref.at[:, t, s],
            dst_ref=out_ref.at[:, t, s],
            send_sem=send,
            recv_sem=recv,
            device_id={"sp": me, "tp": to},
            device_id_type=MESH,
        )

    order = sorted(range(1, n_sp), key=lambda d: min(d, n_sp - d))
    for d in reversed(order):
        sp_copy(d).start()
    own = pltpu.make_async_copy(rows_ref.at[me], out_ref.at[:, mt, me], own_sem)
    own.start()
    own.wait()
    started = []

    def spread(d):
        s = (me - d + n_sp) % n_sp
        for g in range(1, groups):
            copy = tp_copy(mt, s, across[g - 1], y_send.at[g, d], y_recv.at[g, d])
            copy.start()
            started.append(copy)
        if inner == 2:
            copy = tp_copy(mt, s, partner, c_send.at[0, d], c_recv.at[0, d])
            copy.start()
            started.append(copy)

    def relay(d):
        s = (me - d + n_sp) % n_sp
        for g in range(1, groups):
            source = ((o - g + groups) % groups) * inner + mt % inner
            tp_copy(source, s, partner, y_send.at[g, d], y_recv.at[g, d]).wait_recv()
            if inner == 2:
                copy = tp_copy(source, s, partner, c_send.at[g, d], c_recv.at[g, d])
                copy.start()
                started.append(copy)

    order = order[::-1]
    sequence = [0] + order
    spread(0)
    for i, d in enumerate(order):
        sp_copy(d).wait_recv()
        spread(d)
        relay(sequence[i])
    relay(sequence[-1])
    for d in range(n_sp):
        s = (me - d + n_sp) % n_sp
        if inner == 2:
            for g in range(groups):
                source = ((o - g + groups) % groups) * inner + (1 - mt % inner)
                tp_copy(source, s, partner, c_send.at[g, d], c_recv.at[g, d]).wait_recv()
    for copy in started:
        copy.wait_send()
    for d in order:
        sp_copy(d).wait_send()


def dispatch(n_sp, n_tp, rows):
    _, experts, cap, width = rows.shape
    groups = n_tp // pair_of(n_tp)
    sem = pltpu.SemaphoreType.DMA
    hbm = pl.BlockSpec(memory_space=pltpu.VMEM)
    return pl.pallas_call(
        functools.partial(dispatch_kernel, n_sp, n_tp),
        out_shape=jax.ShapeDtypeStruct((experts, n_tp, n_sp, cap, width), rows.dtype),
        in_specs=[hbm],
        out_specs=pl.BlockSpec(memory_space=pl.ANY),
        scratch_shapes=[
            sem((n_sp,)),
            sem((n_sp,)),
            sem((groups, n_sp)),
            sem((groups, n_sp)),
            sem((groups, n_sp)),
            sem((groups, n_sp)),
            sem,
        ],
        compiler_params=pltpu.CompilerParams(
            collective_id=1, has_side_effects=True, vmem_limit_bytes=VMEM_LIMIT
        ),
    )(rows)


def collect_kernel(
    n_sp,
    n_tp,
    part_ref,
    out_ref,
    from_core,
    from_across,
    summed,
    total,
    c_send,
    c_recv,
    y_send,
    y_recv,
    sp_send,
    sp_recv,
):
    me, mt = lax.axis_index("sp"), lax.axis_index("tp")
    inner, across, partner = tp_peers(n_tp)
    groups = n_tp // inner
    o, c = mt // inner, mt % inner
    greet_all(n_sp, n_tp)
    order = sorted(range(1, n_sp), key=lambda d: min(d, n_sp - d), reverse=True) + [0]

    def to_of(d):
        return (me + d) % n_sp

    def core_copy(d, g):
        row = ((o + g) % groups) * inner + (inner - 1 - c)
        return pltpu.make_async_remote_copy(
            src_ref=part_ref.at[:, row, to_of(d)],
            dst_ref=from_core.at[d, g],
            send_sem=c_send.at[d, g],
            recv_sem=c_recv.at[d, g],
            device_id={"sp": me, "tp": partner},
            device_id_type=MESH,
        )

    def across_copy(d, g):
        return pltpu.make_async_remote_copy(
            src_ref=summed.at[d, g],
            dst_ref=from_across.at[d, g],
            send_sem=y_send.at[d, g],
            recv_sem=y_recv.at[d, g],
            device_id={"sp": me, "tp": across[g - 1]},
            device_id_type=MESH,
        )

    def sp_copy(d):
        return pltpu.make_async_remote_copy(
            src_ref=total.at[d],
            dst_ref=out_ref.at[me],
            send_sem=sp_send.at[d],
            recv_sem=sp_recv.at[d],
            device_id={"sp": to_of(d), "tp": mt},
            device_id_type=MESH,
        )

    if inner == 2:
        for d in order:
            for g in list(range(1, groups)) + [0]:
                core_copy(d, g).start()

    def pair_sum(d, g):
        row = ((o + g) % groups) * inner + c
        value = part_ref[:, row, to_of(d)].astype(jnp.float32)
        if inner == 2:
            core_copy(d, g).wait_recv()
            value = value + from_core[d, g].astype(jnp.float32)
        return value

    def first(d):
        for g in range(1, groups):
            summed[d, g] = pair_sum(d, g).astype(summed.dtype)
            across_copy(d, g).start()

    def second(d):
        value = pair_sum(d, 0)
        for g in range(1, groups):
            across_copy(d, g).wait_recv()
            value = value + from_across[d, g].astype(jnp.float32)
        value = value.astype(total.dtype)
        if d == 0:
            out_ref[me] = value
        else:
            total[d] = value
            sp_copy(d).start()

    ahead = min(3, n_sp)
    for d in order[:ahead]:
        first(d)
    for i, d in enumerate(order):
        second(d)
        if i + ahead < n_sp:
            first(order[i + ahead])
    for d in range(1, n_sp):
        sp_copy(d).wait_recv()
    for d in range(n_sp):
        if d:
            sp_copy(d).wait_send()
        for g in range(groups):
            if g:
                across_copy(d, g).wait_send()
            if inner == 2:
                core_copy(d, g).wait_send()


def collect(n_sp, n_tp, part):
    experts, _, _, cap, width = part.shape
    groups = n_tp // pair_of(n_tp)
    sem = pltpu.SemaphoreType.DMA
    vmem = pl.BlockSpec(memory_space=pltpu.VMEM)
    piece = (experts, cap, width)
    return pl.pallas_call(
        functools.partial(collect_kernel, n_sp, n_tp),
        out_shape=jax.ShapeDtypeStruct((n_sp,) + piece, part.dtype),
        in_specs=[vmem],
        out_specs=vmem,
        scratch_shapes=[
            pltpu.VMEM((n_sp, groups) + piece, part.dtype),
            pltpu.VMEM((n_sp, groups) + piece, part.dtype),
            pltpu.VMEM((n_sp, groups) + piece, part.dtype),
            pltpu.VMEM((n_sp,) + piece, part.dtype),
            sem((n_sp, groups)),
            sem((n_sp, groups)),
            sem((n_sp, groups)),
            sem((n_sp, groups)),
            sem((n_sp,)),
            sem((n_sp,)),
        ],
        compiler_params=pltpu.CompilerParams(
            collective_id=2, has_side_effects=True, vmem_limit_bytes=VMEM_LIMIT
        ),
    )(part)


def attention_phase(n_sp, n_tp, r, arrived, filler):
    inner, pair = 2, 2
    length = n_sp // inner
    me, mt = lax.axis_index("sp"), lax.axis_index("tp")
    z, x = me // inner, me % inner
    y, c = mt // pair, mt % pair
    rows, qk = r.q1_ref.shape[0], r.q1_ref.shape[1] // 2
    vd = r.v_ref.shape[1] // 2
    keys = 2 * qk
    scale = 1.0 / math.sqrt(qk)
    exact = math.frexp(scale)[0] == 0.5
    early, after = (scale, 1.0) if exact else (1.0, scale)
    home = c == z // pair
    partner = y * pair + (1 - c)
    across = z * inner + (1 - x)

    def spot(zz):
        return zz * inner + x

    for h in range(2):
        at = slice(h * qk, (h + 1) * qk)
        block = jnp.concatenate([r.k1_ref[:, at], r.k2_ref[:, at]], axis=1)
        turned = jnp.concatenate(
            [
                r.v_ref[base : base + vd, h * vd : (h + 1) * vd].astype(jnp.float32).T
                for base in range(0, rows, vd)
            ],
            axis=0,
        ).astype(jnp.bfloat16)
        query = jnp.concatenate([r.q1_ref[:, at], r.q2_ref[:, at]], axis=1) * jnp.bfloat16(early)
        r.kv_out[h, :, 0:keys] = block
        r.kv_out[h, :, keys : keys + vd] = turned
        r.q_out[h] = query

        @pl.when(z == pair * c + h)
        def _():
            r.held[z, 0, :, 0:keys] = block
            r.held[z, 0, :, keys : keys + vd] = turned
            r.q_in[h] = query

    r.lam_mine[...] = jnp.full(r.lam_mine.shape, r.lam_ref[z % pair], jnp.float32)
    r.m_ref[...] = jnp.full(r.m_ref.shape, -1e30, jnp.float32)
    r.l_ref[...] = jnp.zeros(r.l_ref.shape, jnp.float32)
    r.acc_ref[...] = jnp.zeros(r.acc_ref.shape, jnp.float32)
    r.qt[...] = jnp.zeros(r.qt.shape, r.qt.dtype)
    arrived()

    def remote(src, dst, send, recv, sp, tp):
        return pltpu.make_async_remote_copy(
            src_ref=src,
            dst_ref=dst,
            send_sem=send,
            recv_sem=recv,
            device_id={"sp": sp, "tp": tp},
            device_id_type=MESH,
        )

    def first_q(h):
        return remote(
            r.q_out.at[h],
            r.q_in.at[z % pair],
            r.first_send.at[0, h],
            r.q_recv.at[z % pair],
            spot(pair * c + h),
            y * pair + z // pair,
        )

    def first_kv(h):
        return remote(
            r.kv_out.at[h],
            r.held.at[z, 0],
            r.first_send.at[1, h],
            r.kv_recv.at[z, 0],
            spot(pair * c + h),
            y * pair + z // pair,
        )

    def to_core(zz, side):
        block = r.held.at[zz, side]
        return remote(block, block, r.core_send.at[zz, side], r.kv_recv.at[zz, side], me, partner)

    def to_side(zz):
        return remote(
            r.held.at[zz, 0], r.held.at[zz, 1], r.side_send.at[zz], r.kv_recv.at[zz, 1], across, mt
        )

    lam_copy = remote(r.lam_mine, r.lam_far, r.lam_sem.at[0], r.lam_sem.at[1], me, partner)

    def away(h):
        return z != pair * c + h

    order = [z, z + 1 - 2 * (z % pair), pair - z // pair, (length - 1) * (1 - z // pair)]

    @pl.when(home)
    def _():
        to_side(z).start()
        to_core(z, 0).start()

    for h in range(2):

        @pl.when(away(h))
        def _():
            first_q(h).start()

    for h in range(2):

        @pl.when(away(h))
        def _():
            first_kv(h).start()

    lam_copy.start()
    filler()

    for g in range(2):

        @pl.when((z != pair * c + g))
        def _():
            remote(
                r.q_out.at[g], r.q_in.at[g], r.first_send.at[0, g], r.q_recv.at[g], me, mt
            ).wait_recv()

        turned = r.q_in[g].astype(jnp.float32).T.astype(jnp.bfloat16)
        r.qt[0:qk, 2 * g * rows : (2 * g + 1) * rows] = turned[0:qk]
        r.qt[qk:keys, (2 * g + 1) * rows : (2 * g + 2) * rows] = turned[qk:keys]

    def absorb(zz, side):
        block_keys = r.held[zz, side, :, 0:keys]
        turned = jnp.concatenate(
            [r.held[zz, side, base : base + vd, keys : keys + vd] for base in range(0, rows, vd)], axis=1
        )
        for part in range(4):
            at = slice(part * rows, (part + 1) * rows)
            scores = jnp.dot(block_keys, r.qt[:, at], preferred_element_type=jnp.float32)
            if after != 1.0:
                scores = scores * after
            old = r.m_ref[:, at]
            new = jnp.maximum(old, jnp.max(scores, axis=0, keepdims=True))
            shrink = jnp.exp(old - new)
            expo = jnp.exp(scores - new)
            r.m_ref[:, at] = new
            r.l_ref[:, at] = r.l_ref[:, at] * shrink + jnp.sum(expo, axis=0, keepdims=True)
            r.acc_ref[:, at] = r.acc_ref[:, at] * shrink + jnp.dot(
                turned, expo.astype(jnp.bfloat16), preferred_element_type=jnp.float32
            )

    near_first = ((0, 0), (0, 1), (1, 0), (1, 1), (2, 0), (3, 0), (2, 1), (3, 1))
    far_first = ((0, 0), (0, 1), (1, 0), (2, 0), (1, 1), (3, 0), (2, 1), (3, 1))

    def pick(values, n):
        result = values[0]
        for k in range(1, len(values)):
            result = jnp.where(n == k, values[k], result)
        return result

    def step(n, carry):
        at_home = [pick([p[i] for p in near_first], n) for i in range(2)]
        at_far = [pick([p[i] for p in far_first], n) for i in range(2)]
        zz = pick(order, jnp.where(home, at_home[0], at_far[0]))
        side = jnp.where(home, at_home[1], at_far[1])
        direct = zz // pair == c
        local = home & (n == 0)

        @pl.when(jnp.logical_not(local))
        def _():
            to_core(zz, side).wait_recv()

            @pl.when(direct & (side == 0))
            def _():
                to_side(zz).start()

            @pl.when(direct)
            def _():
                to_core(zz, side).start()

        absorb(zz, side)
        return carry

    lax.fori_loop(0, 2 * length, step, 0)

    share = rows // n_tp
    lam_copy.wait()
    lam = jnp.where(home, r.lam_mine[0:1, 0:1], r.lam_far[0:1, 0:1])
    head = y * length + z
    columns = pl.ds(pl.multiple_of(head * vd, vd), vd)

    def piece(g, t):
        to = (mt + t) % n_tp
        span = pl.ds(pl.multiple_of(to * share, share), share)
        return remote(
            r.stage.at[g, span],
            r.token_ref.at[:, columns],
            r.head_send.at[g, t],
            r.head_recv.at[head],
            spot(pair * c + g),
            to,
        )

    def own(g):
        return z == pair * c + g

    for g in (1, 0):
        reads = []
        for which in range(2):
            at = slice((2 * g + which) * rows, (2 * g + which + 1) * rows)
            reads.append(r.acc_ref[:, at] / r.l_ref[:, at])
        combined = reads[0] - lam * reads[1]
        combined = combined * lax.rsqrt(
            jnp.mean(combined * combined, axis=0, keepdims=True) + norm_epsilon
        )
        r.stage[g] = (combined.T * r.gain_ref[...]).astype(jnp.bfloat16)
        for t in range(1, n_tp):
            piece(g, t).start()

        @pl.when(own(g))
        def _():
            r.token_ref[:, columns] = r.stage[g, pl.ds(pl.multiple_of(mt * share, share), share), :]

        @pl.when(jnp.logical_not(own(g)))
        def _():
            piece(g, 0).start()

    def head_copy(hd):
        at = pl.ds(pl.multiple_of(hd * vd, vd), vd)
        return remote(
            r.stage.at[0, 0:share], r.token_ref.at[:, at], r.head_send.at[0, 0], r.head_recv.at[hd], me, mt
        )

    for hd in range(2 * n_tp):

        @pl.when((hd != head) | jnp.logical_not(home))
        def _():
            head_copy(hd).wait_recv()

    for g in range(2):
        for t in range(1, n_tp):
            piece(g, t).wait_send()

        @pl.when(jnp.logical_not(own(g)))
        def _():
            piece(g, 0).wait_send()

        @pl.when(away(g))
        def _():
            first_q(g).wait_send()
            first_kv(g).wait_send()

    for zz in range(length):

        @pl.when(c == zz // pair)
        def _():
            to_side(zz).wait_send()
            to_core(zz, 0).wait_send()
            to_core(zz, 1).wait_send()


def routing_tables(r, experts_in_all, cap):
    ids = r.ids_ref[...].astype(jnp.float32)
    top, share = ids.shape
    names = lax.broadcasted_iota(jnp.int32, (experts_in_all, share), 0).astype(jnp.float32)
    before = lax.broadcasted_iota(jnp.int32, (share, share), 0)
    before = before < lax.broadcasted_iota(jnp.int32, (share, share), 1)
    before = before.astype(jnp.float32).astype(jnp.bfloat16)
    taken = jnp.zeros((experts_in_all, 1), jnp.float32)
    places = lax.broadcasted_iota(jnp.int32, (experts_in_all * cap, share), 0).astype(jnp.float32)
    logits = [r.logits_ref[k : k + 1, :] for k in range(top)]
    highest = functools.reduce(jnp.maximum, logits)
    powers = [jnp.exp(logit - highest) for logit in logits]
    total = sum(powers)
    table = jnp.zeros(places.shape, jnp.float32)
    spread = jnp.zeros(places.shape, jnp.float32)
    for k in range(top):
        hit = (names == ids[k : k + 1, :]).astype(jnp.float32)
        earlier = jnp.dot(hit.astype(jnp.bfloat16), before, preferred_element_type=jnp.float32)
        rank = jnp.sum(hit * (earlier + taken), axis=0, keepdims=True)
        taken = taken + jnp.sum(hit, axis=1, keepdims=True)
        placed = (places == ids[k : k + 1, :] * cap + rank).astype(jnp.float32)
        table = table + placed
        spread = spread + placed * (powers[k] / total * r.prob_ref[...])
    r.table[...] = table.astype(jnp.bfloat16)
    turned = spread.T
    high = turned.astype(jnp.bfloat16)
    r.spread[0:share] = high
    r.spread[share : 2 * share] = (turned - high.astype(jnp.float32)).astype(jnp.bfloat16)


def token_phase(r, wait_weights):
    share, width = r.residual.shape
    tile = math.gcd(width, 512)
    columns = [slice(n, n + tile) for n in range(0, width, tile)]
    wait_weights()
    square = jnp.zeros((share, 1), jnp.float32)
    for at in columns:
        mix = jnp.dot(r.token_ref[...], r.out_w[:, at], preferred_element_type=jnp.float32)
        hidden = (r.residual[:, at].astype(jnp.float32) + mix).astype(jnp.bfloat16)
        r.hidden[:, at] = hidden
        hidden = hidden.astype(jnp.float32)
        square = square + jnp.sum(hidden * hidden, axis=1, keepdims=True)
    factor = lax.rsqrt(square / width + norm_epsilon)
    n_sp, experts, cap = r.outgoing.shape[:3]
    for at in columns:
        normed = r.hidden[:, at].astype(jnp.float32) * factor * r.norm_ref[:, at]
        rows = jnp.dot(
            r.table[...], normed.astype(jnp.bfloat16), preferred_element_type=jnp.float32
        ).astype(jnp.bfloat16)
        r.outgoing[:, :, :, at] = rows.reshape(n_sp, experts, cap, tile)


def expert_phase(n_sp, n_tp, r, weights):
    me, mt = lax.axis_index("sp"), lax.axis_index("tp")
    inner_sp = 2
    z, x = me // inner_sp, me % inner_sp
    inner, across, partner = tp_peers(n_tp)
    groups = n_tp // inner
    o, c = mt // inner, mt % inner
    _, experts, cap, _ = r.outgoing.shape

    def flip(number, by):
        low = (number % 2 + by % 2) % 2
        return (number // 2 + by // 2) % 2 * 2 + low

    def peer_of(i):
        return flip(z, i // inner_sp) * inner_sp + flip(x, i % inner_sp)

    def span(t):
        return pl.ds(pl.multiple_of(t * cap, cap), cap)

    def remote(src, dst, send, recv, sp, tp):
        return pltpu.make_async_remote_copy(
            src_ref=src,
            dst_ref=dst,
            send_sem=send,
            recv_sem=recv,
            device_id={"sp": sp, "tp": tp},
            device_id_type=MESH,
        )

    def sp_copy(i):
        to = peer_of(i)
        block = r.rows.at[i, :, span(mt)]
        return remote(r.outgoing.at[to], block, r.sp_send.at[i], r.sp_recv.at[i], to, mt)

    def across_in(i, g, t):
        block = r.rows.at[i, :, span(t)]
        return remote(block, block, r.y_send.at[g, i], r.y_recv.at[g, i], me, across[g - 1])

    def core_in(i, g, t):
        block = r.rows.at[i, :, span(t)]
        return remote(block, block, r.c_send.at[g, i], r.c_recv.at[g, i], me, partner)

    def core_out(i, g):
        row = ((o + g) % groups) * inner + (inner - 1 - c)
        block = r.part.at[i, :, span(row)]
        return remote(
            block, r.from_core.at[i, g], r.rc_send.at[i, g], r.rc_recv.at[i, g], me, partner
        )

    def across_out(i, g):
        return remote(
            r.summed.at[i, g],
            r.from_across.at[i, g],
            r.ry_send.at[i, g],
            r.ry_recv.at[i, g],
            me,
            across[g - 1],
        )

    def sp_out(i):
        return remote(
            r.total.at[i], r.returned.at[me], r.rs_send.at[i], r.rs_recv.at[i], peer_of(i), mt
        )

    def source(g):
        return ((o - g + groups) % groups) * inner + c

    for i in range(1, n_sp):
        sp_copy(i).start()
    r.rows[0, :, span(mt), :] = r.outgoing[me]

    def spread(i):
        @pl.when(i > 0)
        def _():
            sp_copy(i).wait_recv()

        for g in range(1, groups):
            across_in(i, g, mt).start()
        core_in(i, 0, mt).start()

    def relay(i):
        for g in range(1, groups):
            across_in(i, g, source(g)).wait_recv()
            core_in(i, g, source(g)).start()

    half = n_sp // 2

    def compute(i):
        @pl.when(i == half)
        def _():
            for copy in weights:
                copy.wait()

        for g in range(groups):
            core_in(i, g, source(g)).wait_recv()
        for e in range(experts):
            rows = r.rows[i, e]
            gate = jnp.dot(rows, r.gate_w[e], preferred_element_type=jnp.float32)
            upper = jnp.dot(rows, r.up_w[e], preferred_element_type=jnp.float32)
            middle = (gate / (1.0 + jnp.exp(-gate)) * upper).astype(jnp.bfloat16)
            r.part[i, e] = jnp.dot(middle, r.down_w[e], preferred_element_type=jnp.float32).astype(
                r.part.dtype
            )
        for g in list(range(1, groups)) + [0]:
            core_out(i, g).start()

    def pair_sum(i, g):
        row = ((o + g) % groups) * inner + c
        value = r.part[i, :, span(row), :].astype(jnp.float32)
        core_out(i, g).wait_recv()
        return value + r.from_core[i, g].astype(jnp.float32)

    def first(i):
        for g in range(1, groups):
            r.summed[i, g] = pair_sum(i, g).astype(r.summed.dtype)
            across_out(i, g).start()

    def second(i):
        value = pair_sum(i, 0)
        for g in range(1, groups):
            across_out(i, g).wait_recv()
            value = value + r.from_across[i, g].astype(jnp.float32)
        value = value.astype(r.total.dtype)

        @pl.when(i == 0)
        def _():
            r.returned[me] = value

        @pl.when(i > 0)
        def _():
            r.total[i] = value
            sp_out(i).start()

    def far_first(k):
        near = n_sp - 1 - k
        near = jnp.where(near > 1, half // 2 + n_sp - 1 - half - near, near)
        return jnp.where(k < half, k + half, near)

    def turned(stage):
        return lambda k: stage(far_first(k))

    stages = (spread, relay) + tuple(turned(stage) for stage in (compute, first, second))
    lags = (0, 1, half + 1, half + 2, half + 4)

    def step(i, carry):
        for stage, lag in zip(stages, lags):

            @pl.when((i >= lag) & (i < n_sp + lag))
            def _():
                stage(i - lag)

        return carry

    lax.fori_loop(0, n_sp + lags[-1], step, 0)

    def arrive(i, carry):
        sp_out(i).wait_recv()
        return carry

    lax.fori_loop(1, n_sp, arrive, 0)
    share = r.residual.shape[0]
    width = r.residual.shape[1]
    tile = math.gcd(width, 512)
    for n in range(0, width, tile):
        at = slice(n, n + tile)
        both = jnp.dot(
            r.spread[...],
            r.returned[:, :, :, at].reshape(n_sp * experts * cap, tile),
            preferred_element_type=jnp.float32,
        )
        r.out_ref[:, at] = (
            r.hidden[:, at].astype(jnp.float32) + (both[:share] + both[share:])
        ).astype(jnp.bfloat16)

    def drain(i, carry):
        @pl.when(i > 0)
        def _():
            sp_out(i).wait_send()
            sp_copy(i).wait_send()

        for g in range(groups):
            if g:
                across_in(i, g, mt).wait_send()
                across_out(i, g).wait_send()
            core_in(i, g, mt).wait_send()
            core_out(i, g).wait_send()
        return carry

    lax.fori_loop(0, n_sp, drain, 0)


def layer_kernel(n_sp, n_tp, names, *refs):
    r = types.SimpleNamespace(**dict(zip(names, refs)))
    me, mt = lax.axis_index("sp"), lax.axis_index("tp")
    inner = 2
    z, x = me // inner, me % inner
    barrier = pltpu.get_barrier_semaphore()
    lines = [(zz * inner + x, t) for zz in range(n_sp // inner) for t in range(n_tp)]
    lines += [(zz * inner + (1 - x), mt) for zz in range(n_sp // inner)]
    for sp, tp in lines:

        @pl.when((sp != me) | (tp != mt))
        def _():
            pl.semaphore_signal(
                barrier, inc=1, device_id={"sp": sp, "tp": tp}, device_id_type=MESH
            )

    def loads(pairs):
        copies = [
            pltpu.make_async_copy(getattr(r, src), getattr(r, dst), r.load_sem.at[k])
            for k, (src, dst) in pairs
        ]
        for copy in copies:
            copy.start()
        return copies

    pairs = list(enumerate(LOADED))
    first = loads(pairs[:5])
    middle = loads(pairs[5:7])
    last = loads(pairs[7:])
    for copy in first:
        copy.wait()

    def wait_middle():
        for copy in middle:
            copy.wait()

    experts, cap = r.outgoing.shape[1:3]
    attention_phase(
        n_sp,
        n_tp,
        r,
        lambda: pl.semaphore_wait(barrier, len(lines) - 1),
        lambda: routing_tables(r, n_sp * experts, cap),
    )
    token_phase(r, wait_middle)
    expert_phase(n_sp, n_tp, r, last)


LOADED = (
    ("k1_hbm", "k1_ref"),
    ("k2_hbm", "k2_ref"),
    ("v_hbm", "v_ref"),
    ("q1_hbm", "q1_ref"),
    ("q2_hbm", "q2_ref"),
    ("out_w_hbm", "out_w"),
    ("residual_hbm", "residual"),
    ("gate_hbm", "gate_w"),
    ("up_hbm", "up_w"),
    ("down_hbm", "down_w"),
)


def whole_layer(n_sp, n_tp, cap, big, lam, gain, norm, ids, logits, prob):
    k1, k2, v, q1, q2, out_w, residual, gate, up, down = big
    rows, keys = q1.shape
    length = n_sp // 2
    vd = v.shape[1] // 2
    cols = keys + vd
    share, width = residual.shape
    experts = gate.shape[0]
    slots = n_sp * experts * cap
    groups = n_tp // 2
    bf16, f32 = jnp.bfloat16, jnp.float32
    vmem = pl.BlockSpec(memory_space=pltpu.VMEM)
    dma = pltpu.SemaphoreType.DMA
    piece = (experts, cap, width)
    scratch = [(dst, pltpu.VMEM(a.shape, a.dtype)) for (_, dst), a in zip(LOADED, big)]
    scratch += [
        ("token_ref", pltpu.VMEM((share, out_w.shape[0]), bf16)),
        ("kv_out", pltpu.VMEM((2, rows, cols), bf16)),
        ("q_out", pltpu.VMEM((2, rows, keys), bf16)),
        ("held", pltpu.VMEM((length, 2, rows, cols), bf16)),
        ("q_in", pltpu.VMEM((2, rows, keys), bf16)),
        ("qt", pltpu.VMEM((keys, 4 * rows), bf16)),
        ("m_ref", pltpu.VMEM((1, 4 * rows), f32)),
        ("l_ref", pltpu.VMEM((1, 4 * rows), f32)),
        ("acc_ref", pltpu.VMEM((vd, 4 * rows), f32)),
        ("stage", pltpu.VMEM((2, rows, vd), bf16)),
        ("lam_mine", pltpu.VMEM((8, 128), f32)),
        ("lam_far", pltpu.VMEM((8, 128), f32)),
        ("table", pltpu.VMEM((slots, share), bf16)),
        ("spread", pltpu.VMEM((2 * share, slots), bf16)),
        ("hidden", pltpu.VMEM((share, width), bf16)),
        ("outgoing", pltpu.VMEM((n_sp,) + piece, bf16)),
        ("returned", pltpu.VMEM((n_sp,) + piece, bf16)),
        ("rows", pltpu.VMEM((n_sp, experts, n_tp * cap, width), bf16)),
        ("part", pltpu.VMEM((n_sp, experts, n_tp * cap, width), bf16)),
        ("from_core", pltpu.VMEM((n_sp, groups) + piece, bf16)),
        ("from_across", pltpu.VMEM((n_sp, groups) + piece, bf16)),
        ("summed", pltpu.VMEM((n_sp, groups) + piece, bf16)),
        ("total", pltpu.VMEM((n_sp,) + piece, bf16)),
        ("load_sem", dma((len(LOADED),))),
        ("first_send", dma((2, 2))),
        ("core_send", dma((length, 2))),
        ("side_send", dma((length,))),
        ("kv_recv", dma((length, 2))),
        ("q_recv", dma((2,))),
        ("lam_sem", dma((2,))),
        ("head_send", dma((2, n_tp))),
        ("head_recv", dma((2 * n_tp,))),
        ("sp_send", dma((n_sp,))),
        ("sp_recv", dma((n_sp,))),
        ("y_send", dma((groups, n_sp))),
        ("y_recv", dma((groups, n_sp))),
        ("c_send", dma((groups, n_sp))),
        ("c_recv", dma((groups, n_sp))),
        ("rc_send", dma((n_sp, groups))),
        ("rc_recv", dma((n_sp, groups))),
        ("ry_send", dma((n_sp, groups))),
        ("ry_recv", dma((n_sp, groups))),
        ("rs_send", dma((n_sp,))),
        ("rs_recv", dma((n_sp,))),
    ]
    small = ("gain_ref", "norm_ref", "ids_ref", "logits_ref", "prob_ref")
    names = [src for src, _ in LOADED] + ["lam_ref", *small, "out_ref"]
    names += [name for name, _ in scratch]
    return pl.pallas_call(
        functools.partial(layer_kernel, n_sp, n_tp, names),
        out_shape=jax.ShapeDtypeStruct((share, width), bf16),
        in_specs=[pl.BlockSpec(memory_space=pl.ANY)] * len(LOADED)
        + [pl.BlockSpec(memory_space=pltpu.SMEM)]
        + [vmem] * len(small),
        out_specs=vmem,
        scratch_shapes=[shape for _, shape in scratch],
        compiler_params=pltpu.CompilerParams(
            collective_id=3, has_side_effects=True, vmem_limit_bytes=VMEM_LIMIT
        ),
    )(*big, lam, gain, norm, ids, logits, prob)


def layers_fit(n_sp, n_tp, rows, vd, keys, heads, cap):
    square = heads == 2 and n_sp == 8 and n_tp == 4
    return square and rows % vd == 0 and vd == keys and vd % 128 == 0 and cap % 16 == 0


def on_device(
    n_sp,
    n_tp,
    query_one,
    key_one,
    query_two,
    key_two,
    values,
    mix_lambda,
    head_gain,
    residual_in,
    out_weight,
    norm_gain,
    route_ids,
    route_logits,
    group_prob,
    gate_weight,
    up_weight,
    down_weight,
):
    share = residual_in.shape[0]
    top_count = route_ids.shape[1]
    local_experts = gate_weight.shape[0]
    expert_count = local_experts * n_sp
    capacity = max(2, 2 * share * top_count // expert_count)
    if layers_fit(
        n_sp,
        n_tp,
        query_one.shape[0],
        values.shape[1] // 2,
        query_one.shape[1],
        mix_lambda.shape[0],
        capacity,
    ):
        big = (key_one, key_two, values, query_one, query_two, out_weight, residual_in)
        return whole_layer(
            n_sp,
            n_tp,
            capacity,
            big + (gate_weight, up_weight, down_weight),
            mix_lambda,
            head_gain[None, :],
            norm_gain[None, :],
            route_ids.T,
            route_logits.T,
            group_prob[None, :],
        )
    token_heads = attend(
        n_sp,
        n_tp,
        key_one,
        key_two,
        values,
        query_one,
        query_two,
        mix_lambda,
        head_gain[None, :],
    )
    mix = jnp.dot(token_heads, out_weight, preferred_element_type=jnp.float32)
    hidden_f = (residual_in.astype(jnp.float32) + mix).astype(jnp.bfloat16).astype(jnp.float32)
    normed = (
        hidden_f
        * lax.rsqrt(jnp.mean(hidden_f * hidden_f, axis=-1, keepdims=True) + norm_epsilon)
        * norm_gain
    ).astype(jnp.bfloat16)
    width = normed.shape[1]
    slots = expert_count * capacity
    flat_ids = route_ids.reshape(-1)
    one_hot = (flat_ids[:, None] == jnp.arange(expert_count, dtype=jnp.int32)[None, :]).astype(
        jnp.int32
    )
    earlier = jnp.cumsum(one_hot, axis=0) - one_hot
    rank = jnp.sum(earlier * one_hot, axis=1)
    slot_of = (flat_ids * capacity + rank).reshape(share, top_count)
    places = jnp.arange(slots, dtype=jnp.int32)
    table = sum(
        (places[:, None] == slot_of[None, :, k]).astype(jnp.bfloat16) for k in range(top_count)
    )
    outgoing = jnp.dot(table, normed, preferred_element_type=jnp.float32).astype(jnp.bfloat16)
    outgoing = outgoing.reshape(n_sp, local_experts, capacity, width)
    everyone = dispatch(n_sp, n_tp, outgoing).reshape(
        local_experts, n_tp * n_sp * capacity, width
    )
    gate = jnp.einsum("erd,edf->erf", everyone, gate_weight, preferred_element_type=jnp.float32)
    upper = jnp.einsum("erd,edf->erf", everyone, up_weight, preferred_element_type=jnp.float32)
    middle = (jax.nn.silu(gate) * upper).astype(jnp.bfloat16)
    part_sum = jnp.einsum(
        "erf,efd->erd", middle, down_weight, preferred_element_type=jnp.float32
    ).astype(jnp.bfloat16)
    returned = collect(
        n_sp, n_tp, part_sum.reshape(local_experts, n_tp, n_sp, capacity, width)
    ).reshape(slots, width)
    logits = [route_logits[:, k : k + 1] for k in range(top_count)]
    highest = functools.reduce(jnp.maximum, logits)
    powers = [jnp.exp(logit - highest) for logit in logits]
    route_weight = [power / sum(powers) * group_prob[:, None] for power in powers]
    spread = sum(
        jnp.where(places[None, :] == slot_of[:, k, None], route_weight[k], 0.0)
        for k in range(top_count)
    )
    high = spread.astype(jnp.bfloat16)
    low = (spread - high.astype(jnp.float32)).astype(jnp.bfloat16)
    both = jnp.dot(
        jnp.concatenate([high, low], axis=0), returned, preferred_element_type=jnp.float32
    )
    return (hidden_f + (both[:share] + both[share:])).astype(jnp.bfloat16)


def solution(mesh):
    in_specs = (
        P("sp", "tp"),
        P("sp", "tp"),
        P("sp", "tp"),
        P("sp", "tp"),
        P("sp", "tp"),
        P("tp"),
        P(),
        P(("sp", "tp"), None),
        P(),
        P(),
        P(("sp", "tp"), None),
        P(("sp", "tp"), None),
        P(("sp", "tp")),
        P("sp", None, "tp"),
        P("sp", None, "tp"),
        P("sp", "tp", None),
    )
    out_specs = P(("sp", "tp"), None)
    return jax.shard_map(
        functools.partial(on_device, mesh.shape["sp"], mesh.shape["tp"]),
        mesh=mesh,
        in_specs=in_specs,
        out_specs=out_specs,
        check_vma=False,
    )
```

```python
import functools
import math
import types

import jax
import jax.numpy as jnp
from jax import lax
from jax.experimental import pallas as pl
from jax.experimental.pallas import tpu as pltpu
from jax.sharding import PartitionSpec as P

norm_epsilon = 1e-06
MESH = pl.DeviceIdType.MESH
VMEM_LIMIT = 60 * 1024 * 1024
LAYER_LIMIT = VMEM_LIMIT


def pair_of(count):
    return 2 if count % 2 == 0 else 1


def greet(peers):
    barrier = pltpu.get_barrier_semaphore()
    for peer in peers:
        pl.semaphore_signal(barrier, inc=1, device_id=peer, device_id_type=MESH)
    pl.semaphore_wait(barrier, len(peers))


def attend_kernel(
    n_sp,
    n_tp,
    vd,
    k1_ref,
    k2_ref,
    v_ref,
    q1_ref,
    q2_ref,
    lam_ref,
    gain_ref,
    out_ref,
    kvp,
    qp,
    held,
    q_far,
    m_ref,
    l_ref,
    acc_ref,
    stage,
    cross_send,
    cross_recv,
    line_send,
    line_recv,
    side_send,
    side_recv,
    head_send,
    head_recv,
):
    inner = pair_of(n_sp)
    length = n_sp // inner
    half = length // 2
    me = lax.axis_index("sp")
    mt = lax.axis_index("tp")
    z, x = me // inner, me % inner
    head, zi = z // half, z % half
    rows = q1_ref.shape[0]
    qk = q1_ref.shape[1] // 2
    scale = 1.0 / math.sqrt(qk)
    exact = math.frexp(scale)[0] == 0.5
    early, after = (scale, 1.0) if exact else (1.0, scale)
    other = z * inner + (inner - 1 - x)
    mirror = (length - 1 - z) * inner + x
    far_zi = half - 1 - zi
    for h in range(2):
        kvp[h, :, 0:qk] = k1_ref[:, h * qk : (h + 1) * qk]
        kvp[h, :, qk : 2 * qk] = k2_ref[:, h * qk : (h + 1) * qk]
        kvp[h, :, 2 * qk : 2 * qk + vd] = v_ref[:, h * vd : (h + 1) * vd]
        qp[h, :, 0:qk] = q1_ref[:, h * qk : (h + 1) * qk] * jnp.bfloat16(early)
        qp[h, :, qk : 2 * qk] = q2_ref[:, h * qk : (h + 1) * qk] * jnp.bfloat16(early)

    def line_device(zz):
        return (head * half + zz) * inner + x

    peers = [{"sp": me, "tp": (mt + t) % n_tp} for t in range(1, n_tp)]
    peers += [{"sp": mirror, "tp": (mt + t) % n_tp} for t in range(n_tp)]
    if inner == 2:
        peers.append({"sp": other, "tp": mt})
    if half > 1:
        for shift in sorted({1, half - 1}):
            peers.append({"sp": line_device((zi + shift) % half), "tp": mt})
    greet(peers)

    def remote(src, dst, send, recv, sp):
        return pltpu.make_async_remote_copy(
            src_ref=src,
            dst_ref=dst,
            send_sem=send,
            recv_sem=recv,
            device_id={"sp": sp, "tp": mt},
            device_id_type=MESH,
        )

    cross_q = remote(qp.at[1 - head], q_far, cross_send.at[0], cross_recv.at[0], mirror)
    cross_kv = remote(
        kvp.at[1 - head], held.at[1, far_zi, x], cross_send.at[1], cross_recv.at[1], mirror
    )

    def line_copy(j, src, zz, way):
        ahead = jnp.clip(jnp.where(way == 0, zi + 1, zi - 1), 0, half - 1)
        return remote(
            src,
            held.at[j, zz, x],
            line_send.at[j, way, zz],
            line_recv.at[j, zz],
            line_device(ahead),
        )

    def side_copy(j, src, zz):
        return remote(src, held.at[j, zz, x], side_send.at[j, zz], side_recv.at[j, zz], other)

    def start_from(j, src):
        @pl.when(zi + 1 < half)
        def _():
            line_copy(j, src, zi, 0).start()

        @pl.when(zi > 0)
        def _():
            line_copy(j, src, zi, 1).start()

        if inner == 2:
            side_copy(j, src, zi).start()

    own = kvp.at[head]
    cross_kv.start()
    start_from(0, own)
    cross_q.start()
    m_ref[...] = jnp.full(m_ref.shape, -1e30, jnp.float32)
    l_ref[...] = jnp.zeros(l_ref.shape, jnp.float32)
    acc_ref[...] = jnp.zeros(acc_ref.shape, jnp.float32)

    def absorb(block, q_ref, group):
        vals = block[:, 2 * qk : 2 * qk + vd]
        for which in range(2):
            at = 2 * group + which
            scores = lax.dot_general(
                q_ref[:, which * qk : (which + 1) * qk],
                block[:, which * qk : (which + 1) * qk],
                (((1,), (1,)), ((), ())),
                preferred_element_type=jnp.float32,
            )
            if after != 1.0:
                scores = scores * after
            old = m_ref[at]
            new = jnp.maximum(old, jnp.max(scores, axis=1, keepdims=True))
            shrink = jnp.exp(old - new)
            expo = jnp.exp(scores - new[:, :1])
            m_ref[at] = new
            l_ref[at] = l_ref[at] * shrink + jnp.sum(expo, axis=1, keepdims=True)
            acc_ref[at] = acc_ref[at] * shrink[:, :1] + jnp.dot(
                expo.astype(jnp.bfloat16), vals, preferred_element_type=jnp.float32
            )

    q_own = qp.at[head]

    def absorb_both(block):
        absorb(block, q_own, 0)
        absorb(block, q_far, 1)

    def place(n):
        dist = (n + 1) // 2
        return jnp.where(n % 2 == 1, zi - dist, zi + dist), 1 - n % 2

    def line_steps(j, take):
        def line_step(n, carry):
            zz, way = place(n)

            @pl.when((zz >= 0) & (zz < half))
            def _():
                block = held.at[j, zz, x]
                line_copy(j, block, zz, way).wait_recv()
                ahead = jnp.where(way == 0, zi + 1, zi - 1)

                @pl.when((ahead >= 0) & (ahead < half))
                def _():
                    line_copy(j, block, zz, way).start()

                if inner == 2:
                    side_copy(j, block, zz).start()
                take(block)

            return carry

        lax.fori_loop(1, 2 * half - 1, line_step, 0)

    def line_again(j):
        def again(n, carry):
            zz, _ = place(n)

            @pl.when((zz >= 0) & (zz < half))
            def _():
                absorb(held.at[j, zz, x], q_far, 1)

            return carry

        lax.fori_loop(1, 2 * half - 1, again, 0)

    def side_steps(j, begin):
        def side_step(n, carry):
            zz, _ = place(n)

            @pl.when((zz >= 0) & (zz < half))
            def _():
                block = held.at[j, zz, 1 - x]
                side_copy(j, block, zz).wait_recv()
                absorb_both(block)

            return carry

        lax.fori_loop(begin, 2 * half - 1, side_step, 0)

    near = held.at[0, zi, 1 - x]
    far = held.at[1, zi, x]
    absorb(own, q_own, 0)
    if inner == 2:
        side_copy(0, near, zi).wait_recv()
        absorb(near, q_own, 0)
    line_steps(0, lambda block: absorb(block, q_own, 0))
    cross_kv.wait_recv()
    start_from(1, far)
    absorb(far, q_own, 0)
    cross_q.wait_recv()
    absorb(own, q_far, 1)
    absorb(far, q_far, 1)
    line_steps(1, absorb_both)
    line_again(0)
    if inner == 2:
        absorb(near, q_far, 1)
        side_steps(0, 1)
        side_steps(1, 0)

    share = rows // n_tp
    lam = lam_ref[head]
    columns = pl.ds(pl.multiple_of((mt * 2 + head) * vd, vd), vd)
    copies = []
    for group, sp in ((1, mirror), (0, me)):
        read_a = acc_ref[2 * group] / l_ref[2 * group][:, :1]
        read_b = acc_ref[2 * group + 1] / l_ref[2 * group + 1][:, :1]
        combined = read_a - lam * read_b
        combined = (
            combined
            * lax.rsqrt(jnp.mean(combined * combined, axis=-1, keepdims=True) + norm_epsilon)
            * gain_ref[...]
        )
        stage[group] = combined.astype(jnp.bfloat16)
        for t in range(n_tp):
            to = (mt + t) % n_tp
            span = pl.ds(pl.multiple_of(to * share, share), share)
            if group == 0 and t == 0:
                out_ref[:, columns] = stage[0, span, :]
                continue
            copy = pltpu.make_async_remote_copy(
                src_ref=stage.at[group, span],
                dst_ref=out_ref.at[:, columns],
                send_sem=head_send.at[group, t],
                recv_sem=head_recv.at[group, t],
                device_id={"sp": sp, "tp": to},
                device_id_type=MESH,
            )
            copy.start()
            copies.append(copy)

    cross_q.wait_send()
    cross_kv.wait_send()
    for j in range(2):

        def drain(n, carry):
            zz, way = place(n)

            @pl.when((zz >= 0) & (zz < half))
            def _():
                ahead = jnp.where(way == 0, zi + 1, zi - 1)

                @pl.when((ahead >= 0) & (ahead < half))
                def _():
                    line_copy(j, own, zz, way).wait_send()

                if inner == 2:
                    side_copy(j, own, zz).wait_send()

            return carry

        lax.fori_loop(1, 2 * half - 1, drain, 0)

        @pl.when(zi + 1 < half)
        def _():
            line_copy(j, own, zi, 0).wait_send()

        @pl.when(zi > 0)
        def _():
            line_copy(j, own, zi, 1).wait_send()

        if inner == 2:
            side_copy(j, own, zi).wait_send()
    for copy in copies:
        copy.wait()


def attend(n_sp, n_tp, k1, k2, v, q1, q2, lam, gain):
    rows = q1.shape[0]
    inner = pair_of(n_sp)
    half = n_sp // inner // 2
    assert lam.shape[0] == 2 and half * inner * 2 == n_sp
    vd = v.shape[1] // 2
    qk = q1.shape[1] // 2
    cols = 2 * qk + vd
    vmem = pl.BlockSpec(memory_space=pltpu.VMEM)
    dma = pltpu.SemaphoreType.DMA
    return pl.pallas_call(
        functools.partial(attend_kernel, n_sp, n_tp, vd),
        out_shape=jax.ShapeDtypeStruct((rows // n_tp, n_tp * 2 * vd), jnp.bfloat16),
        in_specs=[vmem] * 5 + [pl.BlockSpec(memory_space=pltpu.SMEM), vmem],
        out_specs=vmem,
        scratch_shapes=[
            pltpu.VMEM((2, rows, cols), jnp.bfloat16),
            pltpu.VMEM((2, rows, 2 * qk), jnp.bfloat16),
            pltpu.VMEM((2, half, inner, rows, cols), jnp.bfloat16),
            pltpu.VMEM((rows, 2 * qk), jnp.bfloat16),
            pltpu.VMEM((4, rows, 128), jnp.float32),
            pltpu.VMEM((4, rows, 128), jnp.float32),
            pltpu.VMEM((4, rows, vd), jnp.float32),
            pltpu.VMEM((2, rows, vd), jnp.bfloat16),
            dma((2,)),
            dma((2,)),
            dma((2, 2, half)),
            dma((2, half)),
            dma((2, half)),
            dma((2, half)),
            dma((2, n_tp)),
            dma((2, n_tp)),
        ],
        compiler_params=pltpu.CompilerParams(
            collective_id=0, has_side_effects=True, vmem_limit_bytes=VMEM_LIMIT
        ),
    )(k1, k2, v, q1, q2, lam, gain)


def tp_peers(n_tp):
    inner = pair_of(n_tp)
    mt = lax.axis_index("tp")
    o, c = mt // inner, mt % inner
    across = [((o + d) % (n_tp // inner)) * inner + c for d in range(1, n_tp // inner)]
    return inner, across, o * inner + (inner - 1 - c)


def greet_all(n_sp, n_tp):
    me, mt = lax.axis_index("sp"), lax.axis_index("tp")
    inner, across, partner = tp_peers(n_tp)
    peers = [{"sp": (me + s) % n_sp, "tp": mt} for s in range(1, n_sp)]
    peers += [{"sp": me, "tp": t} for t in across]
    if inner == 2:
        peers.append({"sp": me, "tp": partner})
    greet(peers)


def dispatch_kernel(
    n_sp, n_tp, rows_ref, out_ref, sp_send, sp_recv, y_send, y_recv, c_send, c_recv, own_sem
):
    me, mt = lax.axis_index("sp"), lax.axis_index("tp")
    inner, across, partner = tp_peers(n_tp)
    groups = n_tp // inner
    o = mt // inner
    greet_all(n_sp, n_tp)

    def sp_copy(d):
        to = (me + d) % n_sp
        return pltpu.make_async_remote_copy(
            src_ref=rows_ref.at[to],
            dst_ref=out_ref.at[:, mt, me],
            send_sem=sp_send.at[d],
            recv_sem=sp_recv.at[d],
            device_id={"sp": to, "tp": mt},
            device_id_type=MESH,
        )

    def tp_copy(t, s, to, send, recv):
        return pltpu.make_async_remote_copy(
            src_ref=out_ref.at[:, t, s],
            dst_ref=out_ref.at[:, t, s],
            send_sem=send,
            recv_sem=recv,
            device_id={"sp": me, "tp": to},
            device_id_type=MESH,
        )

    order = sorted(range(1, n_sp), key=lambda d: min(d, n_sp - d))
    for d in reversed(order):
        sp_copy(d).start()
    own = pltpu.make_async_copy(rows_ref.at[me], out_ref.at[:, mt, me], own_sem)
    own.start()
    own.wait()
    started = []

    def spread(d):
        s = (me - d + n_sp) % n_sp
        for g in range(1, groups):
            copy = tp_copy(mt, s, across[g - 1], y_send.at[g, d], y_recv.at[g, d])
            copy.start()
            started.append(copy)
        if inner == 2:
            copy = tp_copy(mt, s, partner, c_send.at[0, d], c_recv.at[0, d])
            copy.start()
            started.append(copy)

    def relay(d):
        s = (me - d + n_sp) % n_sp
        for g in range(1, groups):
            source = ((o - g + groups) % groups) * inner + mt % inner
            tp_copy(source, s, partner, y_send.at[g, d], y_recv.at[g, d]).wait_recv()
            if inner == 2:
                copy = tp_copy(source, s, partner, c_send.at[g, d], c_recv.at[g, d])
                copy.start()
                started.append(copy)

    order = order[::-1]
    sequence = [0] + order
    spread(0)
    for i, d in enumerate(order):
        sp_copy(d).wait_recv()
        spread(d)
        relay(sequence[i])
    relay(sequence[-1])
    for d in range(n_sp):
        s = (me - d + n_sp) % n_sp
        if inner == 2:
            for g in range(groups):
                source = ((o - g + groups) % groups) * inner + (1 - mt % inner)
                tp_copy(source, s, partner, c_send.at[g, d], c_recv.at[g, d]).wait_recv()
    for copy in started:
        copy.wait_send()
    for d in order:
        sp_copy(d).wait_send()


def dispatch(n_sp, n_tp, rows):
    _, experts, cap, width = rows.shape
    groups = n_tp // pair_of(n_tp)
    sem = pltpu.SemaphoreType.DMA
    hbm = pl.BlockSpec(memory_space=pltpu.VMEM)
    return pl.pallas_call(
        functools.partial(dispatch_kernel, n_sp, n_tp),
        out_shape=jax.ShapeDtypeStruct((experts, n_tp, n_sp, cap, width), rows.dtype),
        in_specs=[hbm],
        out_specs=pl.BlockSpec(memory_space=pl.ANY),
        scratch_shapes=[
            sem((n_sp,)),
            sem((n_sp,)),
            sem((groups, n_sp)),
            sem((groups, n_sp)),
            sem((groups, n_sp)),
            sem((groups, n_sp)),
            sem,
        ],
        compiler_params=pltpu.CompilerParams(
            collective_id=1, has_side_effects=True, vmem_limit_bytes=VMEM_LIMIT
        ),
    )(rows)


def collect_kernel(
    n_sp,
    n_tp,
    part_ref,
    out_ref,
    from_core,
    from_across,
    summed,
    total,
    c_send,
    c_recv,
    y_send,
    y_recv,
    sp_send,
    sp_recv,
):
    me, mt = lax.axis_index("sp"), lax.axis_index("tp")
    inner, across, partner = tp_peers(n_tp)
    groups = n_tp // inner
    o, c = mt // inner, mt % inner
    greet_all(n_sp, n_tp)
    order = sorted(range(1, n_sp), key=lambda d: min(d, n_sp - d), reverse=True) + [0]

    def to_of(d):
        return (me + d) % n_sp

    def core_copy(d, g):
        row = ((o + g) % groups) * inner + (inner - 1 - c)
        return pltpu.make_async_remote_copy(
            src_ref=part_ref.at[:, row, to_of(d)],
            dst_ref=from_core.at[d, g],
            send_sem=c_send.at[d, g],
            recv_sem=c_recv.at[d, g],
            device_id={"sp": me, "tp": partner},
            device_id_type=MESH,
        )

    def across_copy(d, g):
        return pltpu.make_async_remote_copy(
            src_ref=summed.at[d, g],
            dst_ref=from_across.at[d, g],
            send_sem=y_send.at[d, g],
            recv_sem=y_recv.at[d, g],
            device_id={"sp": me, "tp": across[g - 1]},
            device_id_type=MESH,
        )

    def sp_copy(d):
        return pltpu.make_async_remote_copy(
            src_ref=total.at[d],
            dst_ref=out_ref.at[me],
            send_sem=sp_send.at[d],
            recv_sem=sp_recv.at[d],
            device_id={"sp": to_of(d), "tp": mt},
            device_id_type=MESH,
        )

    if inner == 2:
        for d in order:
            for g in list(range(1, groups)) + [0]:
                core_copy(d, g).start()

    def pair_sum(d, g):
        row = ((o + g) % groups) * inner + c
        value = part_ref[:, row, to_of(d)].astype(jnp.float32)
        if inner == 2:
            core_copy(d, g).wait_recv()
            value = value + from_core[d, g].astype(jnp.float32)
        return value

    def first(d):
        for g in range(1, groups):
            summed[d, g] = pair_sum(d, g).astype(summed.dtype)
            across_copy(d, g).start()

    def second(d):
        value = pair_sum(d, 0)
        for g in range(1, groups):
            across_copy(d, g).wait_recv()
            value = value + from_across[d, g].astype(jnp.float32)
        value = value.astype(total.dtype)
        if d == 0:
            out_ref[me] = value
        else:
            total[d] = value
            sp_copy(d).start()

    ahead = min(3, n_sp)
    for d in order[:ahead]:
        first(d)
    for i, d in enumerate(order):
        second(d)
        if i + ahead < n_sp:
            first(order[i + ahead])
    for d in range(1, n_sp):
        sp_copy(d).wait_recv()
    for d in range(n_sp):
        if d:
            sp_copy(d).wait_send()
        for g in range(groups):
            if g:
                across_copy(d, g).wait_send()
            if inner == 2:
                core_copy(d, g).wait_send()


def collect(n_sp, n_tp, part):
    experts, _, _, cap, width = part.shape
    groups = n_tp // pair_of(n_tp)
    sem = pltpu.SemaphoreType.DMA
    vmem = pl.BlockSpec(memory_space=pltpu.VMEM)
    piece = (experts, cap, width)
    return pl.pallas_call(
        functools.partial(collect_kernel, n_sp, n_tp),
        out_shape=jax.ShapeDtypeStruct((n_sp,) + piece, part.dtype),
        in_specs=[vmem],
        out_specs=vmem,
        scratch_shapes=[
            pltpu.VMEM((n_sp, groups) + piece, part.dtype),
            pltpu.VMEM((n_sp, groups) + piece, part.dtype),
            pltpu.VMEM((n_sp, groups) + piece, part.dtype),
            pltpu.VMEM((n_sp,) + piece, part.dtype),
            sem((n_sp, groups)),
            sem((n_sp, groups)),
            sem((n_sp, groups)),
            sem((n_sp, groups)),
            sem((n_sp,)),
            sem((n_sp,)),
        ],
        compiler_params=pltpu.CompilerParams(
            collective_id=2, has_side_effects=True, vmem_limit_bytes=VMEM_LIMIT
        ),
    )(part)


def attention_phase(n_sp, n_tp, r, arrived, filler):
    inner, pair = 2, 2
    length = n_sp // inner
    me, mt = lax.axis_index("sp"), lax.axis_index("tp")
    z, x = me // inner, me % inner
    y, c = mt // pair, mt % pair
    rows, qk = r.q1_ref.shape[0], r.q1_ref.shape[1] // 2
    vd = r.v_ref.shape[1] // 2
    keys = 2 * qk
    scale = 1.0 / math.sqrt(qk)
    exact = math.frexp(scale)[0] == 0.5
    early, after = (scale, 1.0) if exact else (1.0, scale)
    home = c == z // pair
    partner = y * pair + (1 - c)
    across = z * inner + (1 - x)

    def spot(zz):
        return zz * inner + x

    for h in range(2):
        at = slice(h * qk, (h + 1) * qk)
        block = jnp.concatenate([r.k1_ref[:, at], r.k2_ref[:, at]], axis=1)
        turned = jnp.concatenate(
            [
                r.v_ref[base : base + vd, h * vd : (h + 1) * vd].astype(jnp.float32).T
                for base in range(0, rows, vd)
            ],
            axis=0,
        ).astype(jnp.bfloat16)
        query = jnp.concatenate([r.q1_ref[:, at], r.q2_ref[:, at]], axis=1) * jnp.bfloat16(early)
        r.kv_out[h, :, 0:keys] = block
        r.kv_out[h, :, keys : keys + vd] = turned
        r.q_out[h] = query

        @pl.when(z == pair * c + h)
        def _():
            r.held[z, 0, :, 0:keys] = block
            r.held[z, 0, :, keys : keys + vd] = turned
            r.q_in[h] = query

    r.lam_mine[...] = jnp.full(r.lam_mine.shape, r.lam_ref[z % pair], jnp.float32)
    r.m_ref[...] = jnp.full(r.m_ref.shape, -1e30, jnp.float32)
    r.l_ref[...] = jnp.zeros(r.l_ref.shape, jnp.float32)
    r.acc_ref[...] = jnp.zeros(r.acc_ref.shape, jnp.float32)
    r.qt[...] = jnp.zeros(r.qt.shape, r.qt.dtype)
    arrived()

    def remote(src, dst, send, recv, sp, tp):
        return pltpu.make_async_remote_copy(
            src_ref=src,
            dst_ref=dst,
            send_sem=send,
            recv_sem=recv,
            device_id={"sp": sp, "tp": tp},
            device_id_type=MESH,
        )

    def first_q(h):
        return remote(
            r.q_out.at[h],
            r.q_in.at[z % pair],
            r.first_send.at[0, h],
            r.q_recv.at[z % pair],
            spot(pair * c + h),
            y * pair + z // pair,
        )

    def first_kv(h):
        return remote(
            r.kv_out.at[h],
            r.held.at[z, 0],
            r.first_send.at[1, h],
            r.kv_recv.at[z, 0],
            spot(pair * c + h),
            y * pair + z // pair,
        )

    def to_core(zz, side):
        block = r.held.at[zz, side]
        return remote(block, block, r.core_send.at[zz, side], r.kv_recv.at[zz, side], me, partner)

    def to_side(zz):
        return remote(
            r.held.at[zz, 0], r.held.at[zz, 1], r.side_send.at[zz], r.kv_recv.at[zz, 1], across, mt
        )

    lam_copy = remote(r.lam_mine, r.lam_far, r.lam_sem.at[0], r.lam_sem.at[1], me, partner)

    def away(h):
        return z != pair * c + h

    order = [z, z + 1 - 2 * (z % pair), pair - z // pair, (length - 1) * (1 - z // pair)]

    @pl.when(home)
    def _():
        to_side(z).start()
        to_core(z, 0).start()

    for h in range(2):

        @pl.when(away(h))
        def _():
            first_q(h).start()

    for h in range(2):

        @pl.when(away(h))
        def _():
            first_kv(h).start()

    lam_copy.start()
    filler()

    for g in range(2):

        @pl.when((z != pair * c + g))
        def _():
            remote(
                r.q_out.at[g], r.q_in.at[g], r.first_send.at[0, g], r.q_recv.at[g], me, mt
            ).wait_recv()

        turned = r.q_in[g].astype(jnp.float32).T.astype(jnp.bfloat16)
        r.qt[0:qk, 2 * g * rows : (2 * g + 1) * rows] = turned[0:qk]
        r.qt[qk:keys, (2 * g + 1) * rows : (2 * g + 2) * rows] = turned[qk:keys]

    def absorb(zz, side):
        block_keys = r.held[zz, side, :, 0:keys]
        turned = jnp.concatenate(
            [r.held[zz, side, base : base + vd, keys : keys + vd] for base in range(0, rows, vd)], axis=1
        )
        for part in range(4):
            at = slice(part * rows, (part + 1) * rows)
            scores = jnp.dot(block_keys, r.qt[:, at], preferred_element_type=jnp.float32)
            if after != 1.0:
                scores = scores * after
            old = r.m_ref[:, at]
            new = jnp.maximum(old, jnp.max(scores, axis=0, keepdims=True))
            shrink = jnp.exp(old - new)
            expo = jnp.exp(scores - new)
            r.m_ref[:, at] = new
            r.l_ref[:, at] = r.l_ref[:, at] * shrink + jnp.sum(expo, axis=0, keepdims=True)
            r.acc_ref[:, at] = r.acc_ref[:, at] * shrink + jnp.dot(
                turned, expo.astype(jnp.bfloat16), preferred_element_type=jnp.float32
            )

    near_first = ((0, 0), (0, 1), (1, 0), (1, 1), (2, 0), (3, 0), (2, 1), (3, 1))
    far_first = ((0, 0), (0, 1), (1, 0), (2, 0), (1, 1), (3, 0), (2, 1), (3, 1))

    def pick(values, n):
        result = values[0]
        for k in range(1, len(values)):
            result = jnp.where(n == k, values[k], result)
        return result

    def step(n, carry):
        at_home = [pick([p[i] for p in near_first], n) for i in range(2)]
        at_far = [pick([p[i] for p in far_first], n) for i in range(2)]
        zz = pick(order, jnp.where(home, at_home[0], at_far[0]))
        side = jnp.where(home, at_home[1], at_far[1])
        direct = zz // pair == c
        local = home & (n == 0)

        @pl.when(jnp.logical_not(local))
        def _():
            to_core(zz, side).wait_recv()

            @pl.when(direct & (side == 0))
            def _():
                to_side(zz).start()

            @pl.when(direct)
            def _():
                to_core(zz, side).start()

        absorb(zz, side)
        return carry

    lax.fori_loop(0, 2 * length, step, 0)

    share = rows // n_tp
    lam_copy.wait()
    lam = jnp.where(home, r.lam_mine[0:1, 0:1], r.lam_far[0:1, 0:1])
    head = y * length + z
    columns = pl.ds(pl.multiple_of(head * vd, vd), vd)

    def piece(g, t):
        to = (mt + t) % n_tp
        span = pl.ds(pl.multiple_of(to * share, share), share)
        return remote(
            r.stage.at[g, span],
            r.token_ref.at[:, columns],
            r.head_send.at[g, t],
            r.head_recv.at[head],
            spot(pair * c + g),
            to,
        )

    def own(g):
        return z == pair * c + g

    for g in (1, 0):
        reads = []
        for which in range(2):
            at = slice((2 * g + which) * rows, (2 * g + which + 1) * rows)
            reads.append(r.acc_ref[:, at] / r.l_ref[:, at])
        combined = reads[0] - lam * reads[1]
        combined = combined * lax.rsqrt(
            jnp.mean(combined * combined, axis=0, keepdims=True) + norm_epsilon
        )
        r.stage[g] = (combined.T * r.gain_ref[...]).astype(jnp.bfloat16)
        for t in range(1, n_tp):
            piece(g, t).start()

        @pl.when(own(g))
        def _():
            r.token_ref[:, columns] = r.stage[g, pl.ds(pl.multiple_of(mt * share, share), share), :]

        @pl.when(jnp.logical_not(own(g)))
        def _():
            piece(g, 0).start()

    def head_copy(hd):
        at = pl.ds(pl.multiple_of(hd * vd, vd), vd)
        return remote(
            r.stage.at[0, 0:share], r.token_ref.at[:, at], r.head_send.at[0, 0], r.head_recv.at[hd], me, mt
        )

    for hd in range(2 * n_tp):

        @pl.when((hd != head) | jnp.logical_not(home))
        def _():
            head_copy(hd).wait_recv()

    for g in range(2):
        for t in range(1, n_tp):
            piece(g, t).wait_send()

        @pl.when(jnp.logical_not(own(g)))
        def _():
            piece(g, 0).wait_send()

        @pl.when(away(g))
        def _():
            first_q(g).wait_send()
            first_kv(g).wait_send()

    for zz in range(length):

        @pl.when(c == zz // pair)
        def _():
            to_side(zz).wait_send()
            to_core(zz, 0).wait_send()
            to_core(zz, 1).wait_send()


def routing_tables(r, experts_in_all, cap):
    ids = r.ids_ref[...].astype(jnp.float32)
    top, share = ids.shape
    names = lax.broadcasted_iota(jnp.int32, (experts_in_all, share), 0).astype(jnp.float32)
    before = lax.broadcasted_iota(jnp.int32, (share, share), 0)
    before = before < lax.broadcasted_iota(jnp.int32, (share, share), 1)
    before = before.astype(jnp.float32).astype(jnp.bfloat16)
    taken = jnp.zeros((experts_in_all, 1), jnp.float32)
    places = lax.broadcasted_iota(jnp.int32, (experts_in_all * cap, share), 0).astype(jnp.float32)
    logits = [r.logits_ref[k : k + 1, :] for k in range(top)]
    highest = functools.reduce(jnp.maximum, logits)
    powers = [jnp.exp(logit - highest) for logit in logits]
    total = sum(powers)
    table = jnp.zeros(places.shape, jnp.float32)
    spread = jnp.zeros(places.shape, jnp.float32)
    for k in range(top):
        hit = (names == ids[k : k + 1, :]).astype(jnp.float32)
        earlier = jnp.dot(hit.astype(jnp.bfloat16), before, preferred_element_type=jnp.float32)
        rank = jnp.sum(hit * (earlier + taken), axis=0, keepdims=True)
        taken = taken + jnp.sum(hit, axis=1, keepdims=True)
        placed = (places == ids[k : k + 1, :] * cap + rank).astype(jnp.float32)
        table = table + placed
        spread = spread + placed * (powers[k] / total * r.prob_ref[...])
    r.table[...] = table.astype(jnp.bfloat16)
    turned = spread.T
    high = turned.astype(jnp.bfloat16)
    r.spread[0:share] = high
    r.spread[share : 2 * share] = (turned - high.astype(jnp.float32)).astype(jnp.bfloat16)


def token_phase(r, wait_weights):
    share, width = r.residual.shape
    tile = math.gcd(width, 512)
    columns = [slice(n, n + tile) for n in range(0, width, tile)]
    wait_weights()
    square = jnp.zeros((share, 1), jnp.float32)
    for at in columns:
        mix = jnp.dot(r.token_ref[...], r.out_w[:, at], preferred_element_type=jnp.float32)
        hidden = (r.residual[:, at].astype(jnp.float32) + mix).astype(jnp.bfloat16)
        r.hidden[:, at] = hidden
        hidden = hidden.astype(jnp.float32)
        square = square + jnp.sum(hidden * hidden, axis=1, keepdims=True)
    factor = lax.rsqrt(square / width + norm_epsilon)
    n_sp, experts, cap = r.outgoing.shape[:3]
    for at in columns:
        normed = r.hidden[:, at].astype(jnp.float32) * factor * r.norm_ref[:, at]
        rows = jnp.dot(
            r.table[...], normed.astype(jnp.bfloat16), preferred_element_type=jnp.float32
        ).astype(jnp.bfloat16)
        r.outgoing[:, :, :, at] = rows.reshape(n_sp, experts, cap, tile)


def expert_phase(n_sp, n_tp, r, weights):
    me, mt = lax.axis_index("sp"), lax.axis_index("tp")
    inner_sp = 2
    z, x = me // inner_sp, me % inner_sp
    inner, across, partner = tp_peers(n_tp)
    groups = n_tp // inner
    o, c = mt // inner, mt % inner
    _, experts, cap, _ = r.outgoing.shape

    def flip(number, by):
        low = (number % 2 + by % 2) % 2
        return (number // 2 + by // 2) % 2 * 2 + low

    def peer_of(i):
        return flip(z, i // inner_sp) * inner_sp + flip(x, i % inner_sp)

    def span(t):
        return pl.ds(pl.multiple_of(t * cap, cap), cap)

    def remote(src, dst, send, recv, sp, tp):
        return pltpu.make_async_remote_copy(
            src_ref=src,
            dst_ref=dst,
            send_sem=send,
            recv_sem=recv,
            device_id={"sp": sp, "tp": tp},
            device_id_type=MESH,
        )

    pieces = n_sp * experts

    def sp_copy(j):
        i, e = j // experts, j % experts
        to = peer_of(i)
        block = r.rows.at[i, e, span(mt)]
        return remote(r.outgoing.at[to, e], block, r.sp_send.at[j], r.sp_recv.at[j], to, mt)

    def across_in(j, g, t):
        block = r.rows.at[j // experts, j % experts, span(t)]
        return remote(block, block, r.y_send.at[g, j], r.y_recv.at[g, j], me, across[g - 1])

    def core_in(j, g, t):
        block = r.rows.at[j // experts, j % experts, span(t)]
        return remote(block, block, r.c_send.at[g, j], r.c_recv.at[g, j], me, partner)

    def core_out(j, g):
        row = ((o + g) % groups) * inner + (inner - 1 - c)
        block = r.part.at[j, span(row)]
        return remote(
            block, r.from_core.at[j, g], r.rc_send.at[j, g], r.rc_recv.at[j, g], me, partner
        )

    def across_out(j, g):
        return remote(
            r.summed.at[j, g],
            r.from_across.at[j, g],
            r.ry_send.at[j, g],
            r.ry_recv.at[j, g],
            me,
            across[g - 1],
        )

    def sp_out(j):
        i, e = j // experts, j % experts
        block = r.returned.at[me, e]
        return remote(r.total.at[j], block, r.rs_send.at[j], r.rs_recv.at[j], peer_of(i), mt)

    def source(g):
        return ((o - g + groups) % groups) * inner + c

    for j in range(experts, pieces):
        sp_copy(j).start()
    r.rows[0, :, span(mt), :] = r.outgoing[me]

    def spread(j):
        @pl.when(j >= experts)
        def _():
            sp_copy(j).wait_recv()

        for g in range(1, groups):
            across_in(j, g, mt).start()
        core_in(j, 0, mt).start()

    def relay(j):
        for g in range(1, groups):
            across_in(j, g, source(g)).wait_recv()
            core_in(j, g, source(g)).start()

    half = n_sp // 2

    def compute(j):
        @pl.when(j == half * experts)
        def _():
            for copy in weights:
                copy.wait()

        for g in range(groups):
            core_in(j, g, source(g)).wait_recv()
        e = j % experts
        rows = r.rows[j // experts, e]
        gate = jnp.dot(rows, r.gate_w[e], preferred_element_type=jnp.float32)
        upper = jnp.dot(rows, r.up_w[e], preferred_element_type=jnp.float32)
        middle = (gate / (1.0 + jnp.exp(-gate)) * upper).astype(jnp.bfloat16)
        r.part[j] = jnp.dot(middle, r.down_w[e], preferred_element_type=jnp.float32).astype(
            r.part.dtype
        )
        for g in list(range(1, groups)) + [0]:
            core_out(j, g).start()

    def pair_sum(j, g):
        row = ((o + g) % groups) * inner + c
        value = r.part[j, span(row), :].astype(jnp.float32)
        core_out(j, g).wait_recv()
        return value + r.from_core[j, g].astype(jnp.float32)

    def first(j):
        for g in range(1, groups):
            r.summed[j, g] = pair_sum(j, g).astype(r.summed.dtype)
            across_out(j, g).start()

    def second(j):
        value = pair_sum(j, 0)
        for g in range(1, groups):
            across_out(j, g).wait_recv()
            value = value + r.from_across[j, g].astype(jnp.float32)
        value = value.astype(r.total.dtype)

        @pl.when(j < experts)
        def _():
            r.returned[me, j] = value

        @pl.when(j >= experts)
        def _():
            r.total[j] = value
            sp_out(j).start()

    def far_first(n):
        k, e = n // experts, n % experts
        near = n_sp - 1 - k
        near = jnp.where(near > 1, half // 2 + n_sp - 1 - half - near, near)
        return jnp.where(k < half, k + half, near) * experts + e

    def turned(stage):
        return lambda n: stage(far_first(n))

    stages = (spread, relay) + tuple(turned(stage) for stage in (compute, first, second))
    ready = half * experts
    lags = (0, 3, ready + 4, ready + 6, ready + 9)

    def step(n, carry):
        for stage, lag in zip(stages, lags):

            @pl.when((n >= lag) & (n < pieces + lag))
            def _():
                stage(n - lag)

        return carry

    lax.fori_loop(0, pieces + lags[-1], step, 0)

    def arrive(j, carry):
        sp_out(j).wait_recv()
        return carry

    lax.fori_loop(experts, pieces, arrive, 0)
    share = r.residual.shape[0]
    width = r.residual.shape[1]
    tile = math.gcd(width, 512)
    for n in range(0, width, tile):
        at = slice(n, n + tile)
        both = jnp.dot(
            r.spread[...],
            r.returned[:, :, :, at].reshape(pieces * cap, tile),
            preferred_element_type=jnp.float32,
        )
        r.out_ref[:, at] = (r.hidden[:, at].astype(jnp.float32) + (both[:share] + both[share:])).astype(jnp.bfloat16)

    def drain(j, carry):
        @pl.when(j >= experts)
        def _():
            sp_out(j).wait_send()
            sp_copy(j).wait_send()

        for g in range(groups):
            if g:
                across_in(j, g, mt).wait_send()
                across_out(j, g).wait_send()
            core_in(j, g, mt).wait_send()
            core_out(j, g).wait_send()
        return carry

    lax.fori_loop(0, pieces, drain, 0)


def layer_kernel(n_sp, n_tp, names, *refs):
    r = types.SimpleNamespace(**dict(zip(names, refs)))
    me, mt = lax.axis_index("sp"), lax.axis_index("tp")
    inner = 2
    z, x = me // inner, me % inner
    barrier = pltpu.get_barrier_semaphore()
    lines = [(zz * inner + x, t) for zz in range(n_sp // inner) for t in range(n_tp)]
    lines += [(zz * inner + (1 - x), mt) for zz in range(n_sp // inner)]
    for sp, tp in lines:

        @pl.when((sp != me) | (tp != mt))
        def _():
            pl.semaphore_signal(
                barrier, inc=1, device_id={"sp": sp, "tp": tp}, device_id_type=MESH
            )

    def loads(pairs):
        copies = [
            pltpu.make_async_copy(getattr(r, src), getattr(r, dst), r.load_sem.at[k])
            for k, (src, dst) in pairs
        ]
        for copy in copies:
            copy.start()
        return copies

    pairs = list(enumerate(LOADED))
    first = loads(pairs[:5])
    middle = loads(pairs[5:7])
    last = loads(pairs[7:])
    for copy in first:
        copy.wait()

    def wait_middle():
        for copy in middle:
            copy.wait()

    experts, cap = r.outgoing.shape[1:3]
    attention_phase(
        n_sp,
        n_tp,
        r,
        lambda: pl.semaphore_wait(barrier, len(lines) - 1),
        lambda: routing_tables(r, n_sp * experts, cap),
    )
    token_phase(r, wait_middle)
    expert_phase(n_sp, n_tp, r, last)


LOADED = (
    ("k1_hbm", "k1_ref"),
    ("k2_hbm", "k2_ref"),
    ("v_hbm", "v_ref"),
    ("q1_hbm", "q1_ref"),
    ("q2_hbm", "q2_ref"),
    ("out_w_hbm", "out_w"),
    ("residual_hbm", "residual"),
    ("gate_hbm", "gate_w"),
    ("up_hbm", "up_w"),
    ("down_hbm", "down_w"),
)


def whole_layer(n_sp, n_tp, cap, big, lam, gain, norm, ids, logits, prob):
    k1, k2, v, q1, q2, out_w, residual, gate, up, down = big
    rows, keys = q1.shape
    length = n_sp // 2
    vd = v.shape[1] // 2
    cols = keys + vd
    share, width = residual.shape
    experts = gate.shape[0]
    pieces = n_sp * experts
    slots = pieces * cap
    groups = n_tp // 2
    bf16, f32 = jnp.bfloat16, jnp.float32
    vmem = pl.BlockSpec(memory_space=pltpu.VMEM)
    dma = pltpu.SemaphoreType.DMA
    piece = (experts, cap, width)
    scratch = [(dst, pltpu.VMEM(a.shape, a.dtype)) for (_, dst), a in zip(LOADED, big)]
    scratch += [
        ("token_ref", pltpu.VMEM((share, out_w.shape[0]), bf16)),
        ("kv_out", pltpu.VMEM((2, rows, cols), bf16)),
        ("q_out", pltpu.VMEM((2, rows, keys), bf16)),
        ("held", pltpu.VMEM((length, 2, rows, cols), bf16)),
        ("q_in", pltpu.VMEM((2, rows, keys), bf16)),
        ("qt", pltpu.VMEM((keys, 4 * rows), bf16)),
        ("m_ref", pltpu.VMEM((1, 4 * rows), f32)),
        ("l_ref", pltpu.VMEM((1, 4 * rows), f32)),
        ("acc_ref", pltpu.VMEM((vd, 4 * rows), f32)),
        ("stage", pltpu.VMEM((2, rows, vd), bf16)),
        ("lam_mine", pltpu.VMEM((8, 128), f32)),
        ("lam_far", pltpu.VMEM((8, 128), f32)),
        ("table", pltpu.VMEM((slots, share), bf16)),
        ("spread", pltpu.VMEM((2 * share, slots), bf16)),
        ("hidden", pltpu.VMEM((share, width), bf16)),
        ("outgoing", pltpu.VMEM((n_sp,) + piece, bf16)),
        ("returned", pltpu.VMEM((n_sp,) + piece, bf16)),
        ("rows", pltpu.VMEM((n_sp, experts, n_tp * cap, width), bf16)),
        ("part", pltpu.VMEM((pieces, n_tp * cap, width), bf16)),
        ("from_core", pltpu.VMEM((pieces, groups, cap, width), bf16)),
        ("from_across", pltpu.VMEM((pieces, groups, cap, width), bf16)),
        ("summed", pltpu.VMEM((pieces, groups, cap, width), bf16)),
        ("total", pltpu.VMEM((pieces, cap, width), bf16)),
        ("load_sem", dma((len(LOADED),))),
        ("first_send", dma((2, 2))),
        ("core_send", dma((length, 2))),
        ("side_send", dma((length,))),
        ("kv_recv", dma((length, 2))),
        ("q_recv", dma((2,))),
        ("lam_sem", dma((2,))),
        ("head_send", dma((2, n_tp))),
        ("head_recv", dma((2 * n_tp,))),
        ("sp_send", dma((pieces,))),
        ("sp_recv", dma((pieces,))),
        ("y_send", dma((groups, pieces))),
        ("y_recv", dma((groups, pieces))),
        ("c_send", dma((groups, pieces))),
        ("c_recv", dma((groups, pieces))),
        ("rc_send", dma((pieces, groups))),
        ("rc_recv", dma((pieces, groups))),
        ("ry_send", dma((pieces, groups))),
        ("ry_recv", dma((pieces, groups))),
        ("rs_send", dma((pieces,))),
        ("rs_recv", dma((pieces,))),
    ]
    small = ("gain_ref", "norm_ref", "ids_ref", "logits_ref", "prob_ref")
    names = [src for src, _ in LOADED] + ["lam_ref", *small, "out_ref"]
    names += [name for name, _ in scratch]
    return pl.pallas_call(
        functools.partial(layer_kernel, n_sp, n_tp, names),
        out_shape=jax.ShapeDtypeStruct((share, width), bf16),
        in_specs=[pl.BlockSpec(memory_space=pltpu.HBM)] * len(LOADED)
        + [pl.BlockSpec(memory_space=pltpu.SMEM)]
        + [vmem] * len(small),
        out_specs=vmem,
        scratch_shapes=[shape for _, shape in scratch],
        compiler_params=pltpu.CompilerParams(
            collective_id=3, has_side_effects=True, vmem_limit_bytes=LAYER_LIMIT
        ),
    )(*big, lam, gain, norm, ids, logits, prob)


def layers_fit(n_sp, n_tp, rows, vd, keys, heads, cap):
    square = heads == 2 and n_sp == 8 and n_tp == 4
    return square and rows % vd == 0 and vd == keys and vd % 128 == 0 and cap % 16 == 0


def on_device(
    n_sp,
    n_tp,
    query_one,
    key_one,
    query_two,
    key_two,
    values,
    mix_lambda,
    head_gain,
    residual_in,
    out_weight,
    norm_gain,
    route_ids,
    route_logits,
    group_prob,
    gate_weight,
    up_weight,
    down_weight,
):
    share = residual_in.shape[0]
    top_count = route_ids.shape[1]
    local_experts = gate_weight.shape[0]
    expert_count = local_experts * n_sp
    capacity = max(2, 2 * share * top_count // expert_count)
    if layers_fit(
        n_sp,
        n_tp,
        query_one.shape[0],
        values.shape[1] // 2,
        query_one.shape[1],
        mix_lambda.shape[0],
        capacity,
    ):
        big = (key_one, key_two, values, query_one, query_two, out_weight, residual_in)
        return whole_layer(
            n_sp,
            n_tp,
            capacity,
            big + (gate_weight, up_weight, down_weight),
            mix_lambda,
            head_gain[None, :],
            norm_gain[None, :],
            route_ids.T,
            route_logits.T,
            group_prob[None, :],
        )
    token_heads = attend(
        n_sp,
        n_tp,
        key_one,
        key_two,
        values,
        query_one,
        query_two,
        mix_lambda,
        head_gain[None, :],
    )
    mix = jnp.dot(token_heads, out_weight, preferred_element_type=jnp.float32)
    hidden_f = (residual_in.astype(jnp.float32) + mix).astype(jnp.bfloat16).astype(jnp.float32)
    normed = (
        hidden_f
        * lax.rsqrt(jnp.mean(hidden_f * hidden_f, axis=-1, keepdims=True) + norm_epsilon)
        * norm_gain
    ).astype(jnp.bfloat16)
    width = normed.shape[1]
    slots = expert_count * capacity
    flat_ids = route_ids.reshape(-1)
    one_hot = (flat_ids[:, None] == jnp.arange(expert_count, dtype=jnp.int32)[None, :]).astype(
        jnp.int32
    )
    earlier = jnp.cumsum(one_hot, axis=0) - one_hot
    rank = jnp.sum(earlier * one_hot, axis=1)
    slot_of = (flat_ids * capacity + rank).reshape(share, top_count)
    places = jnp.arange(slots, dtype=jnp.int32)
    table = sum(
        (places[:, None] == slot_of[None, :, k]).astype(jnp.bfloat16) for k in range(top_count)
    )
    outgoing = jnp.dot(table, normed, preferred_element_type=jnp.float32).astype(jnp.bfloat16)
    outgoing = outgoing.reshape(n_sp, local_experts, capacity, width)
    everyone = dispatch(n_sp, n_tp, outgoing).reshape(
        local_experts, n_tp * n_sp * capacity, width
    )
    gate = jnp.einsum("erd,edf->erf", everyone, gate_weight, preferred_element_type=jnp.float32)
    upper = jnp.einsum("erd,edf->erf", everyone, up_weight, preferred_element_type=jnp.float32)
    middle = (jax.nn.silu(gate) * upper).astype(jnp.bfloat16)
    part_sum = jnp.einsum(
        "erf,efd->erd", middle, down_weight, preferred_element_type=jnp.float32
    ).astype(jnp.bfloat16)
    returned = collect(
        n_sp, n_tp, part_sum.reshape(local_experts, n_tp, n_sp, capacity, width)
    ).reshape(slots, width)
    logits = [route_logits[:, k : k + 1] for k in range(top_count)]
    highest = functools.reduce(jnp.maximum, logits)
    powers = [jnp.exp(logit - highest) for logit in logits]
    route_weight = [power / sum(powers) * group_prob[:, None] for power in powers]
    spread = sum(
        jnp.where(places[None, :] == slot_of[:, k, None], route_weight[k], 0.0)
        for k in range(top_count)
    )
    high = spread.astype(jnp.bfloat16)
    low = (spread - high.astype(jnp.float32)).astype(jnp.bfloat16)
    both = jnp.dot(
        jnp.concatenate([high, low], axis=0), returned, preferred_element_type=jnp.float32
    )
    return (hidden_f + (both[:share] + both[share:])).astype(jnp.bfloat16)


def solution(mesh):
    in_specs = (
        P("sp", "tp"),
        P("sp", "tp"),
        P("sp", "tp"),
        P("sp", "tp"),
        P("sp", "tp"),
        P("tp"),
        P(),
        P(("sp", "tp"), None),
        P(),
        P(),
        P(("sp", "tp"), None),
        P(("sp", "tp"), None),
        P(("sp", "tp")),
        P("sp", None, "tp"),
        P("sp", None, "tp"),
        P("sp", "tp", None),
    )
    out_specs = P(("sp", "tp"), None)
    return jax.shard_map(
        functools.partial(on_device, mesh.shape["sp"], mesh.shape["tp"]),
        mesh=mesh,
        in_specs=in_specs,
        out_specs=out_specs,
        check_vma=False,
    )
```

```python
import functools
import math
import types

import jax
import jax.numpy as jnp
from jax import lax
from jax.experimental import pallas as pl
from jax.experimental.pallas import tpu as pltpu
from jax.sharding import PartitionSpec as P

norm_epsilon = 1e-06
MESH = pl.DeviceIdType.MESH
VMEM_LIMIT = 60 * 1024 * 1024
LAYER_LIMIT = VMEM_LIMIT


def pair_of(count):
    return 2 if count % 2 == 0 else 1


def greet(peers):
    barrier = pltpu.get_barrier_semaphore()
    for peer in peers:
        pl.semaphore_signal(barrier, inc=1, device_id=peer, device_id_type=MESH)
    pl.semaphore_wait(barrier, len(peers))


def attend_kernel(
    n_sp,
    n_tp,
    vd,
    k1_ref,
    k2_ref,
    v_ref,
    q1_ref,
    q2_ref,
    lam_ref,
    gain_ref,
    out_ref,
    kvp,
    qp,
    held,
    q_far,
    m_ref,
    l_ref,
    acc_ref,
    stage,
    cross_send,
    cross_recv,
    line_send,
    line_recv,
    side_send,
    side_recv,
    head_send,
    head_recv,
):
    inner = pair_of(n_sp)
    length = n_sp // inner
    half = length // 2
    me = lax.axis_index("sp")
    mt = lax.axis_index("tp")
    z, x = me // inner, me % inner
    head, zi = z // half, z % half
    rows = q1_ref.shape[0]
    qk = q1_ref.shape[1] // 2
    scale = 1.0 / math.sqrt(qk)
    exact = math.frexp(scale)[0] == 0.5
    early, after = (scale, 1.0) if exact else (1.0, scale)
    other = z * inner + (inner - 1 - x)
    mirror = (length - 1 - z) * inner + x
    far_zi = half - 1 - zi
    for h in range(2):
        kvp[h, :, 0:qk] = k1_ref[:, h * qk : (h + 1) * qk]
        kvp[h, :, qk : 2 * qk] = k2_ref[:, h * qk : (h + 1) * qk]
        kvp[h, :, 2 * qk : 2 * qk + vd] = v_ref[:, h * vd : (h + 1) * vd]
        qp[h, :, 0:qk] = q1_ref[:, h * qk : (h + 1) * qk] * jnp.bfloat16(early)
        qp[h, :, qk : 2 * qk] = q2_ref[:, h * qk : (h + 1) * qk] * jnp.bfloat16(early)

    def line_device(zz):
        return (head * half + zz) * inner + x

    peers = [{"sp": me, "tp": (mt + t) % n_tp} for t in range(1, n_tp)]
    peers += [{"sp": mirror, "tp": (mt + t) % n_tp} for t in range(n_tp)]
    if inner == 2:
        peers.append({"sp": other, "tp": mt})
    if half > 1:
        for shift in sorted({1, half - 1}):
            peers.append({"sp": line_device((zi + shift) % half), "tp": mt})
    greet(peers)

    def remote(src, dst, send, recv, sp):
        return pltpu.make_async_remote_copy(
            src_ref=src,
            dst_ref=dst,
            send_sem=send,
            recv_sem=recv,
            device_id={"sp": sp, "tp": mt},
            device_id_type=MESH,
        )

    cross_q = remote(qp.at[1 - head], q_far, cross_send.at[0], cross_recv.at[0], mirror)
    cross_kv = remote(
        kvp.at[1 - head], held.at[1, far_zi, x], cross_send.at[1], cross_recv.at[1], mirror
    )

    def line_copy(j, src, zz, way):
        ahead = jnp.clip(jnp.where(way == 0, zi + 1, zi - 1), 0, half - 1)
        return remote(
            src,
            held.at[j, zz, x],
            line_send.at[j, way, zz],
            line_recv.at[j, zz],
            line_device(ahead),
        )

    def side_copy(j, src, zz):
        return remote(src, held.at[j, zz, x], side_send.at[j, zz], side_recv.at[j, zz], other)

    def start_from(j, src):
        @pl.when(zi + 1 < half)
        def _():
            line_copy(j, src, zi, 0).start()

        @pl.when(zi > 0)
        def _():
            line_copy(j, src, zi, 1).start()

        if inner == 2:
            side_copy(j, src, zi).start()

    own = kvp.at[head]
    cross_kv.start()
    start_from(0, own)
    cross_q.start()
    m_ref[...] = jnp.full(m_ref.shape, -1e30, jnp.float32)
    l_ref[...] = jnp.zeros(l_ref.shape, jnp.float32)
    acc_ref[...] = jnp.zeros(acc_ref.shape, jnp.float32)

    def absorb(block, q_ref, group):
        vals = block[:, 2 * qk : 2 * qk + vd]
        for which in range(2):
            at = 2 * group + which
            scores = lax.dot_general(
                q_ref[:, which * qk : (which + 1) * qk],
                block[:, which * qk : (which + 1) * qk],
                (((1,), (1,)), ((), ())),
                preferred_element_type=jnp.float32,
            )
            if after != 1.0:
                scores = scores * after
            old = m_ref[at]
            new = jnp.maximum(old, jnp.max(scores, axis=1, keepdims=True))
            shrink = jnp.exp(old - new)
            expo = jnp.exp(scores - new[:, :1])
            m_ref[at] = new
            l_ref[at] = l_ref[at] * shrink + jnp.sum(expo, axis=1, keepdims=True)
            acc_ref[at] = acc_ref[at] * shrink[:, :1] + jnp.dot(
                expo.astype(jnp.bfloat16), vals, preferred_element_type=jnp.float32
            )

    q_own = qp.at[head]

    def absorb_both(block):
        absorb(block, q_own, 0)
        absorb(block, q_far, 1)

    def place(n):
        dist = (n + 1) // 2
        return jnp.where(n % 2 == 1, zi - dist, zi + dist), 1 - n % 2

    def line_steps(j, take):
        def line_step(n, carry):
            zz, way = place(n)

            @pl.when((zz >= 0) & (zz < half))
            def _():
                block = held.at[j, zz, x]
                line_copy(j, block, zz, way).wait_recv()
                ahead = jnp.where(way == 0, zi + 1, zi - 1)

                @pl.when((ahead >= 0) & (ahead < half))
                def _():
                    line_copy(j, block, zz, way).start()

                if inner == 2:
                    side_copy(j, block, zz).start()
                take(block)

            return carry

        lax.fori_loop(1, 2 * half - 1, line_step, 0)

    def line_again(j):
        def again(n, carry):
            zz, _ = place(n)

            @pl.when((zz >= 0) & (zz < half))
            def _():
                absorb(held.at[j, zz, x], q_far, 1)

            return carry

        lax.fori_loop(1, 2 * half - 1, again, 0)

    def side_steps(j, begin):
        def side_step(n, carry):
            zz, _ = place(n)

            @pl.when((zz >= 0) & (zz < half))
            def _():
                block = held.at[j, zz, 1 - x]
                side_copy(j, block, zz).wait_recv()
                absorb_both(block)

            return carry

        lax.fori_loop(begin, 2 * half - 1, side_step, 0)

    near = held.at[0, zi, 1 - x]
    far = held.at[1, zi, x]
    absorb(own, q_own, 0)
    if inner == 2:
        side_copy(0, near, zi).wait_recv()
        absorb(near, q_own, 0)
    line_steps(0, lambda block: absorb(block, q_own, 0))
    cross_kv.wait_recv()
    start_from(1, far)
    absorb(far, q_own, 0)
    cross_q.wait_recv()
    absorb(own, q_far, 1)
    absorb(far, q_far, 1)
    line_steps(1, absorb_both)
    line_again(0)
    if inner == 2:
        absorb(near, q_far, 1)
        side_steps(0, 1)
        side_steps(1, 0)

    share = rows // n_tp
    lam = lam_ref[head]
    columns = pl.ds(pl.multiple_of((mt * 2 + head) * vd, vd), vd)
    copies = []
    for group, sp in ((1, mirror), (0, me)):
        read_a = acc_ref[2 * group] / l_ref[2 * group][:, :1]
        read_b = acc_ref[2 * group + 1] / l_ref[2 * group + 1][:, :1]
        combined = read_a - lam * read_b
        combined = (
            combined
            * lax.rsqrt(jnp.mean(combined * combined, axis=-1, keepdims=True) + norm_epsilon)
            * gain_ref[...]
        )
        stage[group] = combined.astype(jnp.bfloat16)
        for t in range(n_tp):
            to = (mt + t) % n_tp
            span = pl.ds(pl.multiple_of(to * share, share), share)
            if group == 0 and t == 0:
                out_ref[:, columns] = stage[0, span, :]
                continue
            copy = pltpu.make_async_remote_copy(
                src_ref=stage.at[group, span],
                dst_ref=out_ref.at[:, columns],
                send_sem=head_send.at[group, t],
                recv_sem=head_recv.at[group, t],
                device_id={"sp": sp, "tp": to},
                device_id_type=MESH,
            )
            copy.start()
            copies.append(copy)

    cross_q.wait_send()
    cross_kv.wait_send()
    for j in range(2):

        def drain(n, carry):
            zz, way = place(n)

            @pl.when((zz >= 0) & (zz < half))
            def _():
                ahead = jnp.where(way == 0, zi + 1, zi - 1)

                @pl.when((ahead >= 0) & (ahead < half))
                def _():
                    line_copy(j, own, zz, way).wait_send()

                if inner == 2:
                    side_copy(j, own, zz).wait_send()

            return carry

        lax.fori_loop(1, 2 * half - 1, drain, 0)

        @pl.when(zi + 1 < half)
        def _():
            line_copy(j, own, zi, 0).wait_send()

        @pl.when(zi > 0)
        def _():
            line_copy(j, own, zi, 1).wait_send()

        if inner == 2:
            side_copy(j, own, zi).wait_send()
    for copy in copies:
        copy.wait()


def attend(n_sp, n_tp, k1, k2, v, q1, q2, lam, gain):
    rows = q1.shape[0]
    inner = pair_of(n_sp)
    half = n_sp // inner // 2
    assert lam.shape[0] == 2 and half * inner * 2 == n_sp
    vd = v.shape[1] // 2
    qk = q1.shape[1] // 2
    cols = 2 * qk + vd
    vmem = pl.BlockSpec(memory_space=pltpu.VMEM)
    dma = pltpu.SemaphoreType.DMA
    return pl.pallas_call(
        functools.partial(attend_kernel, n_sp, n_tp, vd),
        out_shape=jax.ShapeDtypeStruct((rows // n_tp, n_tp * 2 * vd), jnp.bfloat16),
        in_specs=[vmem] * 5 + [pl.BlockSpec(memory_space=pltpu.SMEM), vmem],
        out_specs=vmem,
        scratch_shapes=[
            pltpu.VMEM((2, rows, cols), jnp.bfloat16),
            pltpu.VMEM((2, rows, 2 * qk), jnp.bfloat16),
            pltpu.VMEM((2, half, inner, rows, cols), jnp.bfloat16),
            pltpu.VMEM((rows, 2 * qk), jnp.bfloat16),
            pltpu.VMEM((4, rows, 128), jnp.float32),
            pltpu.VMEM((4, rows, 128), jnp.float32),
            pltpu.VMEM((4, rows, vd), jnp.float32),
            pltpu.VMEM((2, rows, vd), jnp.bfloat16),
            dma((2,)),
            dma((2,)),
            dma((2, 2, half)),
            dma((2, half)),
            dma((2, half)),
            dma((2, half)),
            dma((2, n_tp)),
            dma((2, n_tp)),
        ],
        compiler_params=pltpu.CompilerParams(
            collective_id=0, has_side_effects=True, vmem_limit_bytes=VMEM_LIMIT
        ),
    )(k1, k2, v, q1, q2, lam, gain)


def tp_peers(n_tp):
    inner = pair_of(n_tp)
    mt = lax.axis_index("tp")
    o, c = mt // inner, mt % inner
    across = [((o + d) % (n_tp // inner)) * inner + c for d in range(1, n_tp // inner)]
    return inner, across, o * inner + (inner - 1 - c)


def greet_all(n_sp, n_tp):
    me, mt = lax.axis_index("sp"), lax.axis_index("tp")
    inner, across, partner = tp_peers(n_tp)
    peers = [{"sp": (me + s) % n_sp, "tp": mt} for s in range(1, n_sp)]
    peers += [{"sp": me, "tp": t} for t in across]
    if inner == 2:
        peers.append({"sp": me, "tp": partner})
    greet(peers)


def dispatch_kernel(
    n_sp, n_tp, rows_ref, out_ref, sp_send, sp_recv, y_send, y_recv, c_send, c_recv, own_sem
):
    me, mt = lax.axis_index("sp"), lax.axis_index("tp")
    inner, across, partner = tp_peers(n_tp)
    groups = n_tp // inner
    o = mt // inner
    greet_all(n_sp, n_tp)

    def sp_copy(d):
        to = (me + d) % n_sp
        return pltpu.make_async_remote_copy(
            src_ref=rows_ref.at[to],
            dst_ref=out_ref.at[:, mt, me],
            send_sem=sp_send.at[d],
            recv_sem=sp_recv.at[d],
            device_id={"sp": to, "tp": mt},
            device_id_type=MESH,
        )

    def tp_copy(t, s, to, send, recv):
        return pltpu.make_async_remote_copy(
            src_ref=out_ref.at[:, t, s],
            dst_ref=out_ref.at[:, t, s],
            send_sem=send,
            recv_sem=recv,
            device_id={"sp": me, "tp": to},
            device_id_type=MESH,
        )

    order = sorted(range(1, n_sp), key=lambda d: min(d, n_sp - d))
    for d in reversed(order):
        sp_copy(d).start()
    own = pltpu.make_async_copy(rows_ref.at[me], out_ref.at[:, mt, me], own_sem)
    own.start()
    own.wait()
    started = []

    def spread(d):
        s = (me - d + n_sp) % n_sp
        for g in range(1, groups):
            copy = tp_copy(mt, s, across[g - 1], y_send.at[g, d], y_recv.at[g, d])
            copy.start()
            started.append(copy)
        if inner == 2:
            copy = tp_copy(mt, s, partner, c_send.at[0, d], c_recv.at[0, d])
            copy.start()
            started.append(copy)

    def relay(d):
        s = (me - d + n_sp) % n_sp
        for g in range(1, groups):
            source = ((o - g + groups) % groups) * inner + mt % inner
            tp_copy(source, s, partner, y_send.at[g, d], y_recv.at[g, d]).wait_recv()
            if inner == 2:
                copy = tp_copy(source, s, partner, c_send.at[g, d], c_recv.at[g, d])
                copy.start()
                started.append(copy)

    order = order[::-1]
    sequence = [0] + order
    spread(0)
    for i, d in enumerate(order):
        sp_copy(d).wait_recv()
        spread(d)
        relay(sequence[i])
    relay(sequence[-1])
    for d in range(n_sp):
        s = (me - d + n_sp) % n_sp
        if inner == 2:
            for g in range(groups):
                source = ((o - g + groups) % groups) * inner + (1 - mt % inner)
                tp_copy(source, s, partner, c_send.at[g, d], c_recv.at[g, d]).wait_recv()
    for copy in started:
        copy.wait_send()
    for d in order:
        sp_copy(d).wait_send()


def dispatch(n_sp, n_tp, rows):
    _, experts, cap, width = rows.shape
    groups = n_tp // pair_of(n_tp)
    sem = pltpu.SemaphoreType.DMA
    hbm = pl.BlockSpec(memory_space=pltpu.VMEM)
    return pl.pallas_call(
        functools.partial(dispatch_kernel, n_sp, n_tp),
        out_shape=jax.ShapeDtypeStruct((experts, n_tp, n_sp, cap, width), rows.dtype),
        in_specs=[hbm],
        out_specs=pl.BlockSpec(memory_space=pl.ANY),
        scratch_shapes=[
            sem((n_sp,)),
            sem((n_sp,)),
            sem((groups, n_sp)),
            sem((groups, n_sp)),
            sem((groups, n_sp)),
            sem((groups, n_sp)),
            sem,
        ],
        compiler_params=pltpu.CompilerParams(
            collective_id=1, has_side_effects=True, vmem_limit_bytes=VMEM_LIMIT
        ),
    )(rows)


def collect_kernel(
    n_sp,
    n_tp,
    part_ref,
    out_ref,
    from_core,
    from_across,
    summed,
    total,
    c_send,
    c_recv,
    y_send,
    y_recv,
    sp_send,
    sp_recv,
):
    me, mt = lax.axis_index("sp"), lax.axis_index("tp")
    inner, across, partner = tp_peers(n_tp)
    groups = n_tp // inner
    o, c = mt // inner, mt % inner
    greet_all(n_sp, n_tp)
    order = sorted(range(1, n_sp), key=lambda d: min(d, n_sp - d), reverse=True) + [0]

    def to_of(d):
        return (me + d) % n_sp

    def core_copy(d, g):
        row = ((o + g) % groups) * inner + (inner - 1 - c)
        return pltpu.make_async_remote_copy(
            src_ref=part_ref.at[:, row, to_of(d)],
            dst_ref=from_core.at[d, g],
            send_sem=c_send.at[d, g],
            recv_sem=c_recv.at[d, g],
            device_id={"sp": me, "tp": partner},
            device_id_type=MESH,
        )

    def across_copy(d, g):
        return pltpu.make_async_remote_copy(
            src_ref=summed.at[d, g],
            dst_ref=from_across.at[d, g],
            send_sem=y_send.at[d, g],
            recv_sem=y_recv.at[d, g],
            device_id={"sp": me, "tp": across[g - 1]},
            device_id_type=MESH,
        )

    def sp_copy(d):
        return pltpu.make_async_remote_copy(
            src_ref=total.at[d],
            dst_ref=out_ref.at[me],
            send_sem=sp_send.at[d],
            recv_sem=sp_recv.at[d],
            device_id={"sp": to_of(d), "tp": mt},
            device_id_type=MESH,
        )

    if inner == 2:
        for d in order:
            for g in list(range(1, groups)) + [0]:
                core_copy(d, g).start()

    def pair_sum(d, g):
        row = ((o + g) % groups) * inner + c
        value = part_ref[:, row, to_of(d)].astype(jnp.float32)
        if inner == 2:
            core_copy(d, g).wait_recv()
            value = value + from_core[d, g].astype(jnp.float32)
        return value

    def first(d):
        for g in range(1, groups):
            summed[d, g] = pair_sum(d, g).astype(summed.dtype)
            across_copy(d, g).start()

    def second(d):
        value = pair_sum(d, 0)
        for g in range(1, groups):
            across_copy(d, g).wait_recv()
            value = value + from_across[d, g].astype(jnp.float32)
        value = value.astype(total.dtype)
        if d == 0:
            out_ref[me] = value
        else:
            total[d] = value
            sp_copy(d).start()

    ahead = min(3, n_sp)
    for d in order[:ahead]:
        first(d)
    for i, d in enumerate(order):
        second(d)
        if i + ahead < n_sp:
            first(order[i + ahead])
    for d in range(1, n_sp):
        sp_copy(d).wait_recv()
    for d in range(n_sp):
        if d:
            sp_copy(d).wait_send()
        for g in range(groups):
            if g:
                across_copy(d, g).wait_send()
            if inner == 2:
                core_copy(d, g).wait_send()


def collect(n_sp, n_tp, part):
    experts, _, _, cap, width = part.shape
    groups = n_tp // pair_of(n_tp)
    sem = pltpu.SemaphoreType.DMA
    vmem = pl.BlockSpec(memory_space=pltpu.VMEM)
    piece = (experts, cap, width)
    return pl.pallas_call(
        functools.partial(collect_kernel, n_sp, n_tp),
        out_shape=jax.ShapeDtypeStruct((n_sp,) + piece, part.dtype),
        in_specs=[vmem],
        out_specs=vmem,
        scratch_shapes=[
            pltpu.VMEM((n_sp, groups) + piece, part.dtype),
            pltpu.VMEM((n_sp, groups) + piece, part.dtype),
            pltpu.VMEM((n_sp, groups) + piece, part.dtype),
            pltpu.VMEM((n_sp,) + piece, part.dtype),
            sem((n_sp, groups)),
            sem((n_sp, groups)),
            sem((n_sp, groups)),
            sem((n_sp, groups)),
            sem((n_sp,)),
            sem((n_sp,)),
        ],
        compiler_params=pltpu.CompilerParams(
            collective_id=2, has_side_effects=True, vmem_limit_bytes=VMEM_LIMIT
        ),
    )(part)


def attention_phase(n_sp, n_tp, r, arrived, filler):
    inner, pair = 2, 2
    length = n_sp // inner
    me, mt = lax.axis_index("sp"), lax.axis_index("tp")
    z, x = me // inner, me % inner
    y, c = mt // pair, mt % pair
    rows, qk = r.q1_ref.shape[0], r.q1_ref.shape[1] // 2
    vd = r.v_ref.shape[1] // 2
    keys = 2 * qk
    scale = 1.0 / math.sqrt(qk)
    exact = math.frexp(scale)[0] == 0.5
    early, after = (scale, 1.0) if exact else (1.0, scale)
    home = c == z // pair
    partner = y * pair + (1 - c)
    across = z * inner + (1 - x)

    def spot(zz):
        return zz * inner + x

    for h in range(2):
        at = slice(h * qk, (h + 1) * qk)
        block = jnp.concatenate([r.k1_ref[:, at], r.k2_ref[:, at]], axis=1)
        turned = jnp.concatenate(
            [
                r.v_ref[base : base + vd, h * vd : (h + 1) * vd].astype(jnp.float32).T
                for base in range(0, rows, vd)
            ],
            axis=0,
        ).astype(jnp.bfloat16)
        query = jnp.concatenate([r.q1_ref[:, at], r.q2_ref[:, at]], axis=1) * jnp.bfloat16(early)
        r.kv_out[h, :, 0:keys] = block
        r.kv_out[h, :, keys : keys + vd] = turned
        r.q_out[h] = query

        @pl.when(z == pair * c + h)
        def _():
            r.held[z, 0, :, 0:keys] = block
            r.held[z, 0, :, keys : keys + vd] = turned
            r.q_in[h] = query

    r.lam_mine[...] = jnp.full(r.lam_mine.shape, r.lam_ref[z % pair], jnp.float32)
    r.m_ref[...] = jnp.full(r.m_ref.shape, -1e30, jnp.float32)
    r.l_ref[...] = jnp.zeros(r.l_ref.shape, jnp.float32)
    r.acc_ref[...] = jnp.zeros(r.acc_ref.shape, jnp.float32)
    r.qt[...] = jnp.zeros(r.qt.shape, r.qt.dtype)
    arrived()

    def remote(src, dst, send, recv, sp, tp):
        return pltpu.make_async_remote_copy(
            src_ref=src,
            dst_ref=dst,
            send_sem=send,
            recv_sem=recv,
            device_id={"sp": sp, "tp": tp},
            device_id_type=MESH,
        )

    def first_q(h):
        return remote(
            r.q_out.at[h],
            r.q_in.at[z % pair],
            r.first_send.at[0, h],
            r.q_recv.at[z % pair],
            spot(pair * c + h),
            y * pair + z // pair,
        )

    def first_kv(h):
        return remote(
            r.kv_out.at[h],
            r.held.at[z, 0],
            r.first_send.at[1, h],
            r.kv_recv.at[z, 0],
            spot(pair * c + h),
            y * pair + z // pair,
        )

    def to_core(zz, side):
        block = r.held.at[zz, side]
        return remote(block, block, r.core_send.at[zz, side], r.kv_recv.at[zz, side], me, partner)

    def to_side(zz):
        return remote(
            r.held.at[zz, 0], r.held.at[zz, 1], r.side_send.at[zz], r.kv_recv.at[zz, 1], across, mt
        )

    lam_copy = remote(r.lam_mine, r.lam_far, r.lam_sem.at[0], r.lam_sem.at[1], me, partner)

    def away(h):
        return z != pair * c + h

    order = [z, z + 1 - 2 * (z % pair), pair - z // pair, (length - 1) * (1 - z // pair)]

    @pl.when(home)
    def _():
        to_side(z).start()
        to_core(z, 0).start()

    for h in range(2):

        @pl.when(away(h))
        def _():
            first_q(h).start()

    for h in range(2):

        @pl.when(away(h))
        def _():
            first_kv(h).start()

    lam_copy.start()
    filler()

    for g in range(2):

        @pl.when((z != pair * c + g))
        def _():
            remote(
                r.q_out.at[g], r.q_in.at[g], r.first_send.at[0, g], r.q_recv.at[g], me, mt
            ).wait_recv()

        turned = r.q_in[g].astype(jnp.float32).T.astype(jnp.bfloat16)
        r.qt[0:qk, 2 * g * rows : (2 * g + 1) * rows] = turned[0:qk]
        r.qt[qk:keys, (2 * g + 1) * rows : (2 * g + 2) * rows] = turned[qk:keys]

    def absorb(zz, side):
        block_keys = r.held[zz, side, :, 0:keys]
        turned = jnp.concatenate(
            [r.held[zz, side, base : base + vd, keys : keys + vd] for base in range(0, rows, vd)], axis=1
        )
        for part in range(4):
            at = slice(part * rows, (part + 1) * rows)
            scores = jnp.dot(block_keys, r.qt[:, at], preferred_element_type=jnp.float32)
            if after != 1.0:
                scores = scores * after
            old = r.m_ref[:, at]
            new = jnp.maximum(old, jnp.max(scores, axis=0, keepdims=True))
            shrink = jnp.exp(old - new)
            expo = jnp.exp(scores - new)
            r.m_ref[:, at] = new
            r.l_ref[:, at] = r.l_ref[:, at] * shrink + jnp.sum(expo, axis=0, keepdims=True)
            r.acc_ref[:, at] = r.acc_ref[:, at] * shrink + jnp.dot(
                turned, expo.astype(jnp.bfloat16), preferred_element_type=jnp.float32
            )

    near_first = ((0, 0), (0, 1), (1, 0), (1, 1), (2, 0), (3, 0), (2, 1), (3, 1))
    far_first = ((0, 0), (0, 1), (1, 0), (2, 0), (1, 1), (3, 0), (2, 1), (3, 1))

    def pick(values, n):
        result = values[0]
        for k in range(1, len(values)):
            result = jnp.where(n == k, values[k], result)
        return result

    def step(n, carry):
        at_home = [pick([p[i] for p in near_first], n) for i in range(2)]
        at_far = [pick([p[i] for p in far_first], n) for i in range(2)]
        zz = pick(order, jnp.where(home, at_home[0], at_far[0]))
        side = jnp.where(home, at_home[1], at_far[1])
        direct = zz // pair == c
        local = home & (n == 0)

        @pl.when(jnp.logical_not(local))
        def _():
            to_core(zz, side).wait_recv()

            @pl.when(direct & (side == 0))
            def _():
                to_side(zz).start()

            @pl.when(direct)
            def _():
                to_core(zz, side).start()

        absorb(zz, side)
        return carry

    lax.fori_loop(0, 2 * length, step, 0)

    share = rows // n_tp
    lam_copy.wait()
    lam = jnp.where(home, r.lam_mine[0:1, 0:1], r.lam_far[0:1, 0:1])
    head = y * length + z
    columns = pl.ds(pl.multiple_of(head * vd, vd), vd)

    def piece(g, t):
        to = (mt + t) % n_tp
        span = pl.ds(pl.multiple_of(to * share, share), share)
        return remote(
            r.stage.at[g, span],
            r.token_ref.at[:, columns],
            r.head_send.at[g, t],
            r.head_recv.at[head],
            spot(pair * c + g),
            to,
        )

    def own(g):
        return z == pair * c + g

    for g in (1, 0):
        reads = []
        for which in range(2):
            at = slice((2 * g + which) * rows, (2 * g + which + 1) * rows)
            reads.append(r.acc_ref[:, at] / r.l_ref[:, at])
        combined = reads[0] - lam * reads[1]
        combined = combined * lax.rsqrt(
            jnp.mean(combined * combined, axis=0, keepdims=True) + norm_epsilon
        )
        r.stage[g] = (combined.T * r.gain_ref[...]).astype(jnp.bfloat16)
        for t in range(1, n_tp):
            piece(g, t).start()

        @pl.when(own(g))
        def _():
            r.token_ref[:, columns] = r.stage[g, pl.ds(pl.multiple_of(mt * share, share), share), :]

        @pl.when(jnp.logical_not(own(g)))
        def _():
            piece(g, 0).start()

    def head_copy(hd):
        at = pl.ds(pl.multiple_of(hd * vd, vd), vd)
        return remote(
            r.stage.at[0, 0:share], r.token_ref.at[:, at], r.head_send.at[0, 0], r.head_recv.at[hd], me, mt
        )

    for hd in range(2 * n_tp):

        @pl.when((hd != head) | jnp.logical_not(home))
        def _():
            head_copy(hd).wait_recv()

    def finish():
        for g in range(2):
            for t in range(1, n_tp):
                piece(g, t).wait_send()

            @pl.when(jnp.logical_not(own(g)))
            def _():
                piece(g, 0).wait_send()

            @pl.when(away(g))
            def _():
                first_q(g).wait_send()
                first_kv(g).wait_send()

        for zz in range(length):

            @pl.when(c == zz // pair)
            def _():
                to_side(zz).wait_send()
                to_core(zz, 0).wait_send()
                to_core(zz, 1).wait_send()

    return finish


def routing_tables(r, experts_in_all, cap):
    ids = r.ids_ref[...].astype(jnp.float32)
    top, share = ids.shape
    names = lax.broadcasted_iota(jnp.int32, (experts_in_all, share), 0).astype(jnp.float32)
    before = lax.broadcasted_iota(jnp.int32, (share, share), 0)
    before = before < lax.broadcasted_iota(jnp.int32, (share, share), 1)
    before = before.astype(jnp.float32).astype(jnp.bfloat16)
    taken = jnp.zeros((experts_in_all, 1), jnp.float32)
    places = lax.broadcasted_iota(jnp.int32, (experts_in_all * cap, share), 0).astype(jnp.float32)
    logits = [r.logits_ref[k : k + 1, :] for k in range(top)]
    highest = functools.reduce(jnp.maximum, logits)
    powers = [jnp.exp(logit - highest) for logit in logits]
    total = sum(powers)
    table = jnp.zeros(places.shape, jnp.float32)
    spread = jnp.zeros(places.shape, jnp.float32)
    for k in range(top):
        hit = (names == ids[k : k + 1, :]).astype(jnp.float32)
        earlier = jnp.dot(hit.astype(jnp.bfloat16), before, preferred_element_type=jnp.float32)
        rank = jnp.sum(hit * (earlier + taken), axis=0, keepdims=True)
        taken = taken + jnp.sum(hit, axis=1, keepdims=True)
        placed = (places == ids[k : k + 1, :] * cap + rank).astype(jnp.float32)
        table = table + placed
        spread = spread + placed * (powers[k] / total * r.prob_ref[...])
    r.table[...] = table.astype(jnp.bfloat16)
    turned = spread.T
    high = turned.astype(jnp.bfloat16)
    r.spread[0:share] = high
    r.spread[share : 2 * share] = (turned - high.astype(jnp.float32)).astype(jnp.bfloat16)


def token_phase(r, wait_weights):
    share, width = r.residual.shape
    tile = math.gcd(width, 512)
    columns = [slice(n, n + tile) for n in range(0, width, tile)]
    wait_weights()
    square = jnp.zeros((share, 1), jnp.float32)
    for at in columns:
        mix = jnp.dot(r.token_ref[...], r.out_w[:, at], preferred_element_type=jnp.float32)
        hidden = (r.residual[:, at].astype(jnp.float32) + mix).astype(jnp.bfloat16)
        r.hidden[:, at] = hidden
        hidden = hidden.astype(jnp.float32)
        square = square + jnp.sum(hidden * hidden, axis=1, keepdims=True)
    factor = lax.rsqrt(square / width + norm_epsilon)
    n_sp, experts, cap = r.outgoing.shape[:3]
    for at in columns:
        normed = r.hidden[:, at].astype(jnp.float32) * factor * r.norm_ref[:, at]
        rows = jnp.dot(
            r.table[...], normed.astype(jnp.bfloat16), preferred_element_type=jnp.float32
        ).astype(jnp.bfloat16)
        r.outgoing[:, :, :, at] = rows.reshape(n_sp, experts, cap, tile)


def expert_phase(n_sp, n_tp, r, weights, finish):
    me, mt = lax.axis_index("sp"), lax.axis_index("tp")
    inner_sp = 2
    z, x = me // inner_sp, me % inner_sp
    inner, across, partner = tp_peers(n_tp)
    groups = n_tp // inner
    o, c = mt // inner, mt % inner
    _, experts, cap, _ = r.outgoing.shape

    def flip(number, by):
        low = (number % 2 + by % 2) % 2
        return (number // 2 + by // 2) % 2 * 2 + low

    def peer_of(i):
        return flip(z, i // inner_sp) * inner_sp + flip(x, i % inner_sp)

    def span(t):
        return pl.ds(pl.multiple_of(t * cap, cap), cap)

    def remote(src, dst, send, recv, sp, tp):
        return pltpu.make_async_remote_copy(
            src_ref=src,
            dst_ref=dst,
            send_sem=send,
            recv_sem=recv,
            device_id={"sp": sp, "tp": tp},
            device_id_type=MESH,
        )

    pieces = n_sp * experts

    def sp_copy(j):
        i, e = j // experts, j % experts
        to = peer_of(i)
        block = r.rows.at[i, e, span(mt)]
        return remote(r.outgoing.at[to, e], block, r.sp_send.at[j], r.sp_recv.at[j], to, mt)

    def across_in(j, g, t):
        block = r.rows.at[j // experts, j % experts, span(t)]
        return remote(block, block, r.y_send.at[g, j], r.y_recv.at[g, j], me, across[g - 1])

    def core_in(j, g, t):
        block = r.rows.at[j // experts, j % experts, span(t)]
        return remote(block, block, r.c_send.at[g, j], r.c_recv.at[g, j], me, partner)

    def core_out(j, g):
        row = ((o + g) % groups) * inner + (inner - 1 - c)
        block = r.part.at[j, span(row)]
        return remote(
            block, r.from_core.at[j, g], r.rc_send.at[j, g], r.rc_recv.at[j, g], me, partner
        )

    def across_out(j, g):
        return remote(
            r.summed.at[j, g],
            r.from_across.at[j, g],
            r.ry_send.at[j, g],
            r.ry_recv.at[j, g],
            me,
            across[g - 1],
        )

    def sp_out(j):
        i, e = j // experts, j % experts
        block = r.returned.at[me, e]
        return remote(r.total.at[j], block, r.rs_send.at[j], r.rs_recv.at[j], peer_of(i), mt)

    def source(g):
        return ((o - g + groups) % groups) * inner + c

    for j in (2, 8, 4, 3, 9, 5, 10, 6, 11, 7, 12, 13, 14, 15):
        sp_copy(j).start()
    r.rows[0, :, span(mt), :] = r.outgoing[me]

    def spread(j):
        @pl.when(j >= experts)
        def _():
            sp_copy(j).wait_recv()

        for g in range(1, groups):
            across_in(j, g, mt).start()
        core_in(j, 0, mt).start()

    def relay(j):
        for g in range(1, groups):
            across_in(j, g, source(g)).wait_recv()
            core_in(j, g, source(g)).start()

    half = n_sp // 2
    ready = half * experts

    def compute(j):
        @pl.when(j == ready)
        def _():
            for copy in weights:
                copy.wait()

        for g in range(groups):
            core_in(j, g, source(g)).wait_recv()
        e = j % experts
        rows = r.rows[j // experts, e]
        gate = jnp.dot(rows, r.gate_w[e], preferred_element_type=jnp.float32)
        upper = jnp.dot(rows, r.up_w[e], preferred_element_type=jnp.float32)
        middle = (gate / (1.0 + jnp.exp(-gate)) * upper).astype(jnp.bfloat16)
        r.part[j] = jnp.dot(middle, r.down_w[e], preferred_element_type=jnp.float32).astype(
            r.part.dtype
        )
        for g in list(range(1, groups)) + [0]:
            core_out(j, g).start()

    def pair_sum(j, g):
        row = ((o + g) % groups) * inner + c
        value = r.part[j, span(row), :].astype(jnp.float32)
        core_out(j, g).wait_recv()
        return value + r.from_core[j, g].astype(jnp.float32)

    def first(j):
        for g in range(1, groups):
            r.summed[j, g] = pair_sum(j, g).astype(r.summed.dtype)
            across_out(j, g).start()

    def second(j):
        value = pair_sum(j, 0)
        for g in range(1, groups):
            across_out(j, g).wait_recv()
            value = value + r.from_across[j, g].astype(jnp.float32)
        value = value.astype(r.total.dtype)

        @pl.when(j < experts)
        def _():
            r.returned[me, j] = value

        @pl.when(j >= experts)
        def _():
            r.total[j] = value
            sp_out(j).start()

    def far_first(n):
        near = jnp.where(n < ready + half, n - half, jnp.where(n < ready + 6, n - 10, n - 14))
        return jnp.where(n < ready, n + ready, near)

    def arrival(n):
        mixed = n // 2 + jnp.where(n % 2 == 0, 6, 2)
        return jnp.where((n < half) | (n >= ready + half), n, mixed)

    def turned(stage):
        return lambda n: stage(far_first(n))

    stages = tuple((lambda n, f=f: f(arrival(n))) for f in (spread, relay)) + tuple(turned(stage) for stage in (compute, first, second))
    lags = (0, 3, 12, 14, 17)

    def step(n, carry):
        for stage, lag in zip(stages, lags):

            @pl.when((n >= lag) & (n < pieces + lag))
            def _():
                stage(n - lag)

        return carry

    lax.fori_loop(0, pieces + lags[-1], step, 0)

    finish()

    def drain(j, carry):
        @pl.when(j >= experts)
        def _():
            sp_out(j).wait_send()
            sp_copy(j).wait_send()

        for g in range(groups):
            if g:
                across_in(j, g, mt).wait_send()
                across_out(j, g).wait_send()
            core_in(j, g, mt).wait_send()
            core_out(j, g).wait_send()
        return carry

    lax.fori_loop(0, pieces, drain, 0)

    def arrive(j, carry):
        sp_out(j).wait_recv()
        return carry

    lax.fori_loop(experts, pieces, arrive, 0)
    share = r.residual.shape[0]
    width = r.residual.shape[1]
    tile = math.gcd(width, 512)
    for n in range(0, width, tile):
        at = slice(n, n + tile)
        both = jnp.dot(
            r.spread[...],
            r.returned[:, :, :, at].reshape(pieces * cap, tile),
            preferred_element_type=jnp.float32,
        )
        r.out_ref[:, at] = (r.hidden[:, at].astype(jnp.float32) + (both[:share] + both[share:])).astype(jnp.bfloat16)


def layer_kernel(n_sp, n_tp, names, *refs):
    r = types.SimpleNamespace(**dict(zip(names, refs)))
    me, mt = lax.axis_index("sp"), lax.axis_index("tp")
    inner = 2
    z, x = me // inner, me % inner
    barrier = pltpu.get_barrier_semaphore()
    lines = [(zz * inner + x, t) for zz in range(n_sp // inner) for t in range(n_tp)]
    lines += [(zz * inner + (1 - x), mt) for zz in range(n_sp // inner)]
    for sp, tp in lines:

        @pl.when((sp != me) | (tp != mt))
        def _():
            pl.semaphore_signal(
                barrier, inc=1, device_id={"sp": sp, "tp": tp}, device_id_type=MESH
            )

    def loads(pairs):
        copies = [
            pltpu.make_async_copy(getattr(r, src), getattr(r, dst), r.load_sem.at[k])
            for k, (src, dst) in pairs
        ]
        for copy in copies:
            copy.start()
        return copies

    pairs = list(enumerate(LOADED))
    first = loads(pairs[:5])
    middle = loads(pairs[5:7])
    last = loads(pairs[7:])
    for copy in first:
        copy.wait()

    def wait_middle():
        for copy in middle:
            copy.wait()

    experts, cap = r.outgoing.shape[1:3]
    finish = attention_phase(
        n_sp,
        n_tp,
        r,
        lambda: pl.semaphore_wait(barrier, len(lines) - 1),
        lambda: routing_tables(r, n_sp * experts, cap),
    )
    token_phase(r, wait_middle)
    expert_phase(n_sp, n_tp, r, last, finish)


LOADED = (
    ("k1_hbm", "k1_ref"),
    ("k2_hbm", "k2_ref"),
    ("v_hbm", "v_ref"),
    ("q1_hbm", "q1_ref"),
    ("q2_hbm", "q2_ref"),
    ("out_w_hbm", "out_w"),
    ("residual_hbm", "residual"),
    ("gate_hbm", "gate_w"),
    ("up_hbm", "up_w"),
    ("down_hbm", "down_w"),
)


def whole_layer(n_sp, n_tp, cap, big, lam, gain, norm, ids, logits, prob):
    k1, k2, v, q1, q2, out_w, residual, gate, up, down = big
    rows, keys = q1.shape
    length = n_sp // 2
    vd = v.shape[1] // 2
    cols = keys + vd
    share, width = residual.shape
    experts = gate.shape[0]
    pieces = n_sp * experts
    slots = pieces * cap
    groups = n_tp // 2
    bf16, f32 = jnp.bfloat16, jnp.float32
    vmem = pl.BlockSpec(memory_space=pltpu.VMEM)
    dma = pltpu.SemaphoreType.DMA
    piece = (experts, cap, width)
    scratch = [(dst, pltpu.VMEM(a.shape, a.dtype)) for (_, dst), a in zip(LOADED, big)]
    scratch += [
        ("token_ref", pltpu.VMEM((share, out_w.shape[0]), bf16)),
        ("kv_out", pltpu.VMEM((2, rows, cols), bf16)),
        ("q_out", pltpu.VMEM((2, rows, keys), bf16)),
        ("held", pltpu.VMEM((length, 2, rows, cols), bf16)),
        ("q_in", pltpu.VMEM((2, rows, keys), bf16)),
        ("qt", pltpu.VMEM((keys, 4 * rows), bf16)),
        ("m_ref", pltpu.VMEM((1, 4 * rows), f32)),
        ("l_ref", pltpu.VMEM((1, 4 * rows), f32)),
        ("acc_ref", pltpu.VMEM((vd, 4 * rows), f32)),
        ("stage", pltpu.VMEM((2, rows, vd), bf16)),
        ("lam_mine", pltpu.VMEM((8, 128), f32)),
        ("lam_far", pltpu.VMEM((8, 128), f32)),
        ("table", pltpu.VMEM((slots, share), bf16)),
        ("spread", pltpu.VMEM((2 * share, slots), bf16)),
        ("hidden", pltpu.VMEM((share, width), bf16)),
        ("outgoing", pltpu.VMEM((n_sp,) + piece, bf16)),
        ("returned", pltpu.VMEM((n_sp,) + piece, bf16)),
        ("rows", pltpu.VMEM((n_sp, experts, n_tp * cap, width), bf16)),
        ("part", pltpu.VMEM((pieces, n_tp * cap, width), bf16)),
        ("from_core", pltpu.VMEM((pieces, groups, cap, width), bf16)),
        ("from_across", pltpu.VMEM((pieces, groups, cap, width), bf16)),
        ("summed", pltpu.VMEM((pieces, groups, cap, width), bf16)),
        ("total", pltpu.VMEM((pieces, cap, width), bf16)),
        ("load_sem", dma((len(LOADED),))),
        ("first_send", dma((2, 2))),
        ("core_send", dma((length, 2))),
        ("side_send", dma((length,))),
        ("kv_recv", dma((length, 2))),
        ("q_recv", dma((2,))),
        ("lam_sem", dma((2,))),
        ("head_send", dma((2, n_tp))),
        ("head_recv", dma((2 * n_tp,))),
        ("sp_send", dma((pieces,))),
        ("sp_recv", dma((pieces,))),
        ("y_send", dma((groups, pieces))),
        ("y_recv", dma((groups, pieces))),
        ("c_send", dma((groups, pieces))),
        ("c_recv", dma((groups, pieces))),
        ("rc_send", dma((pieces, groups))),
        ("rc_recv", dma((pieces, groups))),
        ("ry_send", dma((pieces, groups))),
        ("ry_recv", dma((pieces, groups))),
        ("rs_send", dma((pieces,))),
        ("rs_recv", dma((pieces,))),
    ]
    small = ("gain_ref", "norm_ref", "ids_ref", "logits_ref", "prob_ref")
    names = [src for src, _ in LOADED] + ["lam_ref", *small, "out_ref"]
    names += [name for name, _ in scratch]
    return pl.pallas_call(
        functools.partial(layer_kernel, n_sp, n_tp, names),
        out_shape=jax.ShapeDtypeStruct((share, width), bf16),
        in_specs=[pl.BlockSpec(memory_space=pltpu.HBM)] * len(LOADED)
        + [pl.BlockSpec(memory_space=pltpu.SMEM)]
        + [vmem] * len(small),
        out_specs=vmem,
        scratch_shapes=[shape for _, shape in scratch],
        compiler_params=pltpu.CompilerParams(
            collective_id=3, has_side_effects=True, vmem_limit_bytes=LAYER_LIMIT
        ),
    )(*big, lam, gain, norm, ids, logits, prob)


def layers_fit(n_sp, n_tp, rows, vd, keys, heads, experts, cap):
    square = heads == 2 and experts == 2 and n_sp == 8 and n_tp == 4
    return square and rows % vd == 0 and vd == keys and vd % 128 == 0 and cap % 16 == 0


def on_device(
    n_sp,
    n_tp,
    query_one,
    key_one,
    query_two,
    key_two,
    values,
    mix_lambda,
    head_gain,
    residual_in,
    out_weight,
    norm_gain,
    route_ids,
    route_logits,
    group_prob,
    gate_weight,
    up_weight,
    down_weight,
):
    share = residual_in.shape[0]
    top_count = route_ids.shape[1]
    local_experts = gate_weight.shape[0]
    expert_count = local_experts * n_sp
    capacity = max(2, 2 * share * top_count // expert_count)
    if layers_fit(
        n_sp,
        n_tp,
        query_one.shape[0],
        values.shape[1] // 2,
        query_one.shape[1],
        mix_lambda.shape[0],
        local_experts,
        capacity,
    ):
        big = (key_one, key_two, values, query_one, query_two, out_weight, residual_in)
        return whole_layer(
            n_sp,
            n_tp,
            capacity,
            big + (gate_weight, up_weight, down_weight),
            mix_lambda,
            head_gain[None, :],
            norm_gain[None, :],
            route_ids.T,
            route_logits.T,
            group_prob[None, :],
        )
    token_heads = attend(
        n_sp,
        n_tp,
        key_one,
        key_two,
        values,
        query_one,
        query_two,
        mix_lambda,
        head_gain[None, :],
    )
    mix = jnp.dot(token_heads, out_weight, preferred_element_type=jnp.float32)
    hidden_f = (residual_in.astype(jnp.float32) + mix).astype(jnp.bfloat16).astype(jnp.float32)
    normed = (
        hidden_f
        * lax.rsqrt(jnp.mean(hidden_f * hidden_f, axis=-1, keepdims=True) + norm_epsilon)
        * norm_gain
    ).astype(jnp.bfloat16)
    width = normed.shape[1]
    slots = expert_count * capacity
    flat_ids = route_ids.reshape(-1)
    one_hot = (flat_ids[:, None] == jnp.arange(expert_count, dtype=jnp.int32)[None, :]).astype(
        jnp.int32
    )
    earlier = jnp.cumsum(one_hot, axis=0) - one_hot
    rank = jnp.sum(earlier * one_hot, axis=1)
    slot_of = (flat_ids * capacity + rank).reshape(share, top_count)
    places = jnp.arange(slots, dtype=jnp.int32)
    table = sum(
        (places[:, None] == slot_of[None, :, k]).astype(jnp.bfloat16) for k in range(top_count)
    )
    outgoing = jnp.dot(table, normed, preferred_element_type=jnp.float32).astype(jnp.bfloat16)
    outgoing = outgoing.reshape(n_sp, local_experts, capacity, width)
    everyone = dispatch(n_sp, n_tp, outgoing).reshape(
        local_experts, n_tp * n_sp * capacity, width
    )
    gate = jnp.einsum("erd,edf->erf", everyone, gate_weight, preferred_element_type=jnp.float32)
    upper = jnp.einsum("erd,edf->erf", everyone, up_weight, preferred_element_type=jnp.float32)
    middle = (jax.nn.silu(gate) * upper).astype(jnp.bfloat16)
    part_sum = jnp.einsum(
        "erf,efd->erd", middle, down_weight, preferred_element_type=jnp.float32
    ).astype(jnp.bfloat16)
    returned = collect(
        n_sp, n_tp, part_sum.reshape(local_experts, n_tp, n_sp, capacity, width)
    ).reshape(slots, width)
    logits = [route_logits[:, k : k + 1] for k in range(top_count)]
    highest = functools.reduce(jnp.maximum, logits)
    powers = [jnp.exp(logit - highest) for logit in logits]
    route_weight = [power / sum(powers) * group_prob[:, None] for power in powers]
    spread = sum(
        jnp.where(places[None, :] == slot_of[:, k, None], route_weight[k], 0.0)
        for k in range(top_count)
    )
    high = spread.astype(jnp.bfloat16)
    low = (spread - high.astype(jnp.float32)).astype(jnp.bfloat16)
    both = jnp.dot(
        jnp.concatenate([high, low], axis=0), returned, preferred_element_type=jnp.float32
    )
    return (hidden_f + (both[:share] + both[share:])).astype(jnp.bfloat16)


def solution(mesh):
    in_specs = (
        P("sp", "tp"),
        P("sp", "tp"),
        P("sp", "tp"),
        P("sp", "tp"),
        P("sp", "tp"),
        P("tp"),
        P(),
        P(("sp", "tp"), None),
        P(),
        P(),
        P(("sp", "tp"), None),
        P(("sp", "tp"), None),
        P(("sp", "tp")),
        P("sp", None, "tp"),
        P("sp", None, "tp"),
        P("sp", "tp", None),
    )
    out_specs = P(("sp", "tp"), None)
    return jax.shard_map(
        functools.partial(on_device, mesh.shape["sp"], mesh.shape["tp"]),
        mesh=mesh,
        in_specs=in_specs,
        out_specs=out_specs,
        check_vma=False,
    )
```

```python
import functools
import math
import types

import jax
import jax.numpy as jnp
from jax import lax
from jax.experimental import pallas as pl
from jax.experimental.pallas import tpu as pltpu
from jax.sharding import PartitionSpec as P

norm_epsilon = 1e-06
MESH = pl.DeviceIdType.MESH
VMEM_LIMIT = 60 * 1024 * 1024
LAYER_LIMIT = VMEM_LIMIT


def pair_of(count):
    return 2 if count % 2 == 0 else 1


def greet(peers):
    barrier = pltpu.get_barrier_semaphore()
    for peer in peers:
        pl.semaphore_signal(barrier, inc=1, device_id=peer, device_id_type=MESH)
    pl.semaphore_wait(barrier, len(peers))


def attend_kernel(
    n_sp,
    n_tp,
    vd,
    k1_ref,
    k2_ref,
    v_ref,
    q1_ref,
    q2_ref,
    lam_ref,
    gain_ref,
    out_ref,
    kvp,
    qp,
    held,
    q_far,
    m_ref,
    l_ref,
    acc_ref,
    stage,
    cross_send,
    cross_recv,
    line_send,
    line_recv,
    side_send,
    side_recv,
    head_send,
    head_recv,
):
    inner = pair_of(n_sp)
    length = n_sp // inner
    half = length // 2
    me = lax.axis_index("sp")
    mt = lax.axis_index("tp")
    z, x = me // inner, me % inner
    head, zi = z // half, z % half
    rows = q1_ref.shape[0]
    qk = q1_ref.shape[1] // 2
    scale = 1.0 / math.sqrt(qk)
    exact = math.frexp(scale)[0] == 0.5
    early, after = (scale, 1.0) if exact else (1.0, scale)
    other = z * inner + (inner - 1 - x)
    mirror = (length - 1 - z) * inner + x
    far_zi = half - 1 - zi
    for h in range(2):
        kvp[h, :, 0:qk] = k1_ref[:, h * qk : (h + 1) * qk]
        kvp[h, :, qk : 2 * qk] = k2_ref[:, h * qk : (h + 1) * qk]
        kvp[h, :, 2 * qk : 2 * qk + vd] = v_ref[:, h * vd : (h + 1) * vd]
        qp[h, :, 0:qk] = q1_ref[:, h * qk : (h + 1) * qk] * jnp.bfloat16(early)
        qp[h, :, qk : 2 * qk] = q2_ref[:, h * qk : (h + 1) * qk] * jnp.bfloat16(early)

    def line_device(zz):
        return (head * half + zz) * inner + x

    peers = [{"sp": me, "tp": (mt + t) % n_tp} for t in range(1, n_tp)]
    peers += [{"sp": mirror, "tp": (mt + t) % n_tp} for t in range(n_tp)]
    if inner == 2:
        peers.append({"sp": other, "tp": mt})
    if half > 1:
        for shift in sorted({1, half - 1}):
            peers.append({"sp": line_device((zi + shift) % half), "tp": mt})
    greet(peers)

    def remote(src, dst, send, recv, sp):
        return pltpu.make_async_remote_copy(
            src_ref=src,
            dst_ref=dst,
            send_sem=send,
            recv_sem=recv,
            device_id={"sp": sp, "tp": mt},
            device_id_type=MESH,
        )

    cross_q = remote(qp.at[1 - head], q_far, cross_send.at[0], cross_recv.at[0], mirror)
    cross_kv = remote(
        kvp.at[1 - head], held.at[1, far_zi, x], cross_send.at[1], cross_recv.at[1], mirror
    )

    def line_copy(j, src, zz, way):
        ahead = jnp.clip(jnp.where(way == 0, zi + 1, zi - 1), 0, half - 1)
        return remote(
            src,
            held.at[j, zz, x],
            line_send.at[j, way, zz],
            line_recv.at[j, zz],
            line_device(ahead),
        )

    def side_copy(j, src, zz):
        return remote(src, held.at[j, zz, x], side_send.at[j, zz], side_recv.at[j, zz], other)

    def start_from(j, src):
        @pl.when(zi + 1 < half)
        def _():
            line_copy(j, src, zi, 0).start()

        @pl.when(zi > 0)
        def _():
            line_copy(j, src, zi, 1).start()

        if inner == 2:
            side_copy(j, src, zi).start()

    own = kvp.at[head]
    cross_kv.start()
    start_from(0, own)
    cross_q.start()
    m_ref[...] = jnp.full(m_ref.shape, -1e30, jnp.float32)
    l_ref[...] = jnp.zeros(l_ref.shape, jnp.float32)
    acc_ref[...] = jnp.zeros(acc_ref.shape, jnp.float32)

    def absorb(block, q_ref, group):
        vals = block[:, 2 * qk : 2 * qk + vd]
        for which in range(2):
            at = 2 * group + which
            scores = lax.dot_general(
                q_ref[:, which * qk : (which + 1) * qk],
                block[:, which * qk : (which + 1) * qk],
                (((1,), (1,)), ((), ())),
                preferred_element_type=jnp.float32,
            )
            if after != 1.0:
                scores = scores * after
            old = m_ref[at]
            new = jnp.maximum(old, jnp.max(scores, axis=1, keepdims=True))
            shrink = jnp.exp(old - new)
            expo = jnp.exp(scores - new[:, :1])
            m_ref[at] = new
            l_ref[at] = l_ref[at] * shrink + jnp.sum(expo, axis=1, keepdims=True)
            acc_ref[at] = acc_ref[at] * shrink[:, :1] + jnp.dot(
                expo.astype(jnp.bfloat16), vals, preferred_element_type=jnp.float32
            )

    q_own = qp.at[head]

    def absorb_both(block):
        absorb(block, q_own, 0)
        absorb(block, q_far, 1)

    def place(n):
        dist = (n + 1) // 2
        return jnp.where(n % 2 == 1, zi - dist, zi + dist), 1 - n % 2

    def line_steps(j, take):
        def line_step(n, carry):
            zz, way = place(n)

            @pl.when((zz >= 0) & (zz < half))
            def _():
                block = held.at[j, zz, x]
                line_copy(j, block, zz, way).wait_recv()
                ahead = jnp.where(way == 0, zi + 1, zi - 1)

                @pl.when((ahead >= 0) & (ahead < half))
                def _():
                    line_copy(j, block, zz, way).start()

                if inner == 2:
                    side_copy(j, block, zz).start()
                take(block)

            return carry

        lax.fori_loop(1, 2 * half - 1, line_step, 0)

    def line_again(j):
        def again(n, carry):
            zz, _ = place(n)

            @pl.when((zz >= 0) & (zz < half))
            def _():
                absorb(held.at[j, zz, x], q_far, 1)

            return carry

        lax.fori_loop(1, 2 * half - 1, again, 0)

    def side_steps(j, begin):
        def side_step(n, carry):
            zz, _ = place(n)

            @pl.when((zz >= 0) & (zz < half))
            def _():
                block = held.at[j, zz, 1 - x]
                side_copy(j, block, zz).wait_recv()
                absorb_both(block)

            return carry

        lax.fori_loop(begin, 2 * half - 1, side_step, 0)

    near = held.at[0, zi, 1 - x]
    far = held.at[1, zi, x]
    absorb(own, q_own, 0)
    if inner == 2:
        side_copy(0, near, zi).wait_recv()
        absorb(near, q_own, 0)
    line_steps(0, lambda block: absorb(block, q_own, 0))
    cross_kv.wait_recv()
    start_from(1, far)
    absorb(far, q_own, 0)
    cross_q.wait_recv()
    absorb(own, q_far, 1)
    absorb(far, q_far, 1)
    line_steps(1, absorb_both)
    line_again(0)
    if inner == 2:
        absorb(near, q_far, 1)
        side_steps(0, 1)
        side_steps(1, 0)

    share = rows // n_tp
    lam = lam_ref[head]
    columns = pl.ds(pl.multiple_of((mt * 2 + head) * vd, vd), vd)
    copies = []
    for group, sp in ((1, mirror), (0, me)):
        read_a = acc_ref[2 * group] / l_ref[2 * group][:, :1]
        read_b = acc_ref[2 * group + 1] / l_ref[2 * group + 1][:, :1]
        combined = read_a - lam * read_b
        combined = (
            combined
            * lax.rsqrt(jnp.mean(combined * combined, axis=-1, keepdims=True) + norm_epsilon)
            * gain_ref[...]
        )
        stage[group] = combined.astype(jnp.bfloat16)
        for t in range(n_tp):
            to = (mt + t) % n_tp
            span = pl.ds(pl.multiple_of(to * share, share), share)
            if group == 0 and t == 0:
                out_ref[:, columns] = stage[0, span, :]
                continue
            copy = pltpu.make_async_remote_copy(
                src_ref=stage.at[group, span],
                dst_ref=out_ref.at[:, columns],
                send_sem=head_send.at[group, t],
                recv_sem=head_recv.at[group, t],
                device_id={"sp": sp, "tp": to},
                device_id_type=MESH,
            )
            copy.start()
            copies.append(copy)

    cross_q.wait_send()
    cross_kv.wait_send()
    for j in range(2):

        def drain(n, carry):
            zz, way = place(n)

            @pl.when((zz >= 0) & (zz < half))
            def _():
                ahead = jnp.where(way == 0, zi + 1, zi - 1)

                @pl.when((ahead >= 0) & (ahead < half))
                def _():
                    line_copy(j, own, zz, way).wait_send()

                if inner == 2:
                    side_copy(j, own, zz).wait_send()

            return carry

        lax.fori_loop(1, 2 * half - 1, drain, 0)

        @pl.when(zi + 1 < half)
        def _():
            line_copy(j, own, zi, 0).wait_send()

        @pl.when(zi > 0)
        def _():
            line_copy(j, own, zi, 1).wait_send()

        if inner == 2:
            side_copy(j, own, zi).wait_send()
    for copy in copies:
        copy.wait()


def attend(n_sp, n_tp, k1, k2, v, q1, q2, lam, gain):
    rows = q1.shape[0]
    inner = pair_of(n_sp)
    half = n_sp // inner // 2
    assert lam.shape[0] == 2 and half * inner * 2 == n_sp
    vd = v.shape[1] // 2
    qk = q1.shape[1] // 2
    cols = 2 * qk + vd
    vmem = pl.BlockSpec(memory_space=pltpu.VMEM)
    dma = pltpu.SemaphoreType.DMA
    return pl.pallas_call(
        functools.partial(attend_kernel, n_sp, n_tp, vd),
        out_shape=jax.ShapeDtypeStruct((rows // n_tp, n_tp * 2 * vd), jnp.bfloat16),
        in_specs=[vmem] * 5 + [pl.BlockSpec(memory_space=pltpu.SMEM), vmem],
        out_specs=vmem,
        scratch_shapes=[
            pltpu.VMEM((2, rows, cols), jnp.bfloat16),
            pltpu.VMEM((2, rows, 2 * qk), jnp.bfloat16),
            pltpu.VMEM((2, half, inner, rows, cols), jnp.bfloat16),
            pltpu.VMEM((rows, 2 * qk), jnp.bfloat16),
            pltpu.VMEM((4, rows, 128), jnp.float32),
            pltpu.VMEM((4, rows, 128), jnp.float32),
            pltpu.VMEM((4, rows, vd), jnp.float32),
            pltpu.VMEM((2, rows, vd), jnp.bfloat16),
            dma((2,)),
            dma((2,)),
            dma((2, 2, half)),
            dma((2, half)),
            dma((2, half)),
            dma((2, half)),
            dma((2, n_tp)),
            dma((2, n_tp)),
        ],
        compiler_params=pltpu.CompilerParams(
            collective_id=0, has_side_effects=True, vmem_limit_bytes=VMEM_LIMIT
        ),
    )(k1, k2, v, q1, q2, lam, gain)


def tp_peers(n_tp):
    inner = pair_of(n_tp)
    mt = lax.axis_index("tp")
    o, c = mt // inner, mt % inner
    across = [((o + d) % (n_tp // inner)) * inner + c for d in range(1, n_tp // inner)]
    return inner, across, o * inner + (inner - 1 - c)


def greet_all(n_sp, n_tp):
    me, mt = lax.axis_index("sp"), lax.axis_index("tp")
    inner, across, partner = tp_peers(n_tp)
    peers = [{"sp": (me + s) % n_sp, "tp": mt} for s in range(1, n_sp)]
    peers += [{"sp": me, "tp": t} for t in across]
    if inner == 2:
        peers.append({"sp": me, "tp": partner})
    greet(peers)


def dispatch_kernel(
    n_sp, n_tp, rows_ref, out_ref, sp_send, sp_recv, y_send, y_recv, c_send, c_recv, own_sem
):
    me, mt = lax.axis_index("sp"), lax.axis_index("tp")
    inner, across, partner = tp_peers(n_tp)
    groups = n_tp // inner
    o = mt // inner
    greet_all(n_sp, n_tp)

    def sp_copy(d):
        to = (me + d) % n_sp
        return pltpu.make_async_remote_copy(
            src_ref=rows_ref.at[to],
            dst_ref=out_ref.at[:, mt, me],
            send_sem=sp_send.at[d],
            recv_sem=sp_recv.at[d],
            device_id={"sp": to, "tp": mt},
            device_id_type=MESH,
        )

    def tp_copy(t, s, to, send, recv):
        return pltpu.make_async_remote_copy(
            src_ref=out_ref.at[:, t, s],
            dst_ref=out_ref.at[:, t, s],
            send_sem=send,
            recv_sem=recv,
            device_id={"sp": me, "tp": to},
            device_id_type=MESH,
        )

    order = sorted(range(1, n_sp), key=lambda d: min(d, n_sp - d))
    for d in reversed(order):
        sp_copy(d).start()
    own = pltpu.make_async_copy(rows_ref.at[me], out_ref.at[:, mt, me], own_sem)
    own.start()
    own.wait()
    started = []

    def spread(d):
        s = (me - d + n_sp) % n_sp
        for g in range(1, groups):
            copy = tp_copy(mt, s, across[g - 1], y_send.at[g, d], y_recv.at[g, d])
            copy.start()
            started.append(copy)
        if inner == 2:
            copy = tp_copy(mt, s, partner, c_send.at[0, d], c_recv.at[0, d])
            copy.start()
            started.append(copy)

    def relay(d):
        s = (me - d + n_sp) % n_sp
        for g in range(1, groups):
            source = ((o - g + groups) % groups) * inner + mt % inner
            tp_copy(source, s, partner, y_send.at[g, d], y_recv.at[g, d]).wait_recv()
            if inner == 2:
                copy = tp_copy(source, s, partner, c_send.at[g, d], c_recv.at[g, d])
                copy.start()
                started.append(copy)

    order = order[::-1]
    sequence = [0] + order
    spread(0)
    for i, d in enumerate(order):
        sp_copy(d).wait_recv()
        spread(d)
        relay(sequence[i])
    relay(sequence[-1])
    for d in range(n_sp):
        s = (me - d + n_sp) % n_sp
        if inner == 2:
            for g in range(groups):
                source = ((o - g + groups) % groups) * inner + (1 - mt % inner)
                tp_copy(source, s, partner, c_send.at[g, d], c_recv.at[g, d]).wait_recv()
    for copy in started:
        copy.wait_send()
    for d in order:
        sp_copy(d).wait_send()


def dispatch(n_sp, n_tp, rows):
    _, experts, cap, width = rows.shape
    groups = n_tp // pair_of(n_tp)
    sem = pltpu.SemaphoreType.DMA
    hbm = pl.BlockSpec(memory_space=pltpu.VMEM)
    return pl.pallas_call(
        functools.partial(dispatch_kernel, n_sp, n_tp),
        out_shape=jax.ShapeDtypeStruct((experts, n_tp, n_sp, cap, width), rows.dtype),
        in_specs=[hbm],
        out_specs=pl.BlockSpec(memory_space=pl.ANY),
        scratch_shapes=[
            sem((n_sp,)),
            sem((n_sp,)),
            sem((groups, n_sp)),
            sem((groups, n_sp)),
            sem((groups, n_sp)),
            sem((groups, n_sp)),
            sem,
        ],
        compiler_params=pltpu.CompilerParams(
            collective_id=1, has_side_effects=True, vmem_limit_bytes=VMEM_LIMIT
        ),
    )(rows)


def collect_kernel(
    n_sp,
    n_tp,
    part_ref,
    out_ref,
    from_core,
    from_across,
    summed,
    total,
    c_send,
    c_recv,
    y_send,
    y_recv,
    sp_send,
    sp_recv,
):
    me, mt = lax.axis_index("sp"), lax.axis_index("tp")
    inner, across, partner = tp_peers(n_tp)
    groups = n_tp // inner
    o, c = mt // inner, mt % inner
    greet_all(n_sp, n_tp)
    order = sorted(range(1, n_sp), key=lambda d: min(d, n_sp - d), reverse=True) + [0]

    def to_of(d):
        return (me + d) % n_sp

    def core_copy(d, g):
        row = ((o + g) % groups) * inner + (inner - 1 - c)
        return pltpu.make_async_remote_copy(
            src_ref=part_ref.at[:, row, to_of(d)],
            dst_ref=from_core.at[d, g],
            send_sem=c_send.at[d, g],
            recv_sem=c_recv.at[d, g],
            device_id={"sp": me, "tp": partner},
            device_id_type=MESH,
        )

    def across_copy(d, g):
        return pltpu.make_async_remote_copy(
            src_ref=summed.at[d, g],
            dst_ref=from_across.at[d, g],
            send_sem=y_send.at[d, g],
            recv_sem=y_recv.at[d, g],
            device_id={"sp": me, "tp": across[g - 1]},
            device_id_type=MESH,
        )

    def sp_copy(d):
        return pltpu.make_async_remote_copy(
            src_ref=total.at[d],
            dst_ref=out_ref.at[me],
            send_sem=sp_send.at[d],
            recv_sem=sp_recv.at[d],
            device_id={"sp": to_of(d), "tp": mt},
            device_id_type=MESH,
        )

    if inner == 2:
        for d in order:
            for g in list(range(1, groups)) + [0]:
                core_copy(d, g).start()

    def pair_sum(d, g):
        row = ((o + g) % groups) * inner + c
        value = part_ref[:, row, to_of(d)].astype(jnp.float32)
        if inner == 2:
            core_copy(d, g).wait_recv()
            value = value + from_core[d, g].astype(jnp.float32)
        return value

    def first(d):
        for g in range(1, groups):
            summed[d, g] = pair_sum(d, g).astype(summed.dtype)
            across_copy(d, g).start()

    def second(d):
        value = pair_sum(d, 0)
        for g in range(1, groups):
            across_copy(d, g).wait_recv()
            value = value + from_across[d, g].astype(jnp.float32)
        value = value.astype(total.dtype)
        if d == 0:
            out_ref[me] = value
        else:
            total[d] = value
            sp_copy(d).start()

    ahead = min(3, n_sp)
    for d in order[:ahead]:
        first(d)
    for i, d in enumerate(order):
        second(d)
        if i + ahead < n_sp:
            first(order[i + ahead])
    for d in range(1, n_sp):
        sp_copy(d).wait_recv()
    for d in range(n_sp):
        if d:
            sp_copy(d).wait_send()
        for g in range(groups):
            if g:
                across_copy(d, g).wait_send()
            if inner == 2:
                core_copy(d, g).wait_send()


def collect(n_sp, n_tp, part):
    experts, _, _, cap, width = part.shape
    groups = n_tp // pair_of(n_tp)
    sem = pltpu.SemaphoreType.DMA
    vmem = pl.BlockSpec(memory_space=pltpu.VMEM)
    piece = (experts, cap, width)
    return pl.pallas_call(
        functools.partial(collect_kernel, n_sp, n_tp),
        out_shape=jax.ShapeDtypeStruct((n_sp,) + piece, part.dtype),
        in_specs=[vmem],
        out_specs=vmem,
        scratch_shapes=[
            pltpu.VMEM((n_sp, groups) + piece, part.dtype),
            pltpu.VMEM((n_sp, groups) + piece, part.dtype),
            pltpu.VMEM((n_sp, groups) + piece, part.dtype),
            pltpu.VMEM((n_sp,) + piece, part.dtype),
            sem((n_sp, groups)),
            sem((n_sp, groups)),
            sem((n_sp, groups)),
            sem((n_sp, groups)),
            sem((n_sp,)),
            sem((n_sp,)),
        ],
        compiler_params=pltpu.CompilerParams(
            collective_id=2, has_side_effects=True, vmem_limit_bytes=VMEM_LIMIT
        ),
    )(part)


def attention_phase(n_sp, n_tp, r, arrived, filler):
    inner, pair = 2, 2
    length = n_sp // inner
    me, mt = lax.axis_index("sp"), lax.axis_index("tp")
    z, x = me // inner, me % inner
    y, c = mt // pair, mt % pair
    rows, qk = r.q1_ref.shape[0], r.q1_ref.shape[1] // 2
    vd = r.v_ref.shape[1] // 2
    keys = 2 * qk
    scale = 1.0 / math.sqrt(qk)
    exact = math.frexp(scale)[0] == 0.5
    early, after = (scale, 1.0) if exact else (1.0, scale)
    home = c == z // pair
    partner = y * pair + (1 - c)
    across = z * inner + (1 - x)

    def spot(zz):
        return zz * inner + x

    for h in range(2):
        at = slice(h * qk, (h + 1) * qk)
        block = jnp.concatenate([r.k1_ref[:, at], r.k2_ref[:, at]], axis=1)
        turned = jnp.concatenate(
            [
                r.v_ref[base : base + vd, h * vd : (h + 1) * vd].astype(jnp.float32).T
                for base in range(0, rows, vd)
            ],
            axis=0,
        ).astype(jnp.bfloat16)
        query = jnp.concatenate([r.q1_ref[:, at], r.q2_ref[:, at]], axis=1) * jnp.bfloat16(early)
        r.kv_out[h, :, 0:keys] = block
        r.kv_out[h, :, keys : keys + vd] = turned
        r.q_out[h] = query

        @pl.when(z == pair * c + h)
        def _():
            r.held[z, 0, :, 0:keys] = block
            r.held[z, 0, :, keys : keys + vd] = turned
            r.q_in[h] = query

    r.lam_mine[...] = jnp.full(r.lam_mine.shape, r.lam_ref[z % pair], jnp.float32)
    r.m_ref[...] = jnp.full(r.m_ref.shape, -1e30, jnp.float32)
    r.l_ref[...] = jnp.zeros(r.l_ref.shape, jnp.float32)
    r.acc_ref[...] = jnp.zeros(r.acc_ref.shape, jnp.float32)
    r.qt[...] = jnp.zeros(r.qt.shape, r.qt.dtype)
    arrived()

    def remote(src, dst, send, recv, sp, tp):
        return pltpu.make_async_remote_copy(
            src_ref=src,
            dst_ref=dst,
            send_sem=send,
            recv_sem=recv,
            device_id={"sp": sp, "tp": tp},
            device_id_type=MESH,
        )

    def first_q(h):
        return remote(
            r.q_out.at[h],
            r.q_in.at[z % pair],
            r.first_send.at[0, h],
            r.q_recv.at[z % pair],
            spot(pair * c + h),
            y * pair + z // pair,
        )

    def first_kv(h):
        return remote(
            r.kv_out.at[h],
            r.held.at[z, 0],
            r.first_send.at[1, h],
            r.kv_recv.at[z, 0],
            spot(pair * c + h),
            y * pair + z // pair,
        )

    def to_core(zz, side):
        block = r.held.at[zz, side]
        return remote(block, block, r.core_send.at[zz, side], r.kv_recv.at[zz, side], me, partner)

    def to_side(zz):
        return remote(
            r.held.at[zz, 0], r.held.at[zz, 1], r.side_send.at[zz], r.kv_recv.at[zz, 1], across, mt
        )

    lam_copy = remote(r.lam_mine, r.lam_far, r.lam_sem.at[0], r.lam_sem.at[1], me, partner)

    def away(h):
        return z != pair * c + h

    order = [z, z + 1 - 2 * (z % pair), pair - z // pair, (length - 1) * (1 - z // pair)]

    @pl.when(home)
    def _():
        to_side(z).start()
        to_core(z, 0).start()

    for h in range(2):

        @pl.when(away(h))
        def _():
            first_q(h).start()

    for h in range(2):

        @pl.when(away(h))
        def _():
            first_kv(h).start()

    lam_copy.start()
    filler()

    for g in range(2):

        @pl.when((z != pair * c + g))
        def _():
            remote(
                r.q_out.at[g], r.q_in.at[g], r.first_send.at[0, g], r.q_recv.at[g], me, mt
            ).wait_recv()

        turned = r.q_in[g].astype(jnp.float32).T.astype(jnp.bfloat16)
        r.qt[0:qk, 2 * g * rows : (2 * g + 1) * rows] = turned[0:qk]
        r.qt[qk:keys, (2 * g + 1) * rows : (2 * g + 2) * rows] = turned[qk:keys]

    def absorb(zz, side):
        block_keys = r.held[zz, side, :, 0:keys]
        turned = jnp.concatenate(
            [r.held[zz, side, base : base + vd, keys : keys + vd] for base in range(0, rows, vd)], axis=1
        )
        for part in range(4):
            at = slice(part * rows, (part + 1) * rows)
            scores = jnp.dot(block_keys, r.qt[:, at], preferred_element_type=jnp.float32)
            if after != 1.0:
                scores = scores * after
            old = r.m_ref[:, at]
            new = jnp.maximum(old, jnp.max(scores, axis=0, keepdims=True))
            shrink = jnp.exp(old - new)
            expo = jnp.exp(scores - new)
            r.m_ref[:, at] = new
            r.l_ref[:, at] = r.l_ref[:, at] * shrink + jnp.sum(expo, axis=0, keepdims=True)
            r.acc_ref[:, at] = r.acc_ref[:, at] * shrink + jnp.dot(
                turned, expo.astype(jnp.bfloat16), preferred_element_type=jnp.float32
            )

    near_first = ((0, 0), (0, 1), (1, 0), (1, 1), (2, 0), (3, 0), (2, 1), (3, 1))
    far_first = ((0, 0), (0, 1), (1, 0), (2, 0), (1, 1), (3, 0), (2, 1), (3, 1))

    def pick(values, n):
        result = values[0]
        for k in range(1, len(values)):
            result = jnp.where(n == k, values[k], result)
        return result

    def step(n, carry):
        at_home = [pick([p[i] for p in near_first], n) for i in range(2)]
        at_far = [pick([p[i] for p in far_first], n) for i in range(2)]
        zz = pick(order, jnp.where(home, at_home[0], at_far[0]))
        side = jnp.where(home, at_home[1], at_far[1])
        direct = zz // pair == c
        local = home & (n == 0)

        @pl.when(jnp.logical_not(local))
        def _():
            to_core(zz, side).wait_recv()

            @pl.when(direct & (side == 0))
            def _():
                to_side(zz).start()

            @pl.when(direct)
            def _():
                to_core(zz, side).start()

        absorb(zz, side)
        return carry

    lax.fori_loop(0, 2 * length, step, 0)

    share = rows // n_tp
    lam_copy.wait()
    lam = jnp.where(home, r.lam_mine[0:1, 0:1], r.lam_far[0:1, 0:1])
    head = y * length + z
    columns = pl.ds(pl.multiple_of(head * vd, vd), vd)

    def piece(g, t):
        to = (mt + t) % n_tp
        span = pl.ds(pl.multiple_of(to * share, share), share)
        return remote(
            r.stage.at[g, span],
            r.token_ref.at[:, columns],
            r.head_send.at[g, t],
            r.head_recv.at[head],
            spot(pair * c + g),
            to,
        )

    def own(g):
        return z == pair * c + g

    for g in (1, 0):
        reads = []
        for which in range(2):
            at = slice((2 * g + which) * rows, (2 * g + which + 1) * rows)
            reads.append(r.acc_ref[:, at] / r.l_ref[:, at])
        combined = reads[0] - lam * reads[1]
        combined = combined * lax.rsqrt(
            jnp.mean(combined * combined, axis=0, keepdims=True) + norm_epsilon
        )
        r.stage[g] = (combined.T * r.gain_ref[...]).astype(jnp.bfloat16)
        for t in range(1, n_tp):
            piece(g, t).start()

        @pl.when(own(g))
        def _():
            r.token_ref[:, columns] = r.stage[g, pl.ds(pl.multiple_of(mt * share, share), share), :]

        @pl.when(jnp.logical_not(own(g)))
        def _():
            piece(g, 0).start()

    def head_copy(hd):
        at = pl.ds(pl.multiple_of(hd * vd, vd), vd)
        return remote(
            r.stage.at[0, 0:share], r.token_ref.at[:, at], r.head_send.at[0, 0], r.head_recv.at[hd], me, mt
        )

    for hd in range(2 * n_tp):

        @pl.when((hd != head) | jnp.logical_not(home))
        def _():
            head_copy(hd).wait_recv()

    def finish():
        for g in range(2):
            for t in range(1, n_tp):
                piece(g, t).wait_send()

            @pl.when(jnp.logical_not(own(g)))
            def _():
                piece(g, 0).wait_send()

            @pl.when(away(g))
            def _():
                first_q(g).wait_send()
                first_kv(g).wait_send()

        for zz in range(length):

            @pl.when(c == zz // pair)
            def _():
                to_side(zz).wait_send()
                to_core(zz, 0).wait_send()
                to_core(zz, 1).wait_send()

    return finish


def routing_tables(r, experts_in_all, cap):
    ids = r.ids_ref[...].astype(jnp.float32)
    top, share = ids.shape
    names = lax.broadcasted_iota(jnp.int32, (experts_in_all, share), 0).astype(jnp.float32)
    before = lax.broadcasted_iota(jnp.int32, (share, share), 0)
    before = before < lax.broadcasted_iota(jnp.int32, (share, share), 1)
    before = before.astype(jnp.float32).astype(jnp.bfloat16)
    taken = jnp.zeros((experts_in_all, 1), jnp.float32)
    places = lax.broadcasted_iota(jnp.int32, (experts_in_all * cap, share), 0).astype(jnp.float32)
    logits = [r.logits_ref[k : k + 1, :] for k in range(top)]
    highest = functools.reduce(jnp.maximum, logits)
    powers = [jnp.exp(logit - highest) for logit in logits]
    total = sum(powers)
    table = jnp.zeros(places.shape, jnp.float32)
    spread = jnp.zeros(places.shape, jnp.float32)
    for k in range(top):
        hit = (names == ids[k : k + 1, :]).astype(jnp.float32)
        earlier = jnp.dot(hit.astype(jnp.bfloat16), before, preferred_element_type=jnp.float32)
        rank = jnp.sum(hit * (earlier + taken), axis=0, keepdims=True)
        taken = taken + jnp.sum(hit, axis=1, keepdims=True)
        placed = (places == ids[k : k + 1, :] * cap + rank).astype(jnp.float32)
        table = table + placed
        spread = spread + placed * (powers[k] / total * r.prob_ref[...])
    r.table[...] = table.astype(jnp.bfloat16)
    turned = spread.T
    high = turned.astype(jnp.bfloat16)
    r.spread[0:share] = high
    r.spread[share : 2 * share] = (turned - high.astype(jnp.float32)).astype(jnp.bfloat16)


def token_phase(r, wait_weights):
    share, width = r.residual.shape
    tile = math.gcd(width, 512)
    columns = [slice(n, n + tile) for n in range(0, width, tile)]
    wait_weights()
    square = jnp.zeros((share, 1), jnp.float32)
    for at in columns:
        mix = jnp.dot(r.token_ref[...], r.out_w[:, at], preferred_element_type=jnp.float32)
        hidden = (r.residual[:, at].astype(jnp.float32) + mix).astype(jnp.bfloat16)
        r.hidden[:, at] = hidden
        hidden = hidden.astype(jnp.float32)
        square = square + jnp.sum(hidden * hidden, axis=1, keepdims=True)
    factor = lax.rsqrt(square / width + norm_epsilon)
    n_sp, experts, cap = r.outgoing.shape[:3]
    for at in columns:
        normed = r.hidden[:, at].astype(jnp.float32) * factor * r.norm_ref[:, at]
        rows = jnp.dot(
            r.table[...], normed.astype(jnp.bfloat16), preferred_element_type=jnp.float32
        ).astype(jnp.bfloat16)
        r.outgoing[:, :, :, at] = rows.reshape(n_sp, experts, cap, tile)


def expert_phase(n_sp, n_tp, r, weights, finish):
    me, mt = lax.axis_index("sp"), lax.axis_index("tp")
    inner_sp = 2
    z, x = me // inner_sp, me % inner_sp
    inner, across, partner = tp_peers(n_tp)
    groups = n_tp // inner
    o, c = mt // inner, mt % inner
    _, experts, cap, _ = r.outgoing.shape

    def flip(number, by):
        low = (number % 2 + by % 2) % 2
        return (number // 2 + by // 2) % 2 * 2 + low

    def peer_of(i):
        return flip(z, i // inner_sp) * inner_sp + flip(x, i % inner_sp)

    def span(t):
        return pl.ds(pl.multiple_of(t * cap, cap), cap)

    def remote(src, dst, send, recv, sp, tp):
        return pltpu.make_async_remote_copy(
            src_ref=src,
            dst_ref=dst,
            send_sem=send,
            recv_sem=recv,
            device_id={"sp": sp, "tp": tp},
            device_id_type=MESH,
        )

    pieces = n_sp * experts

    def sp_copy(j):
        i, e = j // experts, j % experts
        to = peer_of(i)
        block = r.rows.at[i, e, span(mt)]
        return remote(r.outgoing.at[to, e], block, r.sp_send.at[j], r.sp_recv.at[j], to, mt)

    def across_in(j, g, t):
        block = r.rows.at[j // experts, j % experts, span(t)]
        return remote(block, block, r.y_send.at[g, j], r.y_recv.at[g, j], me, across[g - 1])

    def core_in(j, g, t):
        block = r.rows.at[j // experts, j % experts, span(t)]
        return remote(block, block, r.c_send.at[g, j], r.c_recv.at[g, j], me, partner)

    def core_out(j, g):
        row = ((o + g) % groups) * inner + (inner - 1 - c)
        block = r.part.at[j, span(row)]
        return remote(
            block, r.from_core.at[j, g], r.rc_send.at[j, g], r.rc_recv.at[j, g], me, partner
        )

    def across_out(j, g):
        return remote(
            r.summed.at[j, g],
            r.from_across.at[j, g],
            r.ry_send.at[j, g],
            r.ry_recv.at[j, g],
            me,
            across[g - 1],
        )

    def sp_out(j):
        i, e = j // experts, j % experts
        block = r.returned.at[me, e]
        return remote(r.total.at[j], block, r.rs_send.at[j], r.rs_recv.at[j], peer_of(i), mt)

    def source(g):
        return ((o - g + groups) % groups) * inner + c

    for j in (2, 8, 4, 3, 9, 5, 10, 6, 11, 7, 12, 13, 14, 15):
        sp_copy(j).start()
    r.rows[0, :, span(mt), :] = r.outgoing[me]

    def spread(j):
        @pl.when(j >= experts)
        def _():
            sp_copy(j).wait_recv()

        for g in range(1, groups):
            across_in(j, g, mt).start()
        core_in(j, 0, mt).start()

    def relay(j):
        for g in range(1, groups):
            across_in(j, g, source(g)).wait_recv()
            core_in(j, g, source(g)).start()

    half = n_sp // 2
    ready = half * experts

    def compute(j):
        @pl.when(j == ready)
        def _():
            for copy in weights:
                copy.wait()

        for g in range(groups):
            core_in(j, g, source(g)).wait_recv()
        e = j % experts
        rows = r.rows[j // experts, e]
        gate = jnp.dot(rows, r.gate_w[e], preferred_element_type=jnp.float32)
        upper = jnp.dot(rows, r.up_w[e], preferred_element_type=jnp.float32)
        middle = (gate / (1.0 + jnp.exp(-gate)) * upper).astype(jnp.bfloat16)
        r.part[j] = jnp.dot(middle, r.down_w[e], preferred_element_type=jnp.float32).astype(
            r.part.dtype
        )
        for g in list(range(1, groups)) + [0]:
            core_out(j, g).start()

    def pair_sum(j, g):
        row = ((o + g) % groups) * inner + c
        value = r.part[j, span(row), :].astype(jnp.float32)
        core_out(j, g).wait_recv()
        return value + r.from_core[j, g].astype(jnp.float32)

    def first(j):
        for g in range(1, groups):
            r.summed[j, g] = pair_sum(j, g).astype(r.summed.dtype)
            across_out(j, g).start()

    def second(j):
        value = pair_sum(j, 0)
        for g in range(1, groups):
            across_out(j, g).wait_recv()
            value = value + r.from_across[j, g].astype(jnp.float32)
        value = value.astype(r.total.dtype)

        @pl.when(j < experts)
        def _():
            r.returned[me, j] = value

        @pl.when(j >= experts)
        def _():
            r.total[j] = value
            sp_out(j).start()

    def far_first(n):
        near = jnp.where(n < ready + half, n - half, jnp.where(n < ready + 6, n - 10, n - 14))
        return jnp.where(n < ready, n + ready, near)

    def arrival(n):
        mixed = n // 2 + jnp.where(n % 2 == 0, 2, 6)
        return jnp.where((n < half) | (n >= ready + half), n, mixed)

    def turned(stage):
        return lambda n: stage(far_first(n))

    stages = tuple((lambda n, f=f: f(arrival(n))) for f in (spread, relay)) + tuple(turned(stage) for stage in (compute, first, second))
    lags = (0, 3, 12, 14, 17)

    def step(n, carry):
        for stage, lag in zip(stages, lags):

            @pl.when((n >= lag) & (n < pieces + lag))
            def _():
                stage(n - lag)

        return carry

    lax.fori_loop(0, pieces + lags[-1], step, 0)

    finish()

    def drain(j, carry):
        @pl.when(j >= experts)
        def _():
            sp_out(j).wait_send()
            sp_copy(j).wait_send()

        for g in range(groups):
            if g:
                across_in(j, g, mt).wait_send()
                across_out(j, g).wait_send()
            core_in(j, g, mt).wait_send()
            core_out(j, g).wait_send()
        return carry

    lax.fori_loop(0, pieces, drain, 0)

    def arrive(j, carry):
        sp_out(j).wait_recv()
        return carry

    lax.fori_loop(experts, pieces, arrive, 0)
    share = r.residual.shape[0]
    width = r.residual.shape[1]
    tile = math.gcd(width, 512)
    for n in range(0, width, tile):
        at = slice(n, n + tile)
        both = jnp.dot(
            r.spread[...],
            r.returned[:, :, :, at].reshape(pieces * cap, tile),
            preferred_element_type=jnp.float32,
        )
        r.out_ref[:, at] = (r.hidden[:, at].astype(jnp.float32) + (both[:share] + both[share:])).astype(jnp.bfloat16)


def layer_kernel(n_sp, n_tp, names, *refs):
    r = types.SimpleNamespace(**dict(zip(names, refs)))
    me, mt = lax.axis_index("sp"), lax.axis_index("tp")
    inner = 2
    z, x = me // inner, me % inner
    barrier = pltpu.get_barrier_semaphore()
    lines = [(zz * inner + x, t) for zz in range(n_sp // inner) for t in range(n_tp)]
    lines += [(zz * inner + (1 - x), mt) for zz in range(n_sp // inner)]
    for sp, tp in lines:

        @pl.when((sp != me) | (tp != mt))
        def _():
            pl.semaphore_signal(
                barrier, inc=1, device_id={"sp": sp, "tp": tp}, device_id_type=MESH
            )

    def loads(pairs):
        copies = [
            pltpu.make_async_copy(getattr(r, src), getattr(r, dst), r.load_sem.at[k])
            for k, (src, dst) in pairs
        ]
        for copy in copies:
            copy.start()
        return copies

    pairs = list(enumerate(LOADED))
    first = loads(pairs[:5])
    middle = loads(pairs[5:7])
    last = loads(pairs[7:])
    for copy in first:
        copy.wait()

    def wait_middle():
        for copy in middle:
            copy.wait()

    experts, cap = r.outgoing.shape[1:3]
    finish = attention_phase(
        n_sp,
        n_tp,
        r,
        lambda: pl.semaphore_wait(barrier, len(lines) - 1),
        lambda: routing_tables(r, n_sp * experts, cap),
    )
    token_phase(r, wait_middle)
    expert_phase(n_sp, n_tp, r, last, finish)


LOADED = (
    ("k1_hbm", "k1_ref"),
    ("k2_hbm", "k2_ref"),
    ("v_hbm", "v_ref"),
    ("q1_hbm", "q1_ref"),
    ("q2_hbm", "q2_ref"),
    ("out_w_hbm", "out_w"),
    ("residual_hbm", "residual"),
    ("gate_hbm", "gate_w"),
    ("up_hbm", "up_w"),
    ("down_hbm", "down_w"),
)


def whole_layer(n_sp, n_tp, cap, big, lam, gain, norm, ids, logits, prob):
    k1, k2, v, q1, q2, out_w, residual, gate, up, down = big
    rows, keys = q1.shape
    length = n_sp // 2
    vd = v.shape[1] // 2
    cols = keys + vd
    share, width = residual.shape
    experts = gate.shape[0]
    pieces = n_sp * experts
    slots = pieces * cap
    groups = n_tp // 2
    bf16, f32 = jnp.bfloat16, jnp.float32
    vmem = pl.BlockSpec(memory_space=pltpu.VMEM)
    dma = pltpu.SemaphoreType.DMA
    piece = (experts, cap, width)
    scratch = [(dst, pltpu.VMEM(a.shape, a.dtype)) for (_, dst), a in zip(LOADED, big)]
    scratch += [
        ("token_ref", pltpu.VMEM((share, out_w.shape[0]), bf16)),
        ("kv_out", pltpu.VMEM((2, rows, cols), bf16)),
        ("q_out", pltpu.VMEM((2, rows, keys), bf16)),
        ("held", pltpu.VMEM((length, 2, rows, cols), bf16)),
        ("q_in", pltpu.VMEM((2, rows, keys), bf16)),
        ("qt", pltpu.VMEM((keys, 4 * rows), bf16)),
        ("m_ref", pltpu.VMEM((1, 4 * rows), f32)),
        ("l_ref", pltpu.VMEM((1, 4 * rows), f32)),
        ("acc_ref", pltpu.VMEM((vd, 4 * rows), f32)),
        ("stage", pltpu.VMEM((2, rows, vd), bf16)),
        ("lam_mine", pltpu.VMEM((8, 128), f32)),
        ("lam_far", pltpu.VMEM((8, 128), f32)),
        ("table", pltpu.VMEM((slots, share), bf16)),
        ("spread", pltpu.VMEM((2 * share, slots), bf16)),
        ("hidden", pltpu.VMEM((share, width), bf16)),
        ("outgoing", pltpu.VMEM((n_sp,) + piece, bf16)),
        ("returned", pltpu.VMEM((n_sp,) + piece, bf16)),
        ("rows", pltpu.VMEM((n_sp, experts, n_tp * cap, width), bf16)),
        ("part", pltpu.VMEM((pieces, n_tp * cap, width), bf16)),
        ("from_core", pltpu.VMEM((pieces, groups, cap, width), bf16)),
        ("from_across", pltpu.VMEM((pieces, groups, cap, width), bf16)),
        ("summed", pltpu.VMEM((pieces, groups, cap, width), bf16)),
        ("total", pltpu.VMEM((pieces, cap, width), bf16)),
        ("load_sem", dma((len(LOADED),))),
        ("first_send", dma((2, 2))),
        ("core_send", dma((length, 2))),
        ("side_send", dma((length,))),
        ("kv_recv", dma((length, 2))),
        ("q_recv", dma((2,))),
        ("lam_sem", dma((2,))),
        ("head_send", dma((2, n_tp))),
        ("head_recv", dma((2 * n_tp,))),
        ("sp_send", dma((pieces,))),
        ("sp_recv", dma((pieces,))),
        ("y_send", dma((groups, pieces))),
        ("y_recv", dma((groups, pieces))),
        ("c_send", dma((groups, pieces))),
        ("c_recv", dma((groups, pieces))),
        ("rc_send", dma((pieces, groups))),
        ("rc_recv", dma((pieces, groups))),
        ("ry_send", dma((pieces, groups))),
        ("ry_recv", dma((pieces, groups))),
        ("rs_send", dma((pieces,))),
        ("rs_recv", dma((pieces,))),
    ]
    small = ("gain_ref", "norm_ref", "ids_ref", "logits_ref", "prob_ref")
    names = [src for src, _ in LOADED] + ["lam_ref", *small, "out_ref"]
    names += [name for name, _ in scratch]
    return pl.pallas_call(
        functools.partial(layer_kernel, n_sp, n_tp, names),
        out_shape=pltpu.VMEM((share, width), bf16),
        in_specs=[pl.BlockSpec(memory_space=pltpu.HBM)] * len(LOADED)
        + [pl.BlockSpec(memory_space=pltpu.SMEM)]
        + [vmem] * len(small),
        out_specs=vmem,
        scratch_shapes=[shape for _, shape in scratch],
        compiler_params=pltpu.CompilerParams(
            collective_id=3, has_side_effects=True, vmem_limit_bytes=LAYER_LIMIT
        ),
    )(*big, lam, gain, norm, ids, logits, prob)


def layers_fit(n_sp, n_tp, rows, vd, keys, heads, experts, cap):
    square = heads == 2 and experts == 2 and n_sp == 8 and n_tp == 4
    return square and rows % vd == 0 and vd == keys and vd % 128 == 0 and cap % 16 == 0


def on_device(
    n_sp,
    n_tp,
    query_one,
    key_one,
    query_two,
    key_two,
    values,
    mix_lambda,
    head_gain,
    residual_in,
    out_weight,
    norm_gain,
    route_ids,
    route_logits,
    group_prob,
    gate_weight,
    up_weight,
    down_weight,
):
    share = residual_in.shape[0]
    top_count = route_ids.shape[1]
    local_experts = gate_weight.shape[0]
    expert_count = local_experts * n_sp
    capacity = max(2, 2 * share * top_count // expert_count)
    if layers_fit(
        n_sp,
        n_tp,
        query_one.shape[0],
        values.shape[1] // 2,
        query_one.shape[1],
        mix_lambda.shape[0],
        local_experts,
        capacity,
    ):
        big = (key_one, key_two, values, query_one, query_two, out_weight, residual_in)
        return whole_layer(
            n_sp,
            n_tp,
            capacity,
            big + (gate_weight, up_weight, down_weight),
            mix_lambda,
            head_gain[None, :],
            norm_gain[None, :],
            route_ids.T,
            route_logits.T,
            group_prob[None, :],
        )
    token_heads = attend(
        n_sp,
        n_tp,
        key_one,
        key_two,
        values,
        query_one,
        query_two,
        mix_lambda,
        head_gain[None, :],
    )
    mix = jnp.dot(token_heads, out_weight, preferred_element_type=jnp.float32)
    hidden_f = (residual_in.astype(jnp.float32) + mix).astype(jnp.bfloat16).astype(jnp.float32)
    normed = (
        hidden_f
        * lax.rsqrt(jnp.mean(hidden_f * hidden_f, axis=-1, keepdims=True) + norm_epsilon)
        * norm_gain
    ).astype(jnp.bfloat16)
    width = normed.shape[1]
    slots = expert_count * capacity
    flat_ids = route_ids.reshape(-1)
    one_hot = (flat_ids[:, None] == jnp.arange(expert_count, dtype=jnp.int32)[None, :]).astype(
        jnp.int32
    )
    earlier = jnp.cumsum(one_hot, axis=0) - one_hot
    rank = jnp.sum(earlier * one_hot, axis=1)
    slot_of = (flat_ids * capacity + rank).reshape(share, top_count)
    places = jnp.arange(slots, dtype=jnp.int32)
    table = sum(
        (places[:, None] == slot_of[None, :, k]).astype(jnp.bfloat16) for k in range(top_count)
    )
    outgoing = jnp.dot(table, normed, preferred_element_type=jnp.float32).astype(jnp.bfloat16)
    outgoing = outgoing.reshape(n_sp, local_experts, capacity, width)
    everyone = dispatch(n_sp, n_tp, outgoing).reshape(
        local_experts, n_tp * n_sp * capacity, width
    )
    gate = jnp.einsum("erd,edf->erf", everyone, gate_weight, preferred_element_type=jnp.float32)
    upper = jnp.einsum("erd,edf->erf", everyone, up_weight, preferred_element_type=jnp.float32)
    middle = (jax.nn.silu(gate) * upper).astype(jnp.bfloat16)
    part_sum = jnp.einsum(
        "erf,efd->erd", middle, down_weight, preferred_element_type=jnp.float32
    ).astype(jnp.bfloat16)
    returned = collect(
        n_sp, n_tp, part_sum.reshape(local_experts, n_tp, n_sp, capacity, width)
    ).reshape(slots, width)
    logits = [route_logits[:, k : k + 1] for k in range(top_count)]
    highest = functools.reduce(jnp.maximum, logits)
    powers = [jnp.exp(logit - highest) for logit in logits]
    route_weight = [power / sum(powers) * group_prob[:, None] for power in powers]
    spread = sum(
        jnp.where(places[None, :] == slot_of[:, k, None], route_weight[k], 0.0)
        for k in range(top_count)
    )
    high = spread.astype(jnp.bfloat16)
    low = (spread - high.astype(jnp.float32)).astype(jnp.bfloat16)
    both = jnp.dot(
        jnp.concatenate([high, low], axis=0), returned, preferred_element_type=jnp.float32
    )
    return (hidden_f + (both[:share] + both[share:])).astype(jnp.bfloat16)


def solution(mesh):
    in_specs = (
        P("sp", "tp"),
        P("sp", "tp"),
        P("sp", "tp"),
        P("sp", "tp"),
        P("sp", "tp"),
        P("tp"),
        P(),
        P(("sp", "tp"), None),
        P(),
        P(),
        P(("sp", "tp"), None),
        P(("sp", "tp"), None),
        P(("sp", "tp")),
        P("sp", None, "tp"),
        P("sp", None, "tp"),
        P("sp", "tp", None),
    )
    out_specs = P(("sp", "tp"), None)
    return jax.shard_map(
        functools.partial(on_device, mesh.shape["sp"], mesh.shape["tp"]),
        mesh=mesh,
        in_specs=in_specs,
        out_specs=out_specs,
        check_vma=False,
    )
```

```python
import functools
import math
import types

import jax
import jax.numpy as jnp
from jax import lax
from jax.experimental import pallas as pl
from jax.experimental.pallas import tpu as pltpu
from jax.sharding import PartitionSpec as P

norm_epsilon = 1e-06
MESH = pl.DeviceIdType.MESH
VMEM_LIMIT = 60 * 1024 * 1024
LAYER_LIMIT = VMEM_LIMIT


def pair_of(count):
    return 2 if count % 2 == 0 else 1


def greet(peers):
    barrier = pltpu.get_barrier_semaphore()
    for peer in peers:
        pl.semaphore_signal(barrier, inc=1, device_id=peer, device_id_type=MESH)
    pl.semaphore_wait(barrier, len(peers))


def attend_kernel(
    n_sp,
    n_tp,
    vd,
    k1_ref,
    k2_ref,
    v_ref,
    q1_ref,
    q2_ref,
    lam_ref,
    gain_ref,
    out_ref,
    kvp,
    qp,
    held,
    q_far,
    m_ref,
    l_ref,
    acc_ref,
    stage,
    cross_send,
    cross_recv,
    line_send,
    line_recv,
    side_send,
    side_recv,
    head_send,
    head_recv,
):
    inner = pair_of(n_sp)
    length = n_sp // inner
    half = length // 2
    me = lax.axis_index("sp")
    mt = lax.axis_index("tp")
    z, x = me // inner, me % inner
    head, zi = z // half, z % half
    rows = q1_ref.shape[0]
    qk = q1_ref.shape[1] // 2
    scale = 1.0 / math.sqrt(qk)
    exact = math.frexp(scale)[0] == 0.5
    early, after = (scale, 1.0) if exact else (1.0, scale)
    other = z * inner + (inner - 1 - x)
    mirror = (length - 1 - z) * inner + x
    far_zi = half - 1 - zi
    for h in range(2):
        kvp[h, :, 0:qk] = k1_ref[:, h * qk : (h + 1) * qk]
        kvp[h, :, qk : 2 * qk] = k2_ref[:, h * qk : (h + 1) * qk]
        kvp[h, :, 2 * qk : 2 * qk + vd] = v_ref[:, h * vd : (h + 1) * vd]
        qp[h, :, 0:qk] = q1_ref[:, h * qk : (h + 1) * qk] * jnp.bfloat16(early)
        qp[h, :, qk : 2 * qk] = q2_ref[:, h * qk : (h + 1) * qk] * jnp.bfloat16(early)

    def line_device(zz):
        return (head * half + zz) * inner + x

    peers = [{"sp": me, "tp": (mt + t) % n_tp} for t in range(1, n_tp)]
    peers += [{"sp": mirror, "tp": (mt + t) % n_tp} for t in range(n_tp)]
    if inner == 2:
        peers.append({"sp": other, "tp": mt})
    if half > 1:
        for shift in sorted({1, half - 1}):
            peers.append({"sp": line_device((zi + shift) % half), "tp": mt})
    greet(peers)

    def remote(src, dst, send, recv, sp):
        return pltpu.make_async_remote_copy(
            src_ref=src,
            dst_ref=dst,
            send_sem=send,
            recv_sem=recv,
            device_id={"sp": sp, "tp": mt},
            device_id_type=MESH,
        )

    cross_q = remote(qp.at[1 - head], q_far, cross_send.at[0], cross_recv.at[0], mirror)
    cross_kv = remote(
        kvp.at[1 - head], held.at[1, far_zi, x], cross_send.at[1], cross_recv.at[1], mirror
    )

    def line_copy(j, src, zz, way):
        ahead = jnp.clip(jnp.where(way == 0, zi + 1, zi - 1), 0, half - 1)
        return remote(
            src,
            held.at[j, zz, x],
            line_send.at[j, way, zz],
            line_recv.at[j, zz],
            line_device(ahead),
        )

    def side_copy(j, src, zz):
        return remote(src, held.at[j, zz, x], side_send.at[j, zz], side_recv.at[j, zz], other)

    def start_from(j, src):
        @pl.when(zi + 1 < half)
        def _():
            line_copy(j, src, zi, 0).start()

        @pl.when(zi > 0)
        def _():
            line_copy(j, src, zi, 1).start()

        if inner == 2:
            side_copy(j, src, zi).start()

    own = kvp.at[head]
    cross_kv.start()
    start_from(0, own)
    cross_q.start()
    m_ref[...] = jnp.full(m_ref.shape, -1e30, jnp.float32)
    l_ref[...] = jnp.zeros(l_ref.shape, jnp.float32)
    acc_ref[...] = jnp.zeros(acc_ref.shape, jnp.float32)

    def absorb(block, q_ref, group):
        vals = block[:, 2 * qk : 2 * qk + vd]
        for which in range(2):
            at = 2 * group + which
            scores = lax.dot_general(
                q_ref[:, which * qk : (which + 1) * qk],
                block[:, which * qk : (which + 1) * qk],
                (((1,), (1,)), ((), ())),
                preferred_element_type=jnp.float32,
            )
            if after != 1.0:
                scores = scores * after
            old = m_ref[at]
            new = jnp.maximum(old, jnp.max(scores, axis=1, keepdims=True))
            shrink = jnp.exp(old - new)
            expo = jnp.exp(scores - new[:, :1])
            m_ref[at] = new
            l_ref[at] = l_ref[at] * shrink + jnp.sum(expo, axis=1, keepdims=True)
            acc_ref[at] = acc_ref[at] * shrink[:, :1] + jnp.dot(
                expo.astype(jnp.bfloat16), vals, preferred_element_type=jnp.float32
            )

    q_own = qp.at[head]

    def absorb_both(block):
        absorb(block, q_own, 0)
        absorb(block, q_far, 1)

    def place(n):
        dist = (n + 1) // 2
        return jnp.where(n % 2 == 1, zi - dist, zi + dist), 1 - n % 2

    def line_steps(j, take):
        def line_step(n, carry):
            zz, way = place(n)

            @pl.when((zz >= 0) & (zz < half))
            def _():
                block = held.at[j, zz, x]
                line_copy(j, block, zz, way).wait_recv()
                ahead = jnp.where(way == 0, zi + 1, zi - 1)

                @pl.when((ahead >= 0) & (ahead < half))
                def _():
                    line_copy(j, block, zz, way).start()

                if inner == 2:
                    side_copy(j, block, zz).start()
                take(block)

            return carry

        lax.fori_loop(1, 2 * half - 1, line_step, 0)

    def line_again(j):
        def again(n, carry):
            zz, _ = place(n)

            @pl.when((zz >= 0) & (zz < half))
            def _():
                absorb(held.at[j, zz, x], q_far, 1)

            return carry

        lax.fori_loop(1, 2 * half - 1, again, 0)

    def side_steps(j, begin):
        def side_step(n, carry):
            zz, _ = place(n)

            @pl.when((zz >= 0) & (zz < half))
            def _():
                block = held.at[j, zz, 1 - x]
                side_copy(j, block, zz).wait_recv()
                absorb_both(block)

            return carry

        lax.fori_loop(begin, 2 * half - 1, side_step, 0)

    near = held.at[0, zi, 1 - x]
    far = held.at[1, zi, x]
    absorb(own, q_own, 0)
    if inner == 2:
        side_copy(0, near, zi).wait_recv()
        absorb(near, q_own, 0)
    line_steps(0, lambda block: absorb(block, q_own, 0))
    cross_kv.wait_recv()
    start_from(1, far)
    absorb(far, q_own, 0)
    cross_q.wait_recv()
    absorb(own, q_far, 1)
    absorb(far, q_far, 1)
    line_steps(1, absorb_both)
    line_again(0)
    if inner == 2:
        absorb(near, q_far, 1)
        side_steps(0, 1)
        side_steps(1, 0)

    share = rows // n_tp
    lam = lam_ref[head]
    columns = pl.ds(pl.multiple_of((mt * 2 + head) * vd, vd), vd)
    copies = []
    for group, sp in ((1, mirror), (0, me)):
        read_a = acc_ref[2 * group] / l_ref[2 * group][:, :1]
        read_b = acc_ref[2 * group + 1] / l_ref[2 * group + 1][:, :1]
        combined = read_a - lam * read_b
        combined = (
            combined
            * lax.rsqrt(jnp.mean(combined * combined, axis=-1, keepdims=True) + norm_epsilon)
            * gain_ref[...]
        )
        stage[group] = combined.astype(jnp.bfloat16)
        for t in range(n_tp):
            to = (mt + t) % n_tp
            span = pl.ds(pl.multiple_of(to * share, share), share)
            if group == 0 and t == 0:
                out_ref[:, columns] = stage[0, span, :]
                continue
            copy = pltpu.make_async_remote_copy(
                src_ref=stage.at[group, span],
                dst_ref=out_ref.at[:, columns],
                send_sem=head_send.at[group, t],
                recv_sem=head_recv.at[group, t],
                device_id={"sp": sp, "tp": to},
                device_id_type=MESH,
            )
            copy.start()
            copies.append(copy)

    cross_q.wait_send()
    cross_kv.wait_send()
    for j in range(2):

        def drain(n, carry):
            zz, way = place(n)

            @pl.when((zz >= 0) & (zz < half))
            def _():
                ahead = jnp.where(way == 0, zi + 1, zi - 1)

                @pl.when((ahead >= 0) & (ahead < half))
                def _():
                    line_copy(j, own, zz, way).wait_send()

                if inner == 2:
                    side_copy(j, own, zz).wait_send()

            return carry

        lax.fori_loop(1, 2 * half - 1, drain, 0)

        @pl.when(zi + 1 < half)
        def _():
            line_copy(j, own, zi, 0).wait_send()

        @pl.when(zi > 0)
        def _():
            line_copy(j, own, zi, 1).wait_send()

        if inner == 2:
            side_copy(j, own, zi).wait_send()
    for copy in copies:
        copy.wait()


def attend(n_sp, n_tp, k1, k2, v, q1, q2, lam, gain):
    rows = q1.shape[0]
    inner = pair_of(n_sp)
    half = n_sp // inner // 2
    assert lam.shape[0] == 2 and half * inner * 2 == n_sp
    vd = v.shape[1] // 2
    qk = q1.shape[1] // 2
    cols = 2 * qk + vd
    vmem = pl.BlockSpec(memory_space=pltpu.VMEM)
    dma = pltpu.SemaphoreType.DMA
    return pl.pallas_call(
        functools.partial(attend_kernel, n_sp, n_tp, vd),
        out_shape=jax.ShapeDtypeStruct((rows // n_tp, n_tp * 2 * vd), jnp.bfloat16),
        in_specs=[vmem] * 5 + [pl.BlockSpec(memory_space=pltpu.SMEM), vmem],
        out_specs=vmem,
        scratch_shapes=[
            pltpu.VMEM((2, rows, cols), jnp.bfloat16),
            pltpu.VMEM((2, rows, 2 * qk), jnp.bfloat16),
            pltpu.VMEM((2, half, inner, rows, cols), jnp.bfloat16),
            pltpu.VMEM((rows, 2 * qk), jnp.bfloat16),
            pltpu.VMEM((4, rows, 128), jnp.float32),
            pltpu.VMEM((4, rows, 128), jnp.float32),
            pltpu.VMEM((4, rows, vd), jnp.float32),
            pltpu.VMEM((2, rows, vd), jnp.bfloat16),
            dma((2,)),
            dma((2,)),
            dma((2, 2, half)),
            dma((2, half)),
            dma((2, half)),
            dma((2, half)),
            dma((2, n_tp)),
            dma((2, n_tp)),
        ],
        compiler_params=pltpu.CompilerParams(
            collective_id=0, has_side_effects=True, vmem_limit_bytes=VMEM_LIMIT
        ),
    )(k1, k2, v, q1, q2, lam, gain)


def tp_peers(n_tp):
    inner = pair_of(n_tp)
    mt = lax.axis_index("tp")
    o, c = mt // inner, mt % inner
    across = [((o + d) % (n_tp // inner)) * inner + c for d in range(1, n_tp // inner)]
    return inner, across, o * inner + (inner - 1 - c)


def greet_all(n_sp, n_tp):
    me, mt = lax.axis_index("sp"), lax.axis_index("tp")
    inner, across, partner = tp_peers(n_tp)
    peers = [{"sp": (me + s) % n_sp, "tp": mt} for s in range(1, n_sp)]
    peers += [{"sp": me, "tp": t} for t in across]
    if inner == 2:
        peers.append({"sp": me, "tp": partner})
    greet(peers)


def dispatch_kernel(
    n_sp, n_tp, rows_ref, out_ref, sp_send, sp_recv, y_send, y_recv, c_send, c_recv, own_sem
):
    me, mt = lax.axis_index("sp"), lax.axis_index("tp")
    inner, across, partner = tp_peers(n_tp)
    groups = n_tp // inner
    o = mt // inner
    greet_all(n_sp, n_tp)

    def sp_copy(d):
        to = (me + d) % n_sp
        return pltpu.make_async_remote_copy(
            src_ref=rows_ref.at[to],
            dst_ref=out_ref.at[:, mt, me],
            send_sem=sp_send.at[d],
            recv_sem=sp_recv.at[d],
            device_id={"sp": to, "tp": mt},
            device_id_type=MESH,
        )

    def tp_copy(t, s, to, send, recv):
        return pltpu.make_async_remote_copy(
            src_ref=out_ref.at[:, t, s],
            dst_ref=out_ref.at[:, t, s],
            send_sem=send,
            recv_sem=recv,
            device_id={"sp": me, "tp": to},
            device_id_type=MESH,
        )

    order = sorted(range(1, n_sp), key=lambda d: min(d, n_sp - d))
    for d in reversed(order):
        sp_copy(d).start()
    own = pltpu.make_async_copy(rows_ref.at[me], out_ref.at[:, mt, me], own_sem)
    own.start()
    own.wait()
    started = []

    def spread(d):
        s = (me - d + n_sp) % n_sp
        for g in range(1, groups):
            copy = tp_copy(mt, s, across[g - 1], y_send.at[g, d], y_recv.at[g, d])
            copy.start()
            started.append(copy)
        if inner == 2:
            copy = tp_copy(mt, s, partner, c_send.at[0, d], c_recv.at[0, d])
            copy.start()
            started.append(copy)

    def relay(d):
        s = (me - d + n_sp) % n_sp
        for g in range(1, groups):
            source = ((o - g + groups) % groups) * inner + mt % inner
            tp_copy(source, s, partner, y_send.at[g, d], y_recv.at[g, d]).wait_recv()
            if inner == 2:
                copy = tp_copy(source, s, partner, c_send.at[g, d], c_recv.at[g, d])
                copy.start()
                started.append(copy)

    order = order[::-1]
    sequence = [0] + order
    spread(0)
    for i, d in enumerate(order):
        sp_copy(d).wait_recv()
        spread(d)
        relay(sequence[i])
    relay(sequence[-1])
    for d in range(n_sp):
        s = (me - d + n_sp) % n_sp
        if inner == 2:
            for g in range(groups):
                source = ((o - g + groups) % groups) * inner + (1 - mt % inner)
                tp_copy(source, s, partner, c_send.at[g, d], c_recv.at[g, d]).wait_recv()
    for copy in started:
        copy.wait_send()
    for d in order:
        sp_copy(d).wait_send()


def dispatch(n_sp, n_tp, rows):
    _, experts, cap, width = rows.shape
    groups = n_tp // pair_of(n_tp)
    sem = pltpu.SemaphoreType.DMA
    hbm = pl.BlockSpec(memory_space=pltpu.VMEM)
    return pl.pallas_call(
        functools.partial(dispatch_kernel, n_sp, n_tp),
        out_shape=jax.ShapeDtypeStruct((experts, n_tp, n_sp, cap, width), rows.dtype),
        in_specs=[hbm],
        out_specs=pl.BlockSpec(memory_space=pl.ANY),
        scratch_shapes=[
            sem((n_sp,)),
            sem((n_sp,)),
            sem((groups, n_sp)),
            sem((groups, n_sp)),
            sem((groups, n_sp)),
            sem((groups, n_sp)),
            sem,
        ],
        compiler_params=pltpu.CompilerParams(
            collective_id=1, has_side_effects=True, vmem_limit_bytes=VMEM_LIMIT
        ),
    )(rows)


def collect_kernel(
    n_sp,
    n_tp,
    part_ref,
    out_ref,
    from_core,
    from_across,
    summed,
    total,
    c_send,
    c_recv,
    y_send,
    y_recv,
    sp_send,
    sp_recv,
):
    me, mt = lax.axis_index("sp"), lax.axis_index("tp")
    inner, across, partner = tp_peers(n_tp)
    groups = n_tp // inner
    o, c = mt // inner, mt % inner
    greet_all(n_sp, n_tp)
    order = sorted(range(1, n_sp), key=lambda d: min(d, n_sp - d), reverse=True) + [0]

    def to_of(d):
        return (me + d) % n_sp

    def core_copy(d, g):
        row = ((o + g) % groups) * inner + (inner - 1 - c)
        return pltpu.make_async_remote_copy(
            src_ref=part_ref.at[:, row, to_of(d)],
            dst_ref=from_core.at[d, g],
            send_sem=c_send.at[d, g],
            recv_sem=c_recv.at[d, g],
            device_id={"sp": me, "tp": partner},
            device_id_type=MESH,
        )

    def across_copy(d, g):
        return pltpu.make_async_remote_copy(
            src_ref=summed.at[d, g],
            dst_ref=from_across.at[d, g],
            send_sem=y_send.at[d, g],
            recv_sem=y_recv.at[d, g],
            device_id={"sp": me, "tp": across[g - 1]},
            device_id_type=MESH,
        )

    def sp_copy(d):
        return pltpu.make_async_remote_copy(
            src_ref=total.at[d],
            dst_ref=out_ref.at[me],
            send_sem=sp_send.at[d],
            recv_sem=sp_recv.at[d],
            device_id={"sp": to_of(d), "tp": mt},
            device_id_type=MESH,
        )

    if inner == 2:
        for d in order:
            for g in list(range(1, groups)) + [0]:
                core_copy(d, g).start()

    def pair_sum(d, g):
        row = ((o + g) % groups) * inner + c
        value = part_ref[:, row, to_of(d)].astype(jnp.float32)
        if inner == 2:
            core_copy(d, g).wait_recv()
            value = value + from_core[d, g].astype(jnp.float32)
        return value

    def first(d):
        for g in range(1, groups):
            summed[d, g] = pair_sum(d, g).astype(summed.dtype)
            across_copy(d, g).start()

    def second(d):
        value = pair_sum(d, 0)
        for g in range(1, groups):
            across_copy(d, g).wait_recv()
            value = value + from_across[d, g].astype(jnp.float32)
        value = value.astype(total.dtype)
        if d == 0:
            out_ref[me] = value
        else:
            total[d] = value
            sp_copy(d).start()

    ahead = min(3, n_sp)
    for d in order[:ahead]:
        first(d)
    for i, d in enumerate(order):
        second(d)
        if i + ahead < n_sp:
            first(order[i + ahead])
    for d in range(1, n_sp):
        sp_copy(d).wait_recv()
    for d in range(n_sp):
        if d:
            sp_copy(d).wait_send()
        for g in range(groups):
            if g:
                across_copy(d, g).wait_send()
            if inner == 2:
                core_copy(d, g).wait_send()


def collect(n_sp, n_tp, part):
    experts, _, _, cap, width = part.shape
    groups = n_tp // pair_of(n_tp)
    sem = pltpu.SemaphoreType.DMA
    vmem = pl.BlockSpec(memory_space=pltpu.VMEM)
    piece = (experts, cap, width)
    return pl.pallas_call(
        functools.partial(collect_kernel, n_sp, n_tp),
        out_shape=jax.ShapeDtypeStruct((n_sp,) + piece, part.dtype),
        in_specs=[vmem],
        out_specs=vmem,
        scratch_shapes=[
            pltpu.VMEM((n_sp, groups) + piece, part.dtype),
            pltpu.VMEM((n_sp, groups) + piece, part.dtype),
            pltpu.VMEM((n_sp, groups) + piece, part.dtype),
            pltpu.VMEM((n_sp,) + piece, part.dtype),
            sem((n_sp, groups)),
            sem((n_sp, groups)),
            sem((n_sp, groups)),
            sem((n_sp, groups)),
            sem((n_sp,)),
            sem((n_sp,)),
        ],
        compiler_params=pltpu.CompilerParams(
            collective_id=2, has_side_effects=True, vmem_limit_bytes=VMEM_LIMIT
        ),
    )(part)


def attention_phase(n_sp, n_tp, r, arrived, filler):
    inner, pair = 2, 2
    length = n_sp // inner
    me, mt = lax.axis_index("sp"), lax.axis_index("tp")
    z, x = me // inner, me % inner
    y, c = mt // pair, mt % pair
    rows, qk = r.q1_ref.shape[0], r.q1_ref.shape[1] // 2
    vd = r.v_ref.shape[1] // 2
    keys = 2 * qk
    scale = 1.0 / math.sqrt(qk)
    exact = math.frexp(scale)[0] == 0.5
    early, after = (scale, 1.0) if exact else (1.0, scale)
    home = c == z // pair
    partner = y * pair + (1 - c)
    across = z * inner + (1 - x)

    def spot(zz):
        return zz * inner + x

    for h in range(2):
        at = slice(h * qk, (h + 1) * qk)
        block = jnp.concatenate([r.k1_ref[:, at], r.k2_ref[:, at]], axis=1)
        turned = jnp.concatenate(
            [
                r.v_ref[base : base + vd, h * vd : (h + 1) * vd].astype(jnp.float32).T
                for base in range(0, rows, vd)
            ],
            axis=0,
        ).astype(jnp.bfloat16)
        query = jnp.concatenate([r.q1_ref[:, at], r.q2_ref[:, at]], axis=1) * jnp.bfloat16(early)
        r.kv_out[h, :, 0:keys] = block
        r.kv_out[h, :, keys : keys + vd] = turned
        r.q_out[h] = query

        @pl.when(z == pair * c + h)
        def _():
            r.held[z, 0, :, 0:keys] = block
            r.held[z, 0, :, keys : keys + vd] = turned
            r.q_in[h] = query

    r.lam_mine[...] = jnp.full(r.lam_mine.shape, r.lam_ref[z % pair], jnp.float32)
    r.m_ref[...] = jnp.full(r.m_ref.shape, -1e30, jnp.float32)
    r.l_ref[...] = jnp.zeros(r.l_ref.shape, jnp.float32)
    r.acc_ref[...] = jnp.zeros(r.acc_ref.shape, jnp.float32)
    r.qt[...] = jnp.zeros(r.qt.shape, r.qt.dtype)
    arrived()

    def remote(src, dst, send, recv, sp, tp):
        return pltpu.make_async_remote_copy(
            src_ref=src,
            dst_ref=dst,
            send_sem=send,
            recv_sem=recv,
            device_id={"sp": sp, "tp": tp},
            device_id_type=MESH,
        )

    def first_q(h):
        return remote(
            r.q_out.at[h],
            r.q_in.at[z % pair],
            r.first_send.at[0, h],
            r.q_recv.at[z % pair],
            spot(pair * c + h),
            y * pair + z // pair,
        )

    def first_kv(h):
        return remote(
            r.kv_out.at[h],
            r.held.at[z, 0],
            r.first_send.at[1, h],
            r.kv_recv.at[z, 0],
            spot(pair * c + h),
            y * pair + z // pair,
        )

    def to_core(zz, side):
        block = r.held.at[zz, side]
        return remote(block, block, r.core_send.at[zz, side], r.kv_recv.at[zz, side], me, partner)

    def to_side(zz):
        return remote(
            r.held.at[zz, 0], r.held.at[zz, 1], r.side_send.at[zz], r.kv_recv.at[zz, 1], across, mt
        )

    lam_copy = remote(r.lam_mine, r.lam_far, r.lam_sem.at[0], r.lam_sem.at[1], me, partner)

    def away(h):
        return z != pair * c + h

    order = [z, z + 1 - 2 * (z % pair), pair - z // pair, (length - 1) * (1 - z // pair)]

    @pl.when(home)
    def _():
        to_side(z).start()
        to_core(z, 0).start()

    for h in range(2):

        @pl.when(away(h))
        def _():
            first_q(h).start()

    for h in range(2):

        @pl.when(away(h))
        def _():
            first_kv(h).start()

    lam_copy.start()
    filler()

    for g in range(2):

        @pl.when((z != pair * c + g))
        def _():
            remote(
                r.q_out.at[g], r.q_in.at[g], r.first_send.at[0, g], r.q_recv.at[g], me, mt
            ).wait_recv()

        turned = r.q_in[g].astype(jnp.float32).T.astype(jnp.bfloat16)
        r.qt[0:qk, 2 * g * rows : (2 * g + 1) * rows] = turned[0:qk]
        r.qt[qk:keys, (2 * g + 1) * rows : (2 * g + 2) * rows] = turned[qk:keys]

    def absorb(zz, side):
        block_keys = r.held[zz, side, :, 0:keys]
        turned = jnp.concatenate(
            [r.held[zz, side, base : base + vd, keys : keys + vd] for base in range(0, rows, vd)], axis=1
        )
        for part in range(4):
            at = slice(part * rows, (part + 1) * rows)
            scores = jnp.dot(block_keys, r.qt[:, at], preferred_element_type=jnp.float32)
            if after != 1.0:
                scores = scores * after
            old = r.m_ref[:, at]
            new = jnp.maximum(old, jnp.max(scores, axis=0, keepdims=True))
            shrink = jnp.exp(old - new)
            expo = jnp.exp(scores - new)
            r.m_ref[:, at] = new
            r.l_ref[:, at] = r.l_ref[:, at] * shrink + jnp.sum(expo, axis=0, keepdims=True)
            r.acc_ref[:, at] = r.acc_ref[:, at] * shrink + jnp.dot(
                turned, expo.astype(jnp.bfloat16), preferred_element_type=jnp.float32
            )

    near_first = ((0, 0), (0, 1), (1, 0), (1, 1), (2, 0), (3, 0), (2, 1), (3, 1))
    far_first = ((0, 0), (0, 1), (1, 0), (2, 0), (1, 1), (3, 0), (2, 1), (3, 1))

    def pick(values, n):
        result = values[0]
        for k in range(1, len(values)):
            result = jnp.where(n == k, values[k], result)
        return result

    def step(n, carry):
        at_home = [pick([p[i] for p in near_first], n) for i in range(2)]
        at_far = [pick([p[i] for p in far_first], n) for i in range(2)]
        zz = pick(order, jnp.where(home, at_home[0], at_far[0]))
        side = jnp.where(home, at_home[1], at_far[1])
        direct = zz // pair == c
        local = home & (n == 0)

        @pl.when(jnp.logical_not(local))
        def _():
            to_core(zz, side).wait_recv()

            @pl.when(direct & (side == 0))
            def _():
                to_side(zz).start()

            @pl.when(direct)
            def _():
                to_core(zz, side).start()

        absorb(zz, side)
        return carry

    lax.fori_loop(0, 2 * length, step, 0)

    share = rows // n_tp
    lam_copy.wait()
    lam = jnp.where(home, r.lam_mine[0:1, 0:1], r.lam_far[0:1, 0:1])
    head = y * length + z
    columns = pl.ds(pl.multiple_of(head * vd, vd), vd)

    def piece(g, t):
        to = (mt + t) % n_tp
        span = pl.ds(pl.multiple_of(to * share, share), share)
        return remote(
            r.stage.at[g, span],
            r.token_ref.at[:, columns],
            r.head_send.at[g, t],
            r.head_recv.at[head],
            spot(pair * c + g),
            to,
        )

    def own(g):
        return z == pair * c + g

    for g in (1, 0):
        reads = []
        for which in range(2):
            at = slice((2 * g + which) * rows, (2 * g + which + 1) * rows)
            reads.append(r.acc_ref[:, at] / r.l_ref[:, at])
        combined = reads[0] - lam * reads[1]
        combined = combined * lax.rsqrt(
            jnp.mean(combined * combined, axis=0, keepdims=True) + norm_epsilon
        )
        r.stage[g] = (combined.T * r.gain_ref[...]).astype(jnp.bfloat16)
        for t in range(1, n_tp):
            piece(g, t).start()

        @pl.when(own(g))
        def _():
            r.token_ref[:, columns] = r.stage[g, pl.ds(pl.multiple_of(mt * share, share), share), :]

        @pl.when(jnp.logical_not(own(g)))
        def _():
            piece(g, 0).start()

    def head_copy(hd):
        at = pl.ds(pl.multiple_of(hd * vd, vd), vd)
        return remote(
            r.stage.at[0, 0:share], r.token_ref.at[:, at], r.head_send.at[0, 0], r.head_recv.at[hd], me, mt
        )

    def heads_of(plane):
        for k in range(length):
            hd = plane * length + k

            @pl.when((hd != head) | jnp.logical_not(home))
            def _():
                head_copy(hd).wait_recv()

    def finish():
        for g in range(2):
            for t in range(1, n_tp):
                piece(g, t).wait_send()

            @pl.when(jnp.logical_not(own(g)))
            def _():
                piece(g, 0).wait_send()

            @pl.when(away(g))
            def _():
                first_q(g).wait_send()
                first_kv(g).wait_send()

        for zz in range(length):

            @pl.when(c == zz // pair)
            def _():
                to_side(zz).wait_send()
                to_core(zz, 0).wait_send()
                to_core(zz, 1).wait_send()

    return finish, heads_of


def routing_tables(r, experts_in_all, cap):
    ids = r.ids_ref[...].astype(jnp.float32)
    top, share = ids.shape
    names = lax.broadcasted_iota(jnp.int32, (experts_in_all, share), 0).astype(jnp.float32)
    before = lax.broadcasted_iota(jnp.int32, (share, share), 0)
    before = before < lax.broadcasted_iota(jnp.int32, (share, share), 1)
    before = before.astype(jnp.float32).astype(jnp.bfloat16)
    taken = jnp.zeros((experts_in_all, 1), jnp.float32)
    places = lax.broadcasted_iota(jnp.int32, (experts_in_all * cap, share), 0).astype(jnp.float32)
    logits = [r.logits_ref[k : k + 1, :] for k in range(top)]
    highest = functools.reduce(jnp.maximum, logits)
    powers = [jnp.exp(logit - highest) for logit in logits]
    total = sum(powers)
    table = jnp.zeros(places.shape, jnp.float32)
    spread = jnp.zeros(places.shape, jnp.float32)
    for k in range(top):
        hit = (names == ids[k : k + 1, :]).astype(jnp.float32)
        earlier = jnp.dot(hit.astype(jnp.bfloat16), before, preferred_element_type=jnp.float32)
        rank = jnp.sum(hit * (earlier + taken), axis=0, keepdims=True)
        taken = taken + jnp.sum(hit, axis=1, keepdims=True)
        placed = (places == ids[k : k + 1, :] * cap + rank).astype(jnp.float32)
        table = table + placed
        spread = spread + placed * (powers[k] / total * r.prob_ref[...])
    r.table[...] = table.astype(jnp.bfloat16)
    turned = spread.T
    high = turned.astype(jnp.bfloat16)
    r.spread[0:share] = high
    r.spread[share : 2 * share] = (turned - high.astype(jnp.float32)).astype(jnp.bfloat16)


def token_phase(r, wait_weights, y, heads_of):
    share, width = r.residual.shape
    tile = math.gcd(width, 512)
    columns = [slice(n, n + tile) for n in range(0, width, tile)]
    wait_weights()
    depth = r.token_ref.shape[1] // 2

    def plane_mix(plane, at):
        span = pl.ds(pl.multiple_of(plane * depth, depth), depth)
        return jnp.dot(
            r.token_ref[:, span], r.out_w[span, at], preferred_element_type=jnp.float32
        )

    heads_of(y)
    for at in columns:
        r.mix[:, at] = plane_mix(y, at) + r.residual[:, at].astype(jnp.float32)
    heads_of(1 - y)
    square = jnp.zeros((share, 1), jnp.float32)
    for at in columns:
        hidden = (r.mix[:, at] + plane_mix(1 - y, at)).astype(jnp.bfloat16)
        r.hidden[:, at] = hidden
        hidden = hidden.astype(jnp.float32)
        square = square + jnp.sum(hidden * hidden, axis=1, keepdims=True)
    factor = lax.rsqrt(square / width + norm_epsilon)
    n_sp, experts, cap = r.outgoing.shape[:3]
    for at in columns:
        normed = r.hidden[:, at].astype(jnp.float32) * factor * r.norm_ref[:, at]
        rows = jnp.dot(
            r.table[...], normed.astype(jnp.bfloat16), preferred_element_type=jnp.float32
        ).astype(jnp.bfloat16)
        r.outgoing[:, :, :, at] = rows.reshape(n_sp, experts, cap, tile)


def expert_phase(n_sp, n_tp, r, weights, finish):
    me, mt = lax.axis_index("sp"), lax.axis_index("tp")
    inner_sp = 2
    z, x = me // inner_sp, me % inner_sp
    inner, across, partner = tp_peers(n_tp)
    groups = n_tp // inner
    o, c = mt // inner, mt % inner
    _, experts, cap, _ = r.outgoing.shape

    def flip(number, by):
        low = (number % 2 + by % 2) % 2
        return (number // 2 + by // 2) % 2 * 2 + low

    def peer_of(i):
        return flip(z, i // inner_sp) * inner_sp + flip(x, i % inner_sp)

    def span(t):
        return pl.ds(pl.multiple_of(t * cap, cap), cap)

    def remote(src, dst, send, recv, sp, tp):
        return pltpu.make_async_remote_copy(
            src_ref=src,
            dst_ref=dst,
            send_sem=send,
            recv_sem=recv,
            device_id={"sp": sp, "tp": tp},
            device_id_type=MESH,
        )

    pieces = n_sp * experts

    def sp_copy(j):
        i, e = j // experts, j % experts
        to = peer_of(i)
        block = r.rows.at[i, e, span(mt)]
        return remote(r.outgoing.at[to, e], block, r.sp_send.at[j], r.sp_recv.at[j], to, mt)

    def across_in(j, g, t):
        block = r.rows.at[j // experts, j % experts, span(t)]
        return remote(block, block, r.y_send.at[g, j], r.y_recv.at[g, j], me, across[g - 1])

    def core_in(j, g, t):
        block = r.rows.at[j // experts, j % experts, span(t)]
        return remote(block, block, r.c_send.at[g, j], r.c_recv.at[g, j], me, partner)

    def core_out(j, g):
        row = ((o + g) % groups) * inner + (inner - 1 - c)
        block = r.part.at[j, span(row)]
        return remote(
            block, r.from_core.at[j, g], r.rc_send.at[j, g], r.rc_recv.at[j, g], me, partner
        )

    def across_out(j, g):
        return remote(
            r.summed.at[j, g],
            r.from_across.at[j, g],
            r.ry_send.at[j, g],
            r.ry_recv.at[j, g],
            me,
            across[g - 1],
        )

    def sp_out(j):
        i, e = j // experts, j % experts
        block = r.returned.at[me, e]
        return remote(r.total.at[j], block, r.rs_send.at[j], r.rs_recv.at[j], peer_of(i), mt)

    def source(g):
        return ((o - g + groups) % groups) * inner + c

    for j in (2, 8, 4, 3, 9, 5, 10, 6, 11, 7, 12, 13, 14, 15):
        sp_copy(j).start()
    r.rows[0, :, span(mt), :] = r.outgoing[me]

    def spread(j):
        @pl.when(j >= experts)
        def _():
            sp_copy(j).wait_recv()

        for g in range(1, groups):
            across_in(j, g, mt).start()
        core_in(j, 0, mt).start()

    def relay(j):
        for g in range(1, groups):
            across_in(j, g, source(g)).wait_recv()
            core_in(j, g, source(g)).start()

    half = n_sp // 2
    ready = half * experts

    def compute(j):
        @pl.when(j == ready)
        def _():
            for copy in weights:
                copy.wait()

        for g in range(groups):
            core_in(j, g, source(g)).wait_recv()
        e = j % experts
        rows = r.rows[j // experts, e]
        gate = jnp.dot(rows, r.gate_w[e], preferred_element_type=jnp.float32)
        upper = jnp.dot(rows, r.up_w[e], preferred_element_type=jnp.float32)
        middle = (gate / (1.0 + jnp.exp(-gate)) * upper).astype(jnp.bfloat16)
        r.part[j] = jnp.dot(middle, r.down_w[e], preferred_element_type=jnp.float32).astype(
            r.part.dtype
        )
        for g in list(range(1, groups)) + [0]:
            core_out(j, g).start()

    def pair_sum(j, g):
        row = ((o + g) % groups) * inner + c
        value = r.part[j, span(row), :].astype(jnp.float32)
        core_out(j, g).wait_recv()
        return value + r.from_core[j, g].astype(jnp.float32)

    def first(j):
        for g in range(1, groups):
            r.summed[j, g] = pair_sum(j, g).astype(r.summed.dtype)
            across_out(j, g).start()

    def second(j):
        value = pair_sum(j, 0)
        for g in range(1, groups):
            across_out(j, g).wait_recv()
            value = value + r.from_across[j, g].astype(jnp.float32)
        value = value.astype(r.total.dtype)

        @pl.when(j < experts)
        def _():
            r.returned[me, j] = value

        @pl.when(j >= experts)
        def _():
            r.total[j] = value
            sp_out(j).start()

    def far_first(n):
        near = jnp.where(n < ready + half, n - half, jnp.where(n < ready + 6, n - 10, n - 14))
        return jnp.where(n < ready, n + ready, near)

    def arrival(n):
        mixed = n // 2 + jnp.where(n % 2 == 0, 2, 6)
        return jnp.where((n < half) | (n >= ready + half), n, mixed)

    def turned(stage):
        return lambda n: stage(far_first(n))

    stages = tuple((lambda n, f=f: f(arrival(n))) for f in (spread, relay)) + tuple(turned(stage) for stage in (compute, first, second))
    lags = (0, 3, 12, 14, 17)

    def step(n, carry):
        for stage, lag in zip(stages, lags):

            @pl.when((n >= lag) & (n < pieces + lag))
            def _():
                stage(n - lag)

        return carry

    lax.fori_loop(0, pieces + lags[-1], step, 0)

    finish()

    def drain(j, carry):
        @pl.when(j >= experts)
        def _():
            sp_out(j).wait_send()
            sp_copy(j).wait_send()

        for g in range(groups):
            if g:
                across_in(j, g, mt).wait_send()
                across_out(j, g).wait_send()
            core_in(j, g, mt).wait_send()
            core_out(j, g).wait_send()
        return carry

    lax.fori_loop(0, pieces, drain, 0)

    def arrive(j, carry):
        sp_out(j).wait_recv()
        return carry

    lax.fori_loop(experts, pieces, arrive, 0)
    share = r.residual.shape[0]
    width = r.residual.shape[1]
    tile = math.gcd(width, 512)
    for n in range(0, width, tile):
        at = slice(n, n + tile)
        both = jnp.dot(
            r.spread[...],
            r.returned[:, :, :, at].reshape(pieces * cap, tile),
            preferred_element_type=jnp.float32,
        )
        r.out_ref[:, at] = (r.hidden[:, at].astype(jnp.float32) + (both[:share] + both[share:])).astype(jnp.bfloat16)


def layer_kernel(n_sp, n_tp, names, *refs):
    r = types.SimpleNamespace(**dict(zip(names, refs)))
    me, mt = lax.axis_index("sp"), lax.axis_index("tp")
    inner = 2
    z, x = me // inner, me % inner
    barrier = pltpu.get_barrier_semaphore()
    lines = [(zz * inner + x, t) for zz in range(n_sp // inner) for t in range(n_tp)]
    lines += [(zz * inner + (1 - x), mt) for zz in range(n_sp // inner)]
    for sp, tp in lines:

        @pl.when((sp != me) | (tp != mt))
        def _():
            pl.semaphore_signal(
                barrier, inc=1, device_id={"sp": sp, "tp": tp}, device_id_type=MESH
            )

    def loads(pairs):
        copies = [
            pltpu.make_async_copy(getattr(r, src), getattr(r, dst), r.load_sem.at[k])
            for k, (src, dst) in pairs
        ]
        for copy in copies:
            copy.start()
        return copies

    pairs = list(enumerate(LOADED))
    first = loads(pairs[:5])
    middle = loads(pairs[5:7])
    last = loads(pairs[7:])
    for copy in first:
        copy.wait()

    def wait_middle():
        for copy in middle:
            copy.wait()

    experts, cap = r.outgoing.shape[1:3]
    finish, heads_of = attention_phase(
        n_sp,
        n_tp,
        r,
        lambda: pl.semaphore_wait(barrier, len(lines) - 1),
        lambda: routing_tables(r, n_sp * experts, cap),
    )
    token_phase(r, wait_middle, mt // 2, heads_of)
    expert_phase(n_sp, n_tp, r, last, finish)


LOADED = (
    ("k1_hbm", "k1_ref"),
    ("k2_hbm", "k2_ref"),
    ("v_hbm", "v_ref"),
    ("q1_hbm", "q1_ref"),
    ("q2_hbm", "q2_ref"),
    ("out_w_hbm", "out_w"),
    ("residual_hbm", "residual"),
    ("gate_hbm", "gate_w"),
    ("up_hbm", "up_w"),
    ("down_hbm", "down_w"),
)


def whole_layer(n_sp, n_tp, cap, big, lam, gain, norm, ids, logits, prob):
    k1, k2, v, q1, q2, out_w, residual, gate, up, down = big
    rows, keys = q1.shape
    length = n_sp // 2
    vd = v.shape[1] // 2
    cols = keys + vd
    share, width = residual.shape
    experts = gate.shape[0]
    pieces = n_sp * experts
    slots = pieces * cap
    groups = n_tp // 2
    bf16, f32 = jnp.bfloat16, jnp.float32
    vmem = pl.BlockSpec(memory_space=pltpu.VMEM)
    dma = pltpu.SemaphoreType.DMA
    piece = (experts, cap, width)
    scratch = [(dst, pltpu.VMEM(a.shape, a.dtype)) for (_, dst), a in zip(LOADED, big)]
    scratch += [
        ("token_ref", pltpu.VMEM((share, out_w.shape[0]), bf16)),
        ("kv_out", pltpu.VMEM((2, rows, cols), bf16)),
        ("q_out", pltpu.VMEM((2, rows, keys), bf16)),
        ("held", pltpu.VMEM((length, 2, rows, cols), bf16)),
        ("q_in", pltpu.VMEM((2, rows, keys), bf16)),
        ("qt", pltpu.VMEM((keys, 4 * rows), bf16)),
        ("m_ref", pltpu.VMEM((1, 4 * rows), f32)),
        ("l_ref", pltpu.VMEM((1, 4 * rows), f32)),
        ("acc_ref", pltpu.VMEM((vd, 4 * rows), f32)),
        ("stage", pltpu.VMEM((2, rows, vd), bf16)),
        ("lam_mine", pltpu.VMEM((8, 128), f32)),
        ("lam_far", pltpu.VMEM((8, 128), f32)),
        ("table", pltpu.VMEM((slots, share), bf16)),
        ("spread", pltpu.VMEM((2 * share, slots), bf16)),
        ("mix", pltpu.VMEM((share, width), f32)),
        ("hidden", pltpu.VMEM((share, width), bf16)),
        ("outgoing", pltpu.VMEM((n_sp,) + piece, bf16)),
        ("returned", pltpu.VMEM((n_sp,) + piece, bf16)),
        ("rows", pltpu.VMEM((n_sp, experts, n_tp * cap, width), bf16)),
        ("part", pltpu.VMEM((pieces, n_tp * cap, width), bf16)),
        ("from_core", pltpu.VMEM((pieces, groups, cap, width), bf16)),
        ("from_across", pltpu.VMEM((pieces, groups, cap, width), bf16)),
        ("summed", pltpu.VMEM((pieces, groups, cap, width), bf16)),
        ("total", pltpu.VMEM((pieces, cap, width), bf16)),
        ("load_sem", dma((len(LOADED),))),
        ("first_send", dma((2, 2))),
        ("core_send", dma((length, 2))),
        ("side_send", dma((length,))),
        ("kv_recv", dma((length, 2))),
        ("q_recv", dma((2,))),
        ("lam_sem", dma((2,))),
        ("head_send", dma((2, n_tp))),
        ("head_recv", dma((2 * n_tp,))),
        ("sp_send", dma((pieces,))),
        ("sp_recv", dma((pieces,))),
        ("y_send", dma((groups, pieces))),
        ("y_recv", dma((groups, pieces))),
        ("c_send", dma((groups, pieces))),
        ("c_recv", dma((groups, pieces))),
        ("rc_send", dma((pieces, groups))),
        ("rc_recv", dma((pieces, groups))),
        ("ry_send", dma((pieces, groups))),
        ("ry_recv", dma((pieces, groups))),
        ("rs_send", dma((pieces,))),
        ("rs_recv", dma((pieces,))),
    ]
    small = ("gain_ref", "norm_ref", "ids_ref", "logits_ref", "prob_ref")
    names = [src for src, _ in LOADED] + ["lam_ref", *small, "out_ref"]
    names += [name for name, _ in scratch]
    return pl.pallas_call(
        functools.partial(layer_kernel, n_sp, n_tp, names),
        out_shape=pltpu.VMEM((share, width), bf16),
        in_specs=[pl.BlockSpec(memory_space=pltpu.HBM)] * len(LOADED)
        + [pl.BlockSpec(memory_space=pltpu.SMEM)]
        + [vmem] * len(small),
        out_specs=vmem,
        scratch_shapes=[shape for _, shape in scratch],
        compiler_params=pltpu.CompilerParams(
            collective_id=3, has_side_effects=True, vmem_limit_bytes=LAYER_LIMIT
        ),
    )(*big, lam, gain, norm, ids, logits, prob)


def layers_fit(n_sp, n_tp, rows, vd, keys, heads, experts, cap):
    square = heads == 2 and experts == 2 and n_sp == 8 and n_tp == 4
    return square and rows % vd == 0 and vd == keys and vd % 128 == 0 and cap % 16 == 0


def on_device(
    n_sp,
    n_tp,
    query_one,
    key_one,
    query_two,
    key_two,
    values,
    mix_lambda,
    head_gain,
    residual_in,
    out_weight,
    norm_gain,
    route_ids,
    route_logits,
    group_prob,
    gate_weight,
    up_weight,
    down_weight,
):
    share = residual_in.shape[0]
    top_count = route_ids.shape[1]
    local_experts = gate_weight.shape[0]
    expert_count = local_experts * n_sp
    capacity = max(2, 2 * share * top_count // expert_count)
    if layers_fit(
        n_sp,
        n_tp,
        query_one.shape[0],
        values.shape[1] // 2,
        query_one.shape[1],
        mix_lambda.shape[0],
        local_experts,
        capacity,
    ):
        big = (key_one, key_two, values, query_one, query_two, out_weight, residual_in)
        return whole_layer(
            n_sp,
            n_tp,
            capacity,
            big + (gate_weight, up_weight, down_weight),
            mix_lambda,
            head_gain[None, :],
            norm_gain[None, :],
            route_ids.T,
            route_logits.T,
            group_prob[None, :],
        )
    token_heads = attend(
        n_sp,
        n_tp,
        key_one,
        key_two,
        values,
        query_one,
        query_two,
        mix_lambda,
        head_gain[None, :],
    )
    mix = jnp.dot(token_heads, out_weight, preferred_element_type=jnp.float32)
    hidden_f = (residual_in.astype(jnp.float32) + mix).astype(jnp.bfloat16).astype(jnp.float32)
    normed = (
        hidden_f
        * lax.rsqrt(jnp.mean(hidden_f * hidden_f, axis=-1, keepdims=True) + norm_epsilon)
        * norm_gain
    ).astype(jnp.bfloat16)
    width = normed.shape[1]
    slots = expert_count * capacity
    flat_ids = route_ids.reshape(-1)
    one_hot = (flat_ids[:, None] == jnp.arange(expert_count, dtype=jnp.int32)[None, :]).astype(
        jnp.int32
    )
    earlier = jnp.cumsum(one_hot, axis=0) - one_hot
    rank = jnp.sum(earlier * one_hot, axis=1)
    slot_of = (flat_ids * capacity + rank).reshape(share, top_count)
    places = jnp.arange(slots, dtype=jnp.int32)
    table = sum(
        (places[:, None] == slot_of[None, :, k]).astype(jnp.bfloat16) for k in range(top_count)
    )
    outgoing = jnp.dot(table, normed, preferred_element_type=jnp.float32).astype(jnp.bfloat16)
    outgoing = outgoing.reshape(n_sp, local_experts, capacity, width)
    everyone = dispatch(n_sp, n_tp, outgoing).reshape(
        local_experts, n_tp * n_sp * capacity, width
    )
    gate = jnp.einsum("erd,edf->erf", everyone, gate_weight, preferred_element_type=jnp.float32)
    upper = jnp.einsum("erd,edf->erf", everyone, up_weight, preferred_element_type=jnp.float32)
    middle = (jax.nn.silu(gate) * upper).astype(jnp.bfloat16)
    part_sum = jnp.einsum(
        "erf,efd->erd", middle, down_weight, preferred_element_type=jnp.float32
    ).astype(jnp.bfloat16)
    returned = collect(
        n_sp, n_tp, part_sum.reshape(local_experts, n_tp, n_sp, capacity, width)
    ).reshape(slots, width)
    logits = [route_logits[:, k : k + 1] for k in range(top_count)]
    highest = functools.reduce(jnp.maximum, logits)
    powers = [jnp.exp(logit - highest) for logit in logits]
    route_weight = [power / sum(powers) * group_prob[:, None] for power in powers]
    spread = sum(
        jnp.where(places[None, :] == slot_of[:, k, None], route_weight[k], 0.0)
        for k in range(top_count)
    )
    high = spread.astype(jnp.bfloat16)
    low = (spread - high.astype(jnp.float32)).astype(jnp.bfloat16)
    both = jnp.dot(
        jnp.concatenate([high, low], axis=0), returned, preferred_element_type=jnp.float32
    )
    return (hidden_f + (both[:share] + both[share:])).astype(jnp.bfloat16)


def solution(mesh):
    in_specs = (
        P("sp", "tp"),
        P("sp", "tp"),
        P("sp", "tp"),
        P("sp", "tp"),
        P("sp", "tp"),
        P("tp"),
        P(),
        P(("sp", "tp"), None),
        P(),
        P(),
        P(("sp", "tp"), None),
        P(("sp", "tp"), None),
        P(("sp", "tp")),
        P("sp", None, "tp"),
        P("sp", None, "tp"),
        P("sp", "tp", None),
    )
    out_specs = P(("sp", "tp"), None)
    return jax.shard_map(
        functools.partial(on_device, mesh.shape["sp"], mesh.shape["tp"]),
        mesh=mesh,
        in_specs=in_specs,
        out_specs=out_specs,
        check_vma=False,
    )
```
